32 devices in a mesh: grp: 2 (over y), sp: 4 (over z), tp: 4 (over x, core).
Axes of the slice: x: 2, y: 2, z: 4, core: 2. Of those that a mesh axis runs over, the one named last changes fastest.
Arguments:
- queries: bfloat16 [4096, 1024], P(('grp', 'sp'), 'tp'), parts along dimension 0, may hold values from -120 to 120
- keys: bfloat16 [4096, 256], P(('grp', 'sp')), parts along dimension 0, may hold values from -6 to 6
- values: bfloat16 [4096, 256], P(('grp', 'sp')), parts along dimension 0, may hold values from -6 to 6
- sink: float32 [8], P('tp'), may hold values from 1 to 5
- resid: bfloat16 [4096, 2048], P(('grp', 'sp')), parts along dimension 0, may hold values from -100 to 100
- out_proj: bfloat16 [1024, 2048], P(None, 'tp'), may hold values from -1.5 to 1.5
- norm_gain: float32 [2048], replicated, may hold values from 0.1 to 1.9
- w_gate: bfloat16 [2048, 6144], P('sp', 'tp'), may hold values from -0.125 to 0.125
- w_up: bfloat16 [2048, 6144], P('sp', 'tp'), may hold values from -0.125 to 0.125
- conv_w: float32 [3, 6144], P(None, 'tp'), may hold values from -3 to 3
- conv_b: float32 [6144], P('tp'), may hold values from -3 to 3
- w_down: bfloat16 [6144, 2048], P('tp', 'sp'), may hold values from -0.21875 to 0.21875
Outputs:
- layer_out: bfloat16 [4096, 2048], P(('grp', 'sp'), 'tp'), parts along dimension 0
The draws below stay inside these ranges and needn't reach their ends.
There are 2 independent parts, one for each index of `grp`. The reference program is written for one: setup_inputs(seed, part) draws one part's arguments, and reference() takes and returns one part's arrays. A program takes and returns all parts, laid end to end along the dimension named above; an argument that names none is the same for every part. Nothing has to cross between parts.
All inputs are finite; a program needn't handle non-finite values.
Results may differ from the reference program's by a relative error of at most 0.015.
Values may be sent and summed in bfloat16 or wider, within the bound.
A program may use at most 64 MiB of HBM per device.

```python
import jax
import jax.numpy as jnp
from jax import lax

D = 2048
FF = 6144
H = 8
KVH = 2
HD = 128
WINDOW = 128
CONV = 3
TOK_DEV = 512
SEQ = 2048


def joint_qk(key):
    base = jax.random.fold_in(key, 11)
    key_q, key_k = jax.random.split(base)
    q_vals = jnp.clip(jax.random.normal(key_q, (SEQ, H, HD), jnp.float32), -6.0, 6.0)
    k_vals = jnp.clip(jax.random.normal(key_k, (SEQ, KVH, HD), jnp.float32), -6.0, 6.0)
    return (q_vals.reshape(SEQ, H * HD), k_vals.reshape(SEQ, KVH * HD))


def draw_queries(key, part):
    return joint_qk(key)[0].astype(jnp.bfloat16)


def draw_keys(key, part):
    return joint_qk(key)[1].astype(jnp.bfloat16)


def draw_resid(key, part):
    base = jax.random.fold_in(key, 23)
    key_n, key_r, key_c = jax.random.split(base, 3)
    trend = 0.5 + jnp.arange(D, dtype=jnp.float32) / D
    columns = jnp.exp(jax.random.uniform(key_c, (D,), jnp.float32, -0.7, 0.7)) * trend
    noise = jnp.clip(jax.random.normal(key_n, (SEQ, D), jnp.float32), -6.0, 6.0)
    rows = jnp.exp(jax.random.uniform(key_r, (SEQ, 1), jnp.float32, -0.69, 1.6))
    return jnp.clip(noise * rows * columns[None, :], -100.0, 100.0).astype(jnp.bfloat16)


def spiked(array, key, source, target, blocks, factor):
    def block_of(dim):
        return (jnp.arange(array.shape[dim]) // (array.shape[dim] // blocks)).reshape((-1,) + (1,) * (array.ndim - 1 - dim))

    first = jax.random.permutation(key, blocks)[block_of(target)]
    other_side = (block_of(target) + blocks // 2) % blocks
    return jnp.where((block_of(source) == first) | (block_of(source) == other_side), factor * array, array)


def steps_of(own_key, dims, cuts, least, high):
    loudness, own = 1.0, jax.random.fold_in(own_key, 6)
    for dim, parts in cuts:
        draws = jnp.exp(jax.random.uniform(jax.random.fold_in(own, dim), (parts,), jnp.float32, least / len(cuts), high / len(cuts)))
        loudness = loudness * jnp.repeat(draws, dims[dim] // parts).reshape([-1 if axis == dim else 1 for axis in range(len(dims))])
    return loudness


def gaussian(key, shape, scale, most, cuts=(), kind=jnp.bfloat16):
    drawn = scale * jax.random.normal(key, shape, jnp.float32)
    if cuts:
        drawn = drawn * steps_of(key, shape, cuts, -0.22, 0.18)
    return jnp.clip(drawn, -most, most).astype(kind)


def noise_with(own_key, extent, scale, reach, cuts, heavy, held_as=jnp.bfloat16):
    drawn = scale * jax.random.normal(own_key, extent, jnp.float32)
    if cuts:
        drawn = drawn * steps_of(own_key, extent, cuts, -0.22, 0.18)
    return jnp.clip(spiked(drawn, jax.random.fold_in(own_key, 3), *heavy), -reach, reach).astype(held_as)


def setup_inputs(seed: int = 0, part: int = 0) -> dict:
    key_list = jax.random.split(jax.random.key(seed), 13)
    own_keys = jax.random.split(jax.random.fold_in(key_list[12], part), 13)
    return {
        "queries": draw_queries(jax.random.fold_in(jax.random.fold_in(key_list[12], part), 71), part),
        "keys": draw_keys(jax.random.fold_in(jax.random.fold_in(key_list[12], part), 71), part),
        "values": gaussian(own_keys[2], (SEQ, KVH * HD), 1.0, 6.0, ((0, 4),)),
        "sink": jnp.clip(1.0 + 4.0 * jax.random.uniform(key_list[3], (H,), jnp.float32) ** steps_of(key_list[3], (H,), ((0, 4),), -0.2, 0.2), 1.0, 5.0),
        "resid": draw_resid(jax.random.fold_in(jax.random.fold_in(key_list[12], part), 71), part),
        "out_proj": gaussian(key_list[5], (H * HD, D), (H * HD // 64) ** -0.5, 1.5, ((1, 4),)),
        "norm_gain": jnp.clip(1.0 + 0.18 * jax.random.normal(key_list[6], (D,), jnp.float32), 0.1, 1.9),
        "w_gate": gaussian(key_list[7], (D, FF), D ** -0.5, 0.125, ((0, 4), (1, 4))),
        "w_up": gaussian(key_list[8], (D, FF), D ** -0.5, 0.125, ((0, 4), (1, 4))),
        "conv_w": gaussian(key_list[9], (CONV, FF), 0.6, 3.0, ((1, 4),), jnp.float32),
        "conv_b": gaussian(key_list[10], (FF,), 0.5, 3.0, ((0, 4),), jnp.float32),
        "w_down": noise_with(key_list[11], (FF, D), (FF // 4) ** -0.5, 0.21875, ((0, 4), (1, 4)), (0, 1, 4, 2.0)),
    }


def reference(queries, keys, values, sink, resid, out_proj, norm_gain, w_gate, w_up, conv_w, conv_b, w_down):
    group = H // KVH
    scale = HD ** (-0.5)
    span = TOK_DEV + 2 * WINDOW
    q_heads = queries.reshape(SEQ, H, HD)
    k_pad = jnp.pad(keys.reshape(SEQ, KVH, HD), ((WINDOW, WINDOW), (0, 0), (0, 0)))
    v_pad = jnp.pad(values.reshape(SEQ, KVH, HD), ((WINDOW, WINDOW), (0, 0), (0, 0)))
    sink_grid = sink.reshape(KVH, group)[:, :, None]

    def block(index):
        start = (index * TOK_DEV).astype(jnp.int32)
        q_block = lax.dynamic_slice_in_dim(q_heads, start, TOK_DEV, 0).astype(jnp.float32)
        q_block = q_block.reshape(TOK_DEV, KVH, group, HD)
        k_block = lax.dynamic_slice_in_dim(k_pad, start, span, 0).astype(jnp.float32)
        v_block = lax.dynamic_slice_in_dim(v_pad, start, span, 0).astype(jnp.float32)
        scores = jnp.einsum('qhgd,khd->hgqk', q_block, k_block) * scale
        q_pos = start + jnp.arange(TOK_DEV, dtype=jnp.int32)[:, None]
        k_pos = start - WINDOW + jnp.arange(span, dtype=jnp.int32)[None, :]
        valid = (jnp.abs(q_pos - k_pos) <= WINDOW) & (k_pos >= 0) & (k_pos < SEQ)
        scores = jnp.where(valid, scores, jnp.float32(-1e+30))
        top = jnp.maximum(lax.optimization_barrier(jnp.max(scores, axis=-1)), sink_grid)
        expo = jnp.exp(scores - top[..., None])
        total = lax.optimization_barrier(jnp.sum(expo, axis=-1)) + jnp.exp(sink_grid - top)
        weights = (expo / total[..., None]).astype(jnp.bfloat16)
        out = jnp.einsum('hgqk,khd->qhgd', weights.astype(jnp.float32), v_block)
        return out.astype(jnp.bfloat16).reshape(TOK_DEV, H * HD)
    mixed = lax.map(block, jnp.arange(SEQ // TOK_DEV, dtype=jnp.int32)).reshape(SEQ, H * HD)
    summed = resid.astype(jnp.float32) + jnp.dot(mixed, out_proj, preferred_element_type=jnp.float32)
    mean = lax.optimization_barrier(jnp.mean(summed, axis=-1, keepdims=True))
    msq = lax.optimization_barrier(jnp.mean(summed * summed, axis=-1, keepdims=True))
    normed = ((summed - mean) * lax.rsqrt(msq - mean * mean + 1e-05) * norm_gain).astype(jnp.bfloat16)
    gate_pre = jnp.dot(normed, w_gate, preferred_element_type=jnp.float32).astype(jnp.bfloat16)
    up_part = jnp.dot(normed, w_up, preferred_element_type=jnp.float32).astype(jnp.bfloat16)
    padded = jnp.pad(gate_pre.astype(jnp.float32), ((1, 1), (0, 0)))
    conv = conv_b
    for tap in range(CONV):
        conv = conv + padded[tap:tap + SEQ] * conv_w[tap]
    act = (jax.nn.silu(conv) * up_part.astype(jnp.float32)).astype(jnp.bfloat16)
    ffn = jnp.dot(act, w_down, preferred_element_type=jnp.float32)
    return (normed.astype(jnp.float32) + ffn).astype(jnp.bfloat16)
```

```python
import functools

import jax
import jax.numpy as jnp
from jax import lax
from jax.experimental import pallas as pl
from jax.experimental.pallas import tpu as pltpu
from jax.sharding import PartitionSpec as P

H = 8
KVH = 2
HD = 128
WINDOW = 128
CONV = 3


def with_halo(cells, sides, width):
    for axis, dim in sides:
        count = lax.axis_size(axis)
        ends = count - 1
        head = lax.slice_in_dim(cells, 0, width, axis=dim)
        tail = lax.slice_in_dim(cells, cells.shape[dim] - width, cells.shape[dim], axis=dim)
        cells = jnp.concatenate(
            [
                lax.ppermute(tail, axis, [(i, (i + 1) % count) for i in range(ends)]),
                cells,
                lax.ppermute(head, axis, [((i + 1) % count, i) for i in range(ends)]),
            ],
            axis=dim,
        )
    return cells


def shards(
    queries, keys, values, sink, resid, out_proj, norm_gain, w_gate, w_up, conv_w, conv_b, w_down
):
    tokens = queries.shape[0]
    width = resid.shape[1]
    heads_here = sink.shape[0]
    group = H // KVH
    scale = HD ** (-0.5)
    first_head = lax.axis_index("tp") * heads_here
    kv_head = first_head // group
    own_keys = lax.dynamic_slice_in_dim(keys, kv_head * HD, HD, 1)
    own_values = lax.dynamic_slice_in_dim(values, kv_head * HD, HD, 1)
    extended = with_halo(jnp.stack([own_keys, own_values]), (("sp", 1),), WINDOW)
    ext_keys = extended[0]
    ext_values = extended[1]
    span = tokens + 2 * WINDOW
    q_heads = queries.reshape(tokens, heads_here, HD)
    scores = (
        jnp.einsum("qhd,kd->hqk", q_heads, ext_keys, preferred_element_type=jnp.float32) * scale
    )
    offset = lax.axis_index("sp") * tokens
    q_pos = offset + jnp.arange(tokens, dtype=jnp.int32)[:, None]
    k_pos = offset - WINDOW + jnp.arange(span, dtype=jnp.int32)[None, :]
    seq_total = tokens * lax.axis_size("sp")
    valid = (jnp.abs(q_pos - k_pos) <= WINDOW) & (k_pos >= 0) & (k_pos < seq_total)
    scores = jnp.where(valid[None], scores, jnp.float32(-1e30))
    sink_col = sink[:, None]
    top = jnp.maximum(jnp.max(scores, axis=-1), sink_col)
    expo = jnp.exp(scores - top[..., None])
    total = jnp.sum(expo, axis=-1) + jnp.exp(sink_col - top)
    weights = (expo / total[..., None]).astype(jnp.bfloat16)
    heads_out = jnp.einsum("hqk,kd->qhd", weights, ext_values, preferred_element_type=jnp.float32)
    heads_out = heads_out.astype(jnp.bfloat16).reshape(tokens, heads_here * HD)
    all_heads = lax.all_gather(heads_out, "tp", axis=1, tiled=True)
    cols = width // lax.axis_size("tp")
    col_start = lax.axis_index("tp") * cols
    full_proj = lax.all_gather(out_proj, "tp", axis=1, tiled=True)
    summed = resid.astype(jnp.float32) + jnp.dot(
        all_heads, full_proj, preferred_element_type=jnp.float32
    )
    mean = jnp.mean(summed, axis=-1, keepdims=True)
    msq = jnp.mean(summed * summed, axis=-1, keepdims=True)
    normed_full = ((summed - mean) * lax.rsqrt(msq - mean * mean + 1e-05) * norm_gain).astype(
        jnp.bfloat16
    )
    normed_own = lax.dynamic_slice_in_dim(normed_full, col_start, cols, 1)
    gate_acc = jnp.dot(
        normed_full,
        lax.all_gather(w_gate, "sp", axis=0, tiled=True),
        preferred_element_type=jnp.float32,
    )
    up_acc = jnp.dot(
        normed_full,
        lax.all_gather(w_up, "sp", axis=0, tiled=True),
        preferred_element_type=jnp.float32,
    )
    gate_pre = gate_acc.astype(jnp.bfloat16)
    up_part = up_acc.astype(jnp.bfloat16)
    padded = with_halo(gate_pre, (("sp", 0),), CONV // 2)
    conv = conv_b
    for tap in range(CONV):
        conv = conv + padded[tap : tap + tokens].astype(jnp.float32) * conv_w[tap]
    act = (jax.nn.silu(conv) * up_part.astype(jnp.float32)).astype(jnp.bfloat16)
    terms = jnp.dot(
        act, lax.all_gather(w_down, "sp", axis=1, tiled=True), preferred_element_type=jnp.float32
    )
    ffn_own = lax.psum_scatter(
        terms.astype(jnp.bfloat16), "tp", scatter_dimension=1, tiled=True
    ).astype(jnp.float32)
    return (normed_own.astype(jnp.float32) + ffn_own).astype(jnp.bfloat16)


EDGE = 16
SPLIT = 2
BF16 = jnp.bfloat16
F32 = jnp.float32


def layer_kernel(
    sizes,
    q_hbm, k_hbm, v_hbm, sink_ref, resid_hbm, proj_hbm, gain_ref, wg_hbm, wu_hbm, cw_ref, cb_ref, wd_hbm,
    out_ref,
    q_ref, kv_ext, resid_ref, proj_all, mixed, summed, normed, wg_all, wu_all, wd_all, gate, up, act,
    terms, near_in, pair_in, far_in, over_in, ret_out, ret_in,
    local_sem, halo_send, halo_recv, z_send, z_recv, y_send, y_recv,
    proj_send, proj_recv, mix_send, mix_recv, norm_send, norm_recv, edge_send, edge_recv, row_send, row_recv,
    near_send, near_recv, pair_send, pair_recv, far_send, far_recv, over_send, over_recv, ret_send, ret_recv,
):
    groups, n, tps = sizes
    g = lax.axis_index("grp")
    s = lax.axis_index("sp")
    t = lax.axis_index("tp")
    tokens, width = resid_hbm.shape
    heads_here = sink_ref.shape[0]
    cols = proj_hbm.shape[1]
    depth = wg_hbm.shape[0]
    hidden = wg_hbm.shape[1]
    part = hidden // 2
    rows2 = 2 * tokens
    has_left, has_right = s > 0, s < n - 1
    inner = has_left & has_right
    outer = jnp.logical_not(inner)
    low = s < n // 2
    mate = s + 1 - 2 * lax.rem(s, 2)
    mirror = n - 1 - s
    beyond = n - 1 - mate
    role = 1 - jnp.where(inner, 1, 0)
    hidden_at = pl.multiple_of(role * part, 128)
    base = pl.multiple_of(EDGE + lax.rem(s, 2) * tokens, EDGE)
    other_base = pl.multiple_of(EDGE + (1 - lax.rem(s, 2)) * tokens, EDGE)
    core = lax.rem(t, 2)
    core_peer = t + 1 - 2 * core
    chip_peer = lax.rem(t + 2, tps)
    own = (wg_hbm, wu_hbm, wd_hbm)
    full = (wg_all, wu_all, wd_all)
    OWN = n - 1

    def remote(src, dst, send, recv, to):
        return pltpu.make_async_remote_copy(
            src_ref=src, dst_ref=dst, send_sem=send, recv_sem=recv,
            device_id=to, device_id_type=pl.DeviceIdType.MESH,
        )

    kv_head = (t * heads_here) // (H // KVH)
    kv_cols = pl.ds(pl.multiple_of(kv_head * HD, HD), HD)

    def local(i):
        src, dst = (
            (q_hbm, q_ref),
            (k_hbm.at[:, kv_cols], kv_ext.at[0, pl.ds(WINDOW, tokens)]),
            (v_hbm.at[:, kv_cols], kv_ext.at[1, pl.ds(WINDOW, tokens)]),
            (proj_hbm, proj_all.at[t]),
            (resid_hbm, resid_ref),
            (wg_hbm.at[:, pl.ds(hidden_at, part)], wg_all.at[OWN]),
            (wu_hbm.at[:, pl.ds(hidden_at, part)], wu_all.at[OWN]),
            (wd_hbm.at[pl.ds(hidden_at, part)], wd_all.at[OWN]),
        )[i]
        return pltpu.make_async_copy(src, dst, local_sem.at[i])

    for i in range(8):
        local(i).start()

    barrier = pltpu.get_barrier_semaphore()

    def greet(to):
        pl.semaphore_signal(barrier, inc=1, device_id=to, device_id_type=pl.DeviceIdType.MESH)

    for j in range(1, n):
        greet({"sp": lax.rem(s + j, n)})
    for j in range(1, groups):
        greet({"grp": lax.rem(g + j, groups)})
    for j in range(1, tps):
        greet({"tp": lax.rem(t + j, tps)})
    for j in range(2):
        greet({"sp": mate, "tp": lax.rem(t - core + 2 + j, tps)})
    pl.semaphore_wait(barrier, n - 1 + groups - 1 + tps - 1 + 2)

    def halo_copy(i, to_left):
        ref = (k_hbm, v_hbm)[i]
        if to_left:
            return remote(ref.at[pl.ds(0, WINDOW), kv_cols], kv_ext.at[i, pl.ds(WINDOW + tokens, WINDOW)],
                          halo_send.at[i, 0], halo_recv.at[i, 0], {"sp": s - 1})
        return remote(ref.at[pl.ds(tokens - WINDOW, WINDOW), kv_cols], kv_ext.at[i, pl.ds(0, WINDOW)],
                      halo_send.at[i, 1], halo_recv.at[i, 1], {"sp": s + 1})

    def chunk_of(m, of, c):
        if m < 2:
            step = depth // (groups * SPLIT)
            return pl.ds(pl.multiple_of((of * SPLIT + c) * step, EDGE), step)
        step = cols // (groups * SPLIT)
        return pl.ds(pl.multiple_of((c * groups + of) * step, 128), step)

    def source(m, r, c):
        if m < 2:
            return own[m].at[chunk_of(m, g, c), pl.ds(r * part, part)]
        return own[m].at[pl.ds(r * part, part), chunk_of(m, g, c)]

    def place(m, slot, of, c):
        if m < 2:
            return full[m].at[slot, chunk_of(m, of, c)]
        return full[m].at[slot, :, chunk_of(m, of, c)]

    IN_ACROSS, IN_BEYOND, IN_MATE, IN_RELAY, OUT_MATE, OUT_MIRROR = range(6)

    def ship(kind, m, c):
        src, slot, to, lane = {
            IN_ACROSS: (None, 1, mirror, 0),
            IN_BEYOND: (None, 1, beyond, 1),
            IN_MATE: (None, 0, mate, 2),
            IN_RELAY: (0, 2, mirror, 3),
            OUT_MATE: (None, 0, mate, 0),
            OUT_MIRROR: (None, 2, mirror, 1),
        }[kind]
        r = 0 if kind in (IN_ACROSS, OUT_MATE) else 1
        src_ref = source(m, r, c) if src is None else place(m, src, g, c)
        return remote(src_ref, place(m, slot, g, c), z_send.at[m, lane, c], z_recv.at[m, slot, c], {"sp": to})

    def ship_all(kind, m):
        for c in range(SPLIT):
            ship(kind, m, c).start()

    def cross(m, slot, c):
        return remote(place(m, slot, g, c), place(m, slot, g, c), y_send.at[m, slot, c], y_recv.at[m, slot, c],
                      {"grp": 1 - g})

    def cross_arrival(m, slot, c):
        return remote(place(m, slot, 1 - g, c), place(m, slot, 1 - g, c), y_send.at[m, slot, c],
                      y_recv.at[m, slot, c], {"grp": 1 - g})

    def take(m, slot, cs=range(SPLIT)):
        for c in cs:
            remote(place(m, slot, g, c), place(m, slot, g, c), z_send.at[m, 0, c], z_recv.at[m, slot, c],
                   {"sp": mate}).wait_recv()
            cross(m, slot, c).start()
            if slot == 0:
                @pl.when(inner)
                def _():
                    ship(IN_RELAY, m, c).start()

    def have(m, slot, cs=range(SPLIT)):
        for c in cs:
            cross_arrival(m, slot, c).wait_recv()

    def spread(src, ref, send, recv, step):
        origin = (t, t, chip_peer)[step]
        return remote(src if step < 2 else ref.at[origin], ref.at[origin], send.at[step], recv.at[step],
                      {"tp": (core_peer, chip_peer, core_peer)[step]})

    def spread_arrival(src, ref, send, recv, step):
        origin = (core_peer, chip_peer, lax.rem(core_peer + 2, tps))[step]
        return remote(src, ref.at[origin], send.at[step], recv.at[step],
                      {"tp": (core_peer, chip_peer, core_peer)[step]})

    proj_args = (proj_hbm, proj_all, proj_send, proj_recv)
    mix_args = (mixed.at[t], mixed, mix_send, mix_recv)

    @pl.when(has_left)
    def _():
        for i in range(2):
            halo_copy(i, True).start()

    @pl.when(has_right)
    def _():
        for i in range(2):
            halo_copy(i, False).start()

    @pl.when(outer)
    def _():
        for m in range(2):
            ship_all(OUT_MATE, m)
            ship_all(OUT_MIRROR, m)

    @pl.when(inner)
    def _():
        for m in range(2):
            ship_all(IN_ACROSS, m)
            ship_all(IN_BEYOND, m)
            ship_all(IN_MATE, m)

    for step in (1, 0):
        spread(*proj_args, step).start()

    @pl.when(jnp.logical_not(has_left))
    def _():
        kv_ext[:, pl.ds(0, WINDOW), :] = jnp.zeros((2, WINDOW, HD), BF16)

    @pl.when(jnp.logical_not(has_right))
    def _():
        kv_ext[:, pl.ds(WINDOW + tokens, WINDOW), :] = jnp.zeros((2, WINDOW, HD), BF16)

    for i in range(3):
        local(i).wait()

    @pl.when(has_right)
    def _():
        for i in range(2):
            halo_copy(i, True).wait_recv()

    @pl.when(has_left)
    def _():
        for i in range(2):
            halo_copy(i, False).wait_recv()

    span = 3 * WINDOW
    seq_total = tokens * n

    @pl.loop(0, tokens // WINDOW)
    def _(b):
        start = pl.multiple_of(b * WINDOW, WINDOW)
        row = lax.broadcasted_iota(jnp.int32, (WINDOW, span), 0)
        col = lax.broadcasted_iota(jnp.int32, (WINDOW, span), 1)
        k_pos = s * tokens + start - WINDOW + col
        valid = (jnp.abs(row + WINDOW - col) <= WINDOW) & (k_pos >= 0) & (k_pos < seq_total)
        kb = kv_ext[0, pl.ds(start, span), :]
        vb = kv_ext[1, pl.ds(start, span), :]
        for h in range(heads_here):
            qb = q_ref[pl.ds(start, WINDOW), h * HD:(h + 1) * HD]
            sc = lax.dot_general(qb, kb, (((1,), (1,)), ((), ())), preferred_element_type=F32) * (HD ** -0.5)
            sc = jnp.where(valid, sc, F32(-1e30))
            sink = sink_ref[h]
            top = jnp.maximum(jnp.max(sc, axis=-1, keepdims=True), sink)
            expo = jnp.exp(sc - top)
            total = jnp.sum(expo, axis=-1, keepdims=True) + jnp.exp(sink - top)
            weights = (expo / total).astype(BF16)
            o = jnp.dot(weights, vb, preferred_element_type=F32)
            mixed[t, pl.ds(start, WINDOW), h * HD:(h + 1) * HD] = o.astype(BF16)

    for step in (1, 0):
        spread(*mix_args, step).start()

    take(0, 0)

    @pl.when(inner)
    def _():
        take(0, 1)

    for args in (proj_args, mix_args):
        spread_arrival(*args, 1).wait_recv()
        spread(*args, 2).start()
    for args in (proj_args, mix_args):
        for step in (0, 2):
            spread_arrival(*args, step).wait_recv()

    @pl.when(inner)
    def _():
        take(1, 0)

    for i in (3, 4):
        local(i).wait()
    lanes = mixed.shape[2]
    block = summed.shape[0]
    strip = 64

    @pl.loop(0, tokens // block)
    def _(b):
        rows = pl.ds(pl.multiple_of(b * block, block), block)

        @pl.loop(0, tps)
        def _(i):
            at = pl.ds(pl.multiple_of(i * cols, 128), cols)
            prod = jnp.dot(mixed[0, rows, :], proj_all[i, pl.ds(0, lanes), :], preferred_element_type=F32)
            for u in range(1, tps):
                prod += jnp.dot(mixed[u, rows, :], proj_all[i, pl.ds(u * lanes, lanes), :],
                                preferred_element_type=F32)
            summed[:, at] = resid_ref[rows, at].astype(F32) + prod

        @pl.loop(0, block // strip)
        def _(i):
            at = pl.multiple_of(i * strip, strip)
            x = summed[pl.ds(at, strip), :]
            mean = jnp.mean(x, axis=-1, keepdims=True)
            msq = jnp.mean(x * x, axis=-1, keepdims=True)
            normed[pl.ds(pl.multiple_of(base + b * block + at, EDGE), strip), :] = (
                (x - mean) * lax.rsqrt(msq - mean * mean + 1e-05) * gain_ref[...]
            ).astype(BF16)

    my_cols = pl.ds(pl.multiple_of(t * cols, 128), cols)

    def norm_part(first, col):
        return normed.at[pl.ds(first, tokens), pl.ds(pl.multiple_of(col * cols, 128), cols)]

    def norm_copy(i, arrival=False):
        first = base if i == 0 and not arrival else other_base
        col = (t, t, t, chip_peer)[i] if not arrival else (t, chip_peer, core_peer, lax.rem(core_peer + 2, tps))[i]
        to = ({"sp": mate}, {"tp": chip_peer}, {"tp": core_peer}, {"tp": core_peer})[i]
        ref = norm_part(first, col)
        return remote(ref, ref, norm_send.at[i], norm_recv.at[i], to)

    edge_from = pl.ds(pl.multiple_of(base + jnp.where(low, tokens - EDGE, 0), EDGE), EDGE)
    edge_over = pl.ds(pl.multiple_of(jnp.where(low, 0, EDGE + rows2), EDGE), EDGE)
    edge_here = pl.ds(pl.multiple_of(jnp.where(low, EDGE + rows2, 0), EDGE), EDGE)

    def edge_copy(i):
        return remote(normed.at[edge_from, my_cols], normed.at[edge_over, my_cols], edge_send.at[i],
                      edge_recv.at[0], {"sp": (mirror, beyond)[i]})

    def edge_arrival():
        ref = normed.at[edge_here, my_cols]
        return remote(ref, ref, edge_send.at[0], edge_recv.at[0], {"sp": mirror})

    def row_copy(j, arrival=False):
        col = lax.rem(t + tps - j, tps) if arrival else t
        ref = normed.at[edge_here, pl.ds(pl.multiple_of(col * cols, 128), cols)]
        return remote(ref, ref, row_send.at[j - 1], row_recv.at[j - 1], {"tp": lax.rem(t + j, tps)})

    tile = 256

    def source_of(slot):
        return (mate, jnp.where(low, n // 2, n // 2 - 1), jnp.where(low, n - 1, 0), s)[slot]

    with_edge = pl.ds(pl.multiple_of(jnp.where(low, EDGE, 0), EDGE), rows2 + EDGE)
    both = pl.ds(EDGE, rows2)

    def gate_up(slot):
        if slot != OWN:
            have(0, slot)
            have(1, slot)
        k = pl.ds(pl.multiple_of(source_of(slot) * depth, 128), depth)

        @pl.loop(0, part // tile)
        def _(i):
            at = pl.ds(pl.multiple_of(i * tile, 128), tile)
            ga = jnp.dot(normed[with_edge, k], wg_all[slot, :, at], preferred_element_type=F32)
            if slot == OWN:
                gate[with_edge, at] = ga
            else:
                gate[with_edge, at] += ga
            ub = jnp.dot(normed[both, k], wu_all[slot, :, at], preferred_element_type=F32)
            if slot == OWN:
                up[:, at] = ub
            else:
                up[:, at] += ub

    @pl.when(inner)
    def _():
        for i in range(2):
            edge_copy(i).start()

    norm_copy(0).start()

    @pl.when(outer)
    def _():
        ship_all(OUT_MATE, 2)
        take(0, 1)
        take(1, 0)

    @pl.when(inner)
    def _():
        ship_all(IN_MATE, 2)
        ship_all(IN_BEYOND, 2)
        ship_all(IN_ACROSS, 2)

    for i in (5, 6, 7):
        local(i).wait()

    take(1, 1)
    norm_copy(0, True).wait_recv()
    norm_copy(1).start()
    norm_copy(2).start()
    take(0, 2)

    @pl.when(inner)
    def _():
        take(2, 0)

    norm_copy(1, True).wait_recv()
    norm_copy(3).start()

    @pl.when(outer)
    def _():
        ship_all(OUT_MIRROR, 2)

    edge_arrival().wait_recv()
    for j in range(1, tps):
        row_copy(j).start()
    norm_copy(2, True).wait_recv()
    norm_copy(3, True).wait_recv()
    for j in range(1, tps):
        row_copy(j, True).wait_recv()
    gate_up(OWN)
    gate_up(0)
    gate_up(1)
    take(1, 2)

    @pl.when(outer)
    def _():
        take(2, 0)

    gate_up(2)

    @pl.when(low)
    def _():
        gate[0:EDGE, :] = jnp.zeros((EDGE, part), F32)

    @pl.when(jnp.logical_not(low))
    def _():
        gate[EDGE + rows2:, :] = jnp.zeros((EDGE, part), F32)

    @pl.loop(0, part // 128)
    def _(i):
        at = pl.ds(pl.multiple_of(i * 128, 128), 128)
        ch = pl.ds(pl.multiple_of(hidden_at + i * 128, 128), 128)
        gate[:, at] = gate[:, at].astype(BF16).astype(F32)
        conv = cb_ref[:, ch]
        for tap in range(CONV):
            conv = conv + gate[pl.ds(EDGE - CONV // 2 + tap, rows2), at] * cw_ref[tap:tap + 1, ch]
        silu = conv / (1.0 + jnp.exp(-conv))
        act[:, at] = (silu * up[:, at].astype(BF16).astype(F32)).astype(BF16)

    half_rows = tokens // 2
    wide = cols // SPLIT
    far_first = (1 - t // 2) * 2

    def is_far(p):
        return (p // 2) != (t // 2)

    def rows_of(i):
        return pl.ds(pl.multiple_of((base if i else other_base) - EDGE, tokens), tokens)

    def half_of(i, c):
        first = (base if i else other_base) - EDGE + c * half_rows
        return pl.ds(pl.multiple_of(first, half_rows), half_rows)

    def half_rows_of(c):
        return pl.ds(pl.multiple_of(c * half_rows, half_rows), half_rows)

    def block_of(c):
        return pl.ds(c * wide, wide)

    def near_copy(i, c):
        return remote(terms.at[core_peer, rows_of(i), block_of(c)], near_in.at[i, :, block_of(c)],
                      near_send.at[i, c], near_recv.at[i, c], {"tp": core_peer})

    def pair_copy(p, i, c):
        q = lax.rem(p, 2)
        return remote(terms.at[p, half_of(i, 1 - core), block_of(c)], pair_in.at[q, i, :, block_of(c)],
                      pair_send.at[q, i, c], pair_recv.at[q, i, c], {"tp": core_peer})

    def far_copy(p, i, c):
        q = lax.rem(p, 2)
        src = terms.at[p, half_of(i, core), block_of(c)]
        if i:
            return remote(src, far_in.at[half_rows_of(core), block_of(c)], far_send.at[q, i, c],
                          far_recv.at[core, c], {"tp": p})
        return remote(src, over_in.at[half_rows_of(core), block_of(c)], far_send.at[q, i, c],
                      over_recv.at[core, c], {"sp": mate, "tp": p})

    def far_arrival(h, c):
        ref = far_in.at[half_rows_of(h), block_of(c)]
        return remote(ref, ref, over_send.at[h, c], far_recv.at[h, c], {"tp": far_first + h})

    def over_arrival(h, c):
        ref = over_in.at[half_rows_of(h), block_of(c)]
        return remote(ref, ref, over_send.at[h, c], over_recv.at[h, c], {"sp": mate, "tp": far_first + h})

    def ret_copy(c):
        return remote(ret_out.at[:, block_of(c)], ret_in.at[:, block_of(c)], ret_send.at[c], ret_recv.at[c],
                      {"sp": mate})

    def down(slot, c, i):
        p = source_of(slot)
        w = wd_all[slot, :, block_of(c)]
        terms[p, rows_of(i), block_of(c)] = jnp.dot(act[rows_of(i), :], w, preferred_element_type=F32).astype(BF16)

        @pl.when(p == core_peer)
        def _():
            near_copy(i, c).start()

        @pl.when(is_far(p))
        def _():
            pair_copy(p, i, c).start()

    def settle(slot, c, i):
        p = source_of(slot)

        @pl.when(is_far(p))
        def _():
            pair_copy(p, i, c).wait_recv()
            rows = half_of(i, core)
            both = (terms[p, rows, block_of(c)].astype(F32)
                    + pair_in[lax.rem(p, 2), i, :, block_of(c)].astype(F32))
            terms[p, rows, block_of(c)] = both.astype(BF16)
            far_copy(p, i, c).start()

        if i == 0:
            @pl.when(p == t)
            def _():
                near_copy(0, c).wait_recv()
                ret_out[:, block_of(c)] = (terms[t, rows_of(0), block_of(c)].astype(F32)
                                           + near_in[0, :, block_of(c)].astype(F32)).astype(BF16)
                ret_copy(c).start()

    def finish(c):
        near_copy(1, c).wait_recv()
        at = pl.ds(pl.multiple_of(t * cols + c * wide, 128), wide)
        out = normed[pl.ds(base, tokens), at].astype(F32) + terms[t, rows_of(1), block_of(c)].astype(F32)
        out = out + near_in[1, :, block_of(c)].astype(F32)
        for h in range(2):
            far_arrival(h, c).wait_recv()
        out = out + far_in[:, block_of(c)].astype(F32)
        ret_copy(c).wait_recv()
        out = out + ret_in[:, block_of(c)].astype(F32)
        for h in range(2):
            over_arrival(h, c).wait_recv()
        out = out + over_in[:, block_of(c)].astype(F32)
        out_ref[:, block_of(c)] = out.astype(BF16)

    def downs(slot, c):
        for i in range(2):
            down(slot, c, i)

    def settles(slot, c):
        for i in range(2):
            settle(slot, c, i)

    early = [(slot, c) for slot in (OWN, 0) for c in range(SPLIT)]
    late = [(slot, c) for slot in (1, 2) for c in range(SPLIT)]
    for at, (slot, c) in enumerate(early):
        if slot != OWN:
            have(2, slot, (c,))
        downs(slot, c)
        if at:
            settles(*early[at - 1])
    take(2, late[0][0], (late[0][1],))
    settles(*early[-1])
    for at, (slot, c) in enumerate(late):
        if at + 1 < len(late):
            take(2, late[at + 1][0], (late[at + 1][1],))
        have(2, slot, (c,))
        downs(slot, c)
        settles(slot, c)
    for c in range(SPLIT):
        finish(c)

    @pl.when(inner)
    def _():
        for kind in (IN_ACROSS, IN_BEYOND, IN_MATE, IN_RELAY):
            for m in range(3):
                for c in range(SPLIT):
                    ship(kind, m, c).wait_send()

    @pl.when(outer)
    def _():
        for kind in (OUT_MATE, OUT_MIRROR):
            for m in range(3):
                for c in range(SPLIT):
                    ship(kind, m, c).wait_send()

    for m in range(3):
        for slot in range(n - 1):
            for c in range(SPLIT):
                cross(m, slot, c).wait_send()
    for i in range(4):
        norm_copy(i).wait_send()
    for j in range(1, tps):
        row_copy(j).wait_send()

    @pl.when(inner)
    def _():
        for i in range(2):
            edge_copy(i).wait_send()

    for c in range(SPLIT):
        ret_copy(c).wait_send()
        for i in range(2):
            near_copy(i, c).wait_send()
            for h in range(2):
                pair_copy(far_first + h, i, c).wait_send()
                far_copy(far_first + h, i, c).wait_send()

    @pl.when(has_left)
    def _():
        for i in range(2):
            halo_copy(i, True).wait_send()

    @pl.when(has_right)
    def _():
        for i in range(2):
            halo_copy(i, False).wait_send()

    for step in range(3):
        spread(*proj_args, step).wait_send()
        spread(*mix_args, step).wait_send()


def kernel_shards(
    sizes, queries, keys, values, sink, resid, out_proj, norm_gain, w_gate, w_up, conv_w, conv_b, w_down
):
    groups, n, tps = sizes
    tokens, width = resid.shape
    cols = out_proj.shape[1]
    depth, hidden = w_gate.shape
    part = hidden // 2
    vmem = pl.BlockSpec(memory_space=pltpu.VMEM)
    hbm = pl.BlockSpec(memory_space=pl.ANY)
    smem = pl.BlockSpec(memory_space=pltpu.SMEM)
    dma = pltpu.SemaphoreType.DMA
    block = (tokens, cols)
    return pl.pallas_call(
        functools.partial(layer_kernel, sizes),
        out_shape=jax.ShapeDtypeStruct((tokens, cols), BF16),
        in_specs=[hbm] * 3 + [smem, hbm, hbm, vmem, hbm, hbm, vmem, vmem, hbm],
        out_specs=vmem,
        scratch_shapes=[
            pltpu.VMEM(queries.shape, BF16),
            pltpu.VMEM((2, tokens + 2 * WINDOW, HD), BF16),
            pltpu.VMEM(resid.shape, BF16),
            pltpu.VMEM((tps,) + out_proj.shape, BF16),
            pltpu.VMEM((tps,) + queries.shape, BF16),
            pltpu.VMEM((tokens // 2, width), F32),
            pltpu.VMEM((2 * tokens + 2 * EDGE, width), BF16),
            pltpu.VMEM((n, depth, part), BF16),
            pltpu.VMEM((n, depth, part), BF16),
            pltpu.VMEM((n, part, cols), BF16),
            pltpu.VMEM((2 * tokens + 2 * EDGE, part), F32),
            pltpu.VMEM((2 * tokens, part), F32),
            pltpu.VMEM((2 * tokens, part), BF16),
            pltpu.VMEM((tps, 2 * tokens, cols), BF16),
            pltpu.VMEM((2,) + block, BF16),
            pltpu.VMEM((2, 2, tokens // 2, cols), BF16),
            pltpu.VMEM(block, BF16),
            pltpu.VMEM(block, BF16),
            pltpu.VMEM(block, BF16),
            pltpu.VMEM(block, BF16),
            dma((8,)), dma((2, 2)), dma((2, 2)),
            dma((3, 4, SPLIT)), dma((3, 3, SPLIT)), dma((3, 3, SPLIT)), dma((3, 3, SPLIT)),
            dma((3,)), dma((3,)), dma((3,)), dma((3,)), dma((4,)), dma((4,)), dma((2,)), dma((1,)),
            dma((3,)), dma((3,)),
            dma((2, SPLIT)), dma((2, SPLIT)), dma((2, 2, SPLIT)), dma((2, 2, SPLIT)),
            dma((2, 2, SPLIT)), dma((2, SPLIT)), dma((2, SPLIT)), dma((2, SPLIT)), dma((SPLIT,)), dma((SPLIT,)),
        ],
        compiler_params=pltpu.CompilerParams(
            collective_id=0, has_side_effects=True, vmem_limit_bytes=67043328
        ),
    )(queries, keys, values, sink, resid, out_proj, norm_gain[None], w_gate, w_up, conv_w, conv_b[None], w_down)


def fits_kernel(sizes, args):
    groups, n, tps = sizes
    queries, resid, out_proj, w_gate, w_down = args[0], args[4], args[5], args[7], args[11]
    share = groups * SPLIT
    weights = 3 * 2 * n * w_gate.shape[0] * w_gate.shape[1]
    return (
        n == 4
        and tps == 4
        and groups == 2
        and w_down.shape[1] == out_proj.shape[1]
        and w_gate.shape[0] % max(share * EDGE, 128) == 0
        and w_down.shape[1] % (share * 128) == 0
        and w_gate.shape[1] % 512 == 0
        and resid.shape[0] % (4 * WINDOW) == 0
        and weights <= 20 * 2 ** 20
    )


def run_shards(sizes, *args):
    if fits_kernel(sizes, args):
        return kernel_shards(sizes, *args)
    return shards(*args)


def solution(mesh):
    sizes = tuple(mesh.shape[axis] for axis in ("grp", "sp", "tp"))
    return jax.shard_map(
        functools.partial(run_shards, sizes),
        mesh=mesh,
        in_specs=(
            P(("grp", "sp"), "tp"),
            P(("grp", "sp"), None),
            P(("grp", "sp"), None),
            P("tp"),
            P(("grp", "sp"), None),
            P(None, "tp"),
            P(),
            P("sp", "tp"),
            P("sp", "tp"),
            P(None, "tp"),
            P("tp"),
            P("tp", "sp"),
        ),
        out_specs=P(("grp", "sp"), "tp"),
        check_vma=False,
    )
```

```python
import functools

import jax
import jax.numpy as jnp
from jax import lax
from jax.experimental import pallas as pl
from jax.experimental.pallas import tpu as pltpu
from jax.sharding import PartitionSpec as P

H = 8
KVH = 2
HD = 128
WINDOW = 128
CONV = 3


def with_halo(cells, sides, width):
    for axis, dim in sides:
        count = lax.axis_size(axis)
        ends = count - 1
        head = lax.slice_in_dim(cells, 0, width, axis=dim)
        tail = lax.slice_in_dim(cells, cells.shape[dim] - width, cells.shape[dim], axis=dim)
        cells = jnp.concatenate(
            [
                lax.ppermute(tail, axis, [(i, (i + 1) % count) for i in range(ends)]),
                cells,
                lax.ppermute(head, axis, [((i + 1) % count, i) for i in range(ends)]),
            ],
            axis=dim,
        )
    return cells


def shards(
    queries, keys, values, sink, resid, out_proj, norm_gain, w_gate, w_up, conv_w, conv_b, w_down
):
    tokens = queries.shape[0]
    width = resid.shape[1]
    heads_here = sink.shape[0]
    group = H // KVH
    scale = HD ** (-0.5)
    first_head = lax.axis_index("tp") * heads_here
    kv_head = first_head // group
    own_keys = lax.dynamic_slice_in_dim(keys, kv_head * HD, HD, 1)
    own_values = lax.dynamic_slice_in_dim(values, kv_head * HD, HD, 1)
    extended = with_halo(jnp.stack([own_keys, own_values]), (("sp", 1),), WINDOW)
    ext_keys = extended[0]
    ext_values = extended[1]
    span = tokens + 2 * WINDOW
    q_heads = queries.reshape(tokens, heads_here, HD)
    scores = (
        jnp.einsum("qhd,kd->hqk", q_heads, ext_keys, preferred_element_type=jnp.float32) * scale
    )
    offset = lax.axis_index("sp") * tokens
    q_pos = offset + jnp.arange(tokens, dtype=jnp.int32)[:, None]
    k_pos = offset - WINDOW + jnp.arange(span, dtype=jnp.int32)[None, :]
    seq_total = tokens * lax.axis_size("sp")
    valid = (jnp.abs(q_pos - k_pos) <= WINDOW) & (k_pos >= 0) & (k_pos < seq_total)
    scores = jnp.where(valid[None], scores, jnp.float32(-1e30))
    sink_col = sink[:, None]
    top = jnp.maximum(jnp.max(scores, axis=-1), sink_col)
    expo = jnp.exp(scores - top[..., None])
    total = jnp.sum(expo, axis=-1) + jnp.exp(sink_col - top)
    weights = (expo / total[..., None]).astype(jnp.bfloat16)
    heads_out = jnp.einsum("hqk,kd->qhd", weights, ext_values, preferred_element_type=jnp.float32)
    heads_out = heads_out.astype(jnp.bfloat16).reshape(tokens, heads_here * HD)
    all_heads = lax.all_gather(heads_out, "tp", axis=1, tiled=True)
    cols = width // lax.axis_size("tp")
    col_start = lax.axis_index("tp") * cols
    full_proj = lax.all_gather(out_proj, "tp", axis=1, tiled=True)
    summed = resid.astype(jnp.float32) + jnp.dot(
        all_heads, full_proj, preferred_element_type=jnp.float32
    )
    mean = jnp.mean(summed, axis=-1, keepdims=True)
    msq = jnp.mean(summed * summed, axis=-1, keepdims=True)
    normed_full = ((summed - mean) * lax.rsqrt(msq - mean * mean + 1e-05) * norm_gain).astype(
        jnp.bfloat16
    )
    normed_own = lax.dynamic_slice_in_dim(normed_full, col_start, cols, 1)
    gate_acc = jnp.dot(
        normed_full,
        lax.all_gather(w_gate, "sp", axis=0, tiled=True),
        preferred_element_type=jnp.float32,
    )
    up_acc = jnp.dot(
        normed_full,
        lax.all_gather(w_up, "sp", axis=0, tiled=True),
        preferred_element_type=jnp.float32,
    )
    gate_pre = gate_acc.astype(jnp.bfloat16)
    up_part = up_acc.astype(jnp.bfloat16)
    padded = with_halo(gate_pre, (("sp", 0),), CONV // 2)
    conv = conv_b
    for tap in range(CONV):
        conv = conv + padded[tap : tap + tokens].astype(jnp.float32) * conv_w[tap]
    act = (jax.nn.silu(conv) * up_part.astype(jnp.float32)).astype(jnp.bfloat16)
    terms = jnp.dot(
        act, lax.all_gather(w_down, "sp", axis=1, tiled=True), preferred_element_type=jnp.float32
    )
    ffn_own = lax.psum_scatter(
        terms.astype(jnp.bfloat16), "tp", scatter_dimension=1, tiled=True
    ).astype(jnp.float32)
    return (normed_own.astype(jnp.float32) + ffn_own).astype(jnp.bfloat16)


EDGE = 16
SPLIT = 2
BF16 = jnp.bfloat16
F32 = jnp.float32


def parts_of(hidden):
    return hidden * 2 // 3, hidden // 3


def layer_kernel(
    sizes,
    q_hbm, k_hbm, v_hbm, sink_ref, resid_hbm, proj_hbm, gain_ref, wg_hbm, wu_hbm, cw_ref, cb_ref, wd_hbm,
    out_ref,
    q_ref, kv_ext, resid_ref, proj_all, mixed, summed, normed, wg_all, wu_all, wd_all, gate, up, act,
    terms, near_in, pair_in, far_in, mid_in, ret_out, ret_in,
    local_sem, halo_send, halo_recv, z_send, z_recv, y_send, y_recv,
    proj_send, proj_recv, mix_send, mix_recv, norm_send, norm_recv, edge_send, edge_recv, row_send, row_recv,
    near_send, near_recv, pair_send, pair_recv, far_send, far_recv, mid_send, mid_recv, ret_send, ret_recv,
):
    groups, n, tps = sizes
    g = lax.axis_index("grp")
    s = lax.axis_index("sp")
    t = lax.axis_index("tp")
    tokens, width = resid_hbm.shape
    heads_here = sink_ref.shape[0]
    cols = proj_hbm.shape[1]
    depth = wg_hbm.shape[0]
    hidden = wg_hbm.shape[1]
    parts = parts_of(hidden)
    starts = (0, parts[0])
    rows2 = 2 * tokens
    has_left, has_right = s > 0, s < n - 1
    inner = has_left & has_right
    outer = jnp.logical_not(inner)
    low = s < n // 2
    mate = s + 1 - 2 * lax.rem(s, 2)
    mirror = n - 1 - s
    beyond = n - 1 - mate
    role = 1 - jnp.where(inner, 1, 0)
    hidden_at = pl.multiple_of(role * parts[0], 128)
    my_part = jnp.where(inner, parts[0], parts[1])
    base = pl.multiple_of(EDGE + lax.rem(s, 2) * tokens, EDGE)
    other_base = pl.multiple_of(EDGE + (1 - lax.rem(s, 2)) * tokens, EDGE)
    core = lax.rem(t, 2)
    core_peer = t + 1 - 2 * core
    chip_peer = lax.rem(t + 2, tps)
    own = (wg_hbm, wu_hbm, wd_hbm)
    full = (wg_all, wu_all, wd_all)
    OWN = n - 1

    def remote(src, dst, send, recv, to):
        return pltpu.make_async_remote_copy(
            src_ref=src, dst_ref=dst, send_sem=send, recv_sem=recv,
            device_id=to, device_id_type=pl.DeviceIdType.MESH,
        )

    kv_head = (t * heads_here) // (H // KVH)
    kv_cols = pl.ds(pl.multiple_of(kv_head * HD, HD), HD)

    def by_role(fn):
        for r, here in enumerate((inner, outer)):
            @pl.when(here)
            def _():
                fn(r)

    def local(i, r=0):
        here, mine = pl.ds(starts[r], parts[r]), pl.ds(0, parts[r])
        src, dst = (
            (q_hbm, q_ref),
            (k_hbm.at[:, kv_cols], kv_ext.at[0, pl.ds(WINDOW, tokens)]),
            (v_hbm.at[:, kv_cols], kv_ext.at[1, pl.ds(WINDOW, tokens)]),
            (proj_hbm, proj_all.at[t]),
            (resid_hbm, resid_ref),
            (wg_hbm.at[:, here], wg_all.at[OWN, :, mine]),
            (wu_hbm.at[:, here], wu_all.at[OWN, :, mine]),
            (wd_hbm.at[here], wd_all.at[OWN, mine]),
        )[i]
        return pltpu.make_async_copy(src, dst, local_sem.at[i])

    for i in range(5):
        local(i).start()
    by_role(lambda r: [local(i, r).start() for i in (5, 6, 7)])

    barrier = pltpu.get_barrier_semaphore()

    def greet(to):
        pl.semaphore_signal(barrier, inc=1, device_id=to, device_id_type=pl.DeviceIdType.MESH)

    for j in range(1, n):
        greet({"sp": lax.rem(s + j, n)})
    for j in range(1, groups):
        greet({"grp": lax.rem(g + j, groups)})
    for j in range(1, tps):
        greet({"tp": lax.rem(t + j, tps)})
    pl.semaphore_wait(barrier, n - 1 + groups - 1 + tps - 1)

    def halo_copy(i, to_left):
        ref = (k_hbm, v_hbm)[i]
        if to_left:
            return remote(ref.at[pl.ds(0, WINDOW), kv_cols], kv_ext.at[i, pl.ds(WINDOW + tokens, WINDOW)],
                          halo_send.at[i, 0], halo_recv.at[i, 0], {"sp": s - 1})
        return remote(ref.at[pl.ds(tokens - WINDOW, WINDOW), kv_cols], kv_ext.at[i, pl.ds(0, WINDOW)],
                      halo_send.at[i, 1], halo_recv.at[i, 1], {"sp": s + 1})

    def chunk_of(m, of, c):
        if m < 2:
            step = depth // (groups * SPLIT)
            return pl.ds(pl.multiple_of((of * SPLIT + c) * step, EDGE), step)
        step = cols // (groups * SPLIT)
        return pl.ds(pl.multiple_of((c * groups + of) * step, 128), step)

    def source(m, r, of, c):
        if m < 2:
            return own[m].at[chunk_of(m, of, c), pl.ds(starts[r], parts[r])]
        return own[m].at[pl.ds(starts[r], parts[r]), chunk_of(m, of, c)]

    def place(m, slot, r, of, c):
        if m < 2:
            return full[m].at[slot, chunk_of(m, of, c), pl.ds(0, parts[r])]
        return full[m].at[slot, pl.ds(0, parts[r]), chunk_of(m, of, c)]

    IN_ACROSS, IN_BEYOND, IN_MATE, IN_RELAY, OUT_MATE, OUT_MIRROR, OUT_REST = range(7)

    def ship(kind, m, c):
        slot, to, lane = {
            IN_ACROSS: (1, mirror, 0),
            IN_BEYOND: (1, beyond, 1),
            IN_MATE: (0, mate, 2),
            IN_RELAY: (2, mirror, 3),
            OUT_MATE: (0, mate, 0),
            OUT_MIRROR: (2, mirror, 1),
            OUT_REST: (0, mate, 2),
        }[kind]
        r = 0 if kind in (IN_ACROSS, IN_RELAY, OUT_MATE, OUT_REST) else 1
        of = 1 - g if kind == OUT_REST else g
        src = place(m, 0, r, of, c) if kind == IN_RELAY else source(m, r, of, c)
        arrive = y_recv.at[m, slot, c] if kind == OUT_REST else z_recv.at[m, slot, c]
        return remote(src, place(m, slot, r, of, c), z_send.at[m, lane, c], arrive, {"sp": to})

    def ship_all(kind, m):
        for c in range(SPLIT):
            ship(kind, m, c).start()

    def direct(m, slot, r):
        return r == 0 and m == 2 and isinstance(slot, int) and slot == 0

    def cross(m, slot, r, c):
        return remote(place(m, slot, r, g, c), place(m, slot, r, g, c), y_send.at[m, slot, c], y_recv.at[m, slot, c],
                      {"grp": 1 - g})

    def take(m, slot, cs=range(SPLIT)):
        def run(r):
            for c in cs:
                remote(place(m, slot, r, g, c), place(m, slot, r, g, c), z_send.at[m, 0, c], z_recv.at[m, slot, c],
                       {"sp": mate}).wait_recv()
                if not direct(m, slot, r):
                    cross(m, slot, r, c).start()
                if isinstance(slot, int) and slot == 0 and r == 0:
                    ship(IN_RELAY, m, c).start()

        by_role(run)

    def have(m, slot, cs=range(SPLIT)):
        def run(r):
            for c in cs:
                ref = place(m, slot, r, 1 - g, c)
                remote(ref, ref, y_send.at[m, slot, c], y_recv.at[m, slot, c], {"grp": 1 - g}).wait_recv()

        by_role(run)

    def spread(src, ref, send, recv, step):
        origin = (t, t, chip_peer)[step]
        return remote(src if step < 2 else ref.at[origin], ref.at[origin], send.at[step], recv.at[step],
                      {"tp": (core_peer, chip_peer, core_peer)[step]})

    def spread_arrival(src, ref, send, recv, step):
        origin = (core_peer, chip_peer, lax.rem(core_peer + 2, tps))[step]
        return remote(src, ref.at[origin], send.at[step], recv.at[step],
                      {"tp": (core_peer, chip_peer, core_peer)[step]})

    proj_args = (proj_hbm, proj_all, proj_send, proj_recv)
    mix_args = (mixed.at[t], mixed, mix_send, mix_recv)

    @pl.when(has_left)
    def _():
        for i in range(2):
            halo_copy(i, True).start()

    @pl.when(has_right)
    def _():
        for i in range(2):
            halo_copy(i, False).start()

    @pl.when(outer)
    def _():
        ship_all(OUT_MATE, 0)
        ship_all(OUT_MATE, 1)
        ship_all(OUT_MIRROR, 0)

    @pl.when(inner)
    def _():
        ship_all(IN_ACROSS, 0)
        ship_all(IN_BEYOND, 0)
        ship_all(IN_MATE, 0)
        ship_all(IN_MATE, 1)

    for step in (1, 0):
        spread(*proj_args, step).start()

    @pl.when(jnp.logical_not(has_left))
    def _():
        kv_ext[:, pl.ds(0, WINDOW), :] = jnp.zeros((2, WINDOW, HD), BF16)

    @pl.when(jnp.logical_not(has_right))
    def _():
        kv_ext[:, pl.ds(WINDOW + tokens, WINDOW), :] = jnp.zeros((2, WINDOW, HD), BF16)

    for i in range(3):
        local(i).wait()

    @pl.when(has_right)
    def _():
        for i in range(2):
            halo_copy(i, True).wait_recv()

    @pl.when(has_left)
    def _():
        for i in range(2):
            halo_copy(i, False).wait_recv()

    span = 3 * WINDOW
    seq_total = tokens * n

    @pl.loop(0, tokens // WINDOW)
    def _(b):
        start = pl.multiple_of(b * WINDOW, WINDOW)
        row = lax.broadcasted_iota(jnp.int32, (WINDOW, span), 0)
        col = lax.broadcasted_iota(jnp.int32, (WINDOW, span), 1)
        k_pos = s * tokens + start - WINDOW + col
        valid = (jnp.abs(row + WINDOW - col) <= WINDOW) & (k_pos >= 0) & (k_pos < seq_total)
        kb = kv_ext[0, pl.ds(start, span), :]
        vb = kv_ext[1, pl.ds(start, span), :]
        for h in range(heads_here):
            qb = q_ref[pl.ds(start, WINDOW), h * HD:(h + 1) * HD]
            sc = lax.dot_general(qb, kb, (((1,), (1,)), ((), ())), preferred_element_type=F32) * (HD ** -0.5)
            sc = jnp.where(valid, sc, F32(-1e30))
            sink = sink_ref[h]
            top = jnp.maximum(jnp.max(sc, axis=-1, keepdims=True), sink)
            expo = jnp.exp(sc - top)
            total = jnp.sum(expo, axis=-1, keepdims=True) + jnp.exp(sink - top)
            weights = (expo / total).astype(BF16)
            o = jnp.dot(weights, vb, preferred_element_type=F32)
            mixed[t, pl.ds(start, WINDOW), h * HD:(h + 1) * HD] = o.astype(BF16)

    for step in (1, 0):
        spread(*mix_args, step).start()

    take(0, 0)

    @pl.when(inner)
    def _():
        take(0, 1)

    for args in (proj_args, mix_args):
        spread_arrival(*args, 1).wait_recv()
        spread(*args, 2).start()
    for args in (proj_args, mix_args):
        for step in (0, 2):
            spread_arrival(*args, step).wait_recv()

    @pl.when(inner)
    def _():
        take(1, 0)

    for i in (3, 4):
        local(i).wait()
    lanes = mixed.shape[2]
    block = summed.shape[0]
    strip = 64

    @pl.loop(0, tokens // block)
    def _(b):
        rows = pl.ds(pl.multiple_of(b * block, block), block)

        @pl.loop(0, tps)
        def _(i):
            at = pl.ds(pl.multiple_of(i * cols, 128), cols)
            prod = jnp.dot(mixed[0, rows, :], proj_all[i, pl.ds(0, lanes), :], preferred_element_type=F32)
            for u in range(1, tps):
                prod += jnp.dot(mixed[u, rows, :], proj_all[i, pl.ds(u * lanes, lanes), :],
                                preferred_element_type=F32)
            summed[:, at] = resid_ref[rows, at].astype(F32) + prod

        @pl.loop(0, block // strip)
        def _(i):
            at = pl.multiple_of(i * strip, strip)
            x = summed[pl.ds(at, strip), :]
            mean = jnp.mean(x, axis=-1, keepdims=True)
            msq = jnp.mean(x * x, axis=-1, keepdims=True)
            normed[pl.ds(pl.multiple_of(base + b * block + at, EDGE), strip), :] = (
                (x - mean) * lax.rsqrt(msq - mean * mean + 1e-05) * gain_ref[...]
            ).astype(BF16)

    my_cols = pl.ds(pl.multiple_of(t * cols, 128), cols)

    def norm_part(first, col):
        return normed.at[pl.ds(first, tokens), pl.ds(pl.multiple_of(col * cols, 128), cols)]

    def norm_copy(i, arrival=False):
        first = base if i == 0 and not arrival else other_base
        col = (t, t, t, chip_peer)[i] if not arrival else (t, chip_peer, core_peer, lax.rem(core_peer + 2, tps))[i]
        to = ({"sp": mate}, {"tp": chip_peer}, {"tp": core_peer}, {"tp": core_peer})[i]
        ref = norm_part(first, col)
        return remote(ref, ref, norm_send.at[i], norm_recv.at[i], to)

    edge_from = pl.ds(pl.multiple_of(base + jnp.where(low, tokens - EDGE, 0), EDGE), EDGE)
    edge_over = pl.ds(pl.multiple_of(jnp.where(low, 0, EDGE + rows2), EDGE), EDGE)
    edge_here = pl.ds(pl.multiple_of(jnp.where(low, EDGE + rows2, 0), EDGE), EDGE)

    def edge_copy(i):
        return remote(normed.at[edge_from, my_cols], normed.at[edge_over, my_cols], edge_send.at[i],
                      edge_recv.at[0], {"sp": (mirror, beyond)[i]})

    def edge_arrival():
        ref = normed.at[edge_here, my_cols]
        return remote(ref, ref, edge_send.at[0], edge_recv.at[0], {"sp": mirror})

    def row_copy(j, arrival=False):
        col = lax.rem(t + tps - j, tps) if arrival else t
        ref = normed.at[edge_here, pl.ds(pl.multiple_of(col * cols, 128), cols)]
        return remote(ref, ref, row_send.at[j - 1], row_recv.at[j - 1], {"tp": lax.rem(t + j, tps)})

    tile = 256

    def source_of(slot):
        return (mate, jnp.where(low, n // 2, n // 2 - 1), jnp.where(low, n - 1, 0), s)[slot]

    with_edge = pl.ds(pl.multiple_of(jnp.where(low, EDGE, 0), EDGE), rows2 + EDGE)
    both = pl.ds(EDGE, rows2)

    def gate_up(slot):
        if slot != OWN:
            have(0, slot)
            have(1, slot)
        k = pl.ds(pl.multiple_of(source_of(slot) * depth, 128), depth)

        @pl.loop(0, my_part // tile)
        def _(i):
            at = pl.ds(pl.multiple_of(i * tile, 128), tile)
            ga = jnp.dot(normed[with_edge, k], wg_all[slot, :, at], preferred_element_type=F32)
            if slot == OWN:
                gate[with_edge, at] = ga
            else:
                gate[with_edge, at] += ga
            ub = jnp.dot(normed[both, k], wu_all[slot, :, at], preferred_element_type=F32)
            if slot == OWN:
                up[:, at] = ub
            else:
                up[:, at] += ub

    @pl.when(inner)
    def _():
        for i in range(2):
            edge_copy(i).start()

    norm_copy(0).start()

    @pl.when(outer)
    def _():
        ship_all(OUT_MIRROR, 1)
        ship_all(OUT_MATE, 2)
        ship_all(OUT_REST, 2)
        take(0, 1)
        take(1, 0)

    @pl.when(inner)
    def _():
        ship_all(IN_ACROSS, 1)
        ship_all(IN_BEYOND, 1)
        ship_all(IN_MATE, 2)
        ship_all(IN_ACROSS, 2)
        ship_all(IN_BEYOND, 2)

    by_role(lambda r: [local(i, r).wait() for i in (5, 6, 7)])

    take(0, 2)

    @pl.when(inner)
    def _():
        take(1, 2)

    norm_copy(0, True).wait_recv()
    norm_copy(1).start()
    norm_copy(2).start()
    edge_arrival().wait_recv()
    for j in range(1, tps):
        row_copy(j).start()

    @pl.when(inner)
    def _():
        take(1, 1)

    norm_copy(1, True).wait_recv()
    norm_copy(3).start()

    @pl.when(outer)
    def _():
        take(1, 2)

    norm_copy(2, True).wait_recv()
    norm_copy(3, True).wait_recv()
    for j in range(1, tps):
        row_copy(j, True).wait_recv()
    gate_up(OWN)
    gate_up(0)

    @pl.when(outer)
    def _():
        take(1, 1)

    gate_up(2)

    take(2, 0)

    gate_up(1)

    @pl.when(low)
    def _():
        gate[0:EDGE, :] = jnp.zeros((EDGE, parts[0]), F32)

    @pl.when(jnp.logical_not(low))
    def _():
        gate[EDGE + rows2:, :] = jnp.zeros((EDGE, parts[0]), F32)

    @pl.when(outer)
    def _():
        ship_all(OUT_MIRROR, 2)

    @pl.when(inner)
    def _():
        take(2, 1, (0,))

    @pl.loop(0, my_part // 128)
    def _(i):
        at = pl.ds(pl.multiple_of(i * 128, 128), 128)
        ch = pl.ds(pl.multiple_of(hidden_at + i * 128, 128), 128)
        gate[:, at] = gate[:, at].astype(BF16).astype(F32)
        conv = cb_ref[:, ch]
        for tap in range(CONV):
            conv = conv + gate[pl.ds(EDGE - CONV // 2 + tap, rows2), at] * cw_ref[tap:tap + 1, ch]
        silu = conv / (1.0 + jnp.exp(-conv))
        act[:, at] = (silu * up[:, at].astype(BF16).astype(F32)).astype(BF16)

    half_rows = tokens // 2
    wide = cols // SPLIT
    far_first = (1 - t // 2) * 2

    def is_far(p):
        return (p // 2) != (t // 2)

    def rows_of(i):
        return pl.ds(pl.multiple_of((base if i else other_base) - EDGE, tokens), tokens)

    def half_of(i, c):
        first = (base if i else other_base) - EDGE + c * half_rows
        return pl.ds(pl.multiple_of(first, half_rows), half_rows)

    def half_rows_of(c):
        return pl.ds(pl.multiple_of(c * half_rows, half_rows), half_rows)

    def block_of(c):
        return pl.ds(c * wide, wide)

    def near_copy(i, c):
        return remote(terms.at[core_peer, rows_of(i), block_of(c)], near_in.at[i, :, block_of(c)],
                      near_send.at[i, c], near_recv.at[i, c], {"tp": core_peer})

    def pair_copy(p, i, c):
        q = lax.rem(p, 2)
        return remote(terms.at[p, half_of(i, 1 - core), block_of(c)], pair_in.at[q, i, :, block_of(c)],
                      pair_send.at[q, i, c], pair_recv.at[q, i, c], {"tp": core_peer})

    def mid_copy(p, c):
        q = lax.rem(p, 2)
        return remote(terms.at[p, half_of(0, core), block_of(c)], mid_in.at[q, :, block_of(c)],
                      mid_send.at[q, c], mid_recv.at[q, c], {"sp": mate})

    def far_copy(p, c):
        return remote(terms.at[p, half_of(1, core), block_of(c)], far_in.at[half_rows_of(core), block_of(c)],
                      far_send.at[lax.rem(p, 2), c], far_recv.at[core, c], {"tp": p})

    def far_arrival(h, c):
        ref = far_in.at[half_rows_of(h), block_of(c)]
        return remote(ref, ref, far_send.at[h, c], far_recv.at[h, c], {"tp": far_first + h})

    def ret_copy(c):
        return remote(ret_out.at[:, block_of(c)], ret_in.at[:, block_of(c)], ret_send.at[c], ret_recv.at[c],
                      {"sp": mate})

    def down(slot, p, c, i):
        def run(r):
            w = wd_all[slot, 0:parts[r], block_of(c)]
            x = act[rows_of(i), 0:parts[r]]
            terms[p, rows_of(i), block_of(c)] = jnp.dot(x, w, preferred_element_type=F32).astype(BF16)

        by_role(run)

        @pl.when(p == core_peer)
        def _():
            near_copy(i, c).start()

        @pl.when(is_far(p))
        def _():
            pair_copy(p, i, c).start()

    def gather(p, c):
        for i in range(2):
            @pl.when(is_far(p))
            def _():
                pair_copy(p, i, c).wait_recv()
                rows = half_of(i, core)
                total = (terms[p, rows, block_of(c)].astype(F32)
                         + pair_in[lax.rem(p, 2), i, :, block_of(c)].astype(F32))
                terms[p, rows, block_of(c)] = total.astype(BF16)
                if i == 0:
                    mid_copy(p, c).start()

        @pl.when(p == t)
        def _():
            near_copy(0, c).wait_recv()
            ret_out[:, block_of(c)] = (terms[t, rows_of(0), block_of(c)].astype(F32)
                                       + near_in[0, :, block_of(c)].astype(F32)).astype(BF16)
            ret_copy(c).start()

    def send_far(p, c):
        @pl.when(is_far(p))
        def _():
            mid_copy(p, c).wait_recv()
            rows = half_of(1, core)
            total = terms[p, rows, block_of(c)].astype(F32) + mid_in[lax.rem(p, 2), :, block_of(c)].astype(F32)
            terms[p, rows, block_of(c)] = total.astype(BF16)
            far_copy(p, c).start()

    def finish(c):
        near_copy(1, c).wait_recv()
        at = pl.ds(pl.multiple_of(t * cols + c * wide, 128), wide)
        out = normed[pl.ds(base, tokens), at].astype(F32) + terms[t, rows_of(1), block_of(c)].astype(F32)
        out = out + near_in[1, :, block_of(c)].astype(F32)
        for h in range(2):
            far_arrival(h, c).wait_recv()
        out = out + far_in[:, block_of(c)].astype(F32)
        ret_copy(c).wait_recv()
        out = out + ret_in[:, block_of(c)].astype(F32)
        out_ref[:, block_of(c)] = out.astype(BF16)

    def downs(slot, p, c):
        for i in range(2):
            down(slot, p, c, i)

    have(2, 0)
    early = [(jnp.where(inner, OWN, 0), jnp.where(inner, s, mate)), (jnp.where(inner, 0, OWN), jnp.where(inner, mate, s))]
    early = [(slot, p, c) for slot, p in early for c in range(SPLIT)]
    late = [(slot, source_of(slot), c) for slot in (1, 2) for c in range(SPLIT)]
    steps = early + late
    head = len(early)
    for at, (slot, p, c) in enumerate(steps):
        if at == head:
            gather(*steps[at - 1][1:])

            @pl.when(outer)
            def _():
                take(2, slot, (c,))

        if at >= head and at + 1 < len(steps):
            take(2, steps[at + 1][0], (steps[at + 1][2],))
        if at >= head:
            have(2, slot, (c,))
        downs(slot, p, c)
        if at >= head:
            gather(p, c)
            send_far(*steps[at - head][1:])
            if at > head:
                send_far(*steps[at - 1][1:])
        elif at:
            gather(*steps[at - 1][1:])
    send_far(*steps[-1][1:])
    for c in range(SPLIT):
        finish(c)

    @pl.when(inner)
    def _():
        for kind in (IN_ACROSS, IN_BEYOND, IN_MATE, IN_RELAY):
            for m in range(3):
                for c in range(SPLIT):
                    ship(kind, m, c).wait_send()

    @pl.when(outer)
    def _():
        for kind in (OUT_MATE, OUT_MIRROR, OUT_REST):
            for m in range(3) if kind != OUT_REST else (2,):
                for c in range(SPLIT):
                    ship(kind, m, c).wait_send()

    def crossed(r):
        for m in range(3):
            for slot in range(n - 1):
                for c in range(SPLIT):
                    if not direct(m, slot, r):
                        cross(m, slot, r, c).wait_send()

    by_role(crossed)
    for i in range(4):
        norm_copy(i).wait_send()
    for j in range(1, tps):
        row_copy(j).wait_send()

    @pl.when(inner)
    def _():
        for i in range(2):
            edge_copy(i).wait_send()

    for c in range(SPLIT):
        ret_copy(c).wait_send()
        for i in range(2):
            near_copy(i, c).wait_send()
            for h in range(2):
                pair_copy(far_first + h, i, c).wait_send()
        for h in range(2):
            mid_copy(far_first + h, c).wait_send()
            far_copy(far_first + h, c).wait_send()

    @pl.when(has_left)
    def _():
        for i in range(2):
            halo_copy(i, True).wait_send()

    @pl.when(has_right)
    def _():
        for i in range(2):
            halo_copy(i, False).wait_send()

    for step in range(3):
        spread(*proj_args, step).wait_send()
        spread(*mix_args, step).wait_send()


def kernel_shards(
    sizes, queries, keys, values, sink, resid, out_proj, norm_gain, w_gate, w_up, conv_w, conv_b, w_down
):
    groups, n, tps = sizes
    tokens, width = resid.shape
    cols = out_proj.shape[1]
    depth, hidden = w_gate.shape
    part = parts_of(hidden)[0]
    vmem = pl.BlockSpec(memory_space=pltpu.VMEM)
    hbm = pl.BlockSpec(memory_space=pl.ANY)
    smem = pl.BlockSpec(memory_space=pltpu.SMEM)
    dma = pltpu.SemaphoreType.DMA
    block = (tokens, cols)
    return pl.pallas_call(
        functools.partial(layer_kernel, sizes),
        out_shape=jax.ShapeDtypeStruct((tokens, cols), BF16),
        in_specs=[hbm] * 3 + [smem, hbm, hbm, vmem, hbm, hbm, vmem, vmem, hbm],
        out_specs=vmem,
        scratch_shapes=[
            pltpu.VMEM(queries.shape, BF16),
            pltpu.VMEM((2, tokens + 2 * WINDOW, HD), BF16),
            pltpu.VMEM(resid.shape, BF16),
            pltpu.VMEM((tps,) + out_proj.shape, BF16),
            pltpu.VMEM((tps,) + queries.shape, BF16),
            pltpu.VMEM((tokens // 2, width), F32),
            pltpu.VMEM((2 * tokens + 2 * EDGE, width), BF16),
            pltpu.VMEM((n, depth, part), BF16),
            pltpu.VMEM((n, depth, part), BF16),
            pltpu.VMEM((n, part, cols), BF16),
            pltpu.VMEM((2 * tokens + 2 * EDGE, part), F32),
            pltpu.VMEM((2 * tokens, part), F32),
            pltpu.VMEM((2 * tokens, part), BF16),
            pltpu.VMEM((tps, 2 * tokens, cols), BF16),
            pltpu.VMEM((2,) + block, BF16),
            pltpu.VMEM((2, 2, tokens // 2, cols), BF16),
            pltpu.VMEM(block, BF16),
            pltpu.VMEM((2, tokens // 2, cols), BF16),
            pltpu.VMEM(block, BF16),
            pltpu.VMEM(block, BF16),
            dma((8,)), dma((2, 2)), dma((2, 2)),
            dma((3, 4, SPLIT)), dma((3, 3, SPLIT)), dma((3, 3, SPLIT)), dma((3, 3, SPLIT)),
            dma((3,)), dma((3,)), dma((3,)), dma((3,)), dma((4,)), dma((4,)), dma((2,)), dma((1,)),
            dma((3,)), dma((3,)),
            dma((2, SPLIT)), dma((2, SPLIT)), dma((2, 2, SPLIT)), dma((2, 2, SPLIT)),
            dma((2, SPLIT)), dma((2, SPLIT)), dma((2, SPLIT)), dma((2, SPLIT)), dma((SPLIT,)), dma((SPLIT,)),
        ],
        compiler_params=pltpu.CompilerParams(
            collective_id=0, has_side_effects=True, vmem_limit_bytes=67043328
        ),
    )(queries, keys, values, sink, resid, out_proj, norm_gain[None], w_gate, w_up, conv_w, conv_b[None], w_down)


def fits_kernel(sizes, args):
    groups, n, tps = sizes
    queries, resid, out_proj, w_gate, w_down = args[0], args[4], args[5], args[7], args[11]
    share = groups * SPLIT
    weights = 3 * 2 * n * w_gate.shape[0] * w_gate.shape[1]
    return (
        n == 4
        and tps == 4
        and groups == 2
        and w_down.shape[1] == out_proj.shape[1]
        and w_gate.shape[0] % max(share * EDGE, 128) == 0
        and w_down.shape[1] % (share * 128) == 0
        and w_gate.shape[1] % 768 == 0
        and resid.shape[0] % (4 * WINDOW) == 0
        and weights <= 20 * 2 ** 20
    )


def run_shards(sizes, *args):
    if fits_kernel(sizes, args):
        return kernel_shards(sizes, *args)
    return shards(*args)


def solution(mesh):
    sizes = tuple(mesh.shape[axis] for axis in ("grp", "sp", "tp"))
    return jax.shard_map(
        functools.partial(run_shards, sizes),
        mesh=mesh,
        in_specs=(
            P(("grp", "sp"), "tp"),
            P(("grp", "sp"), None),
            P(("grp", "sp"), None),
            P("tp"),
            P(("grp", "sp"), None),
            P(None, "tp"),
            P(),
            P("sp", "tp"),
            P("sp", "tp"),
            P(None, "tp"),
            P("tp"),
            P("tp", "sp"),
        ),
        out_specs=P(("grp", "sp"), "tp"),
        check_vma=False,
    )
```

```python
import functools

import jax
import jax.numpy as jnp
from jax import lax
from jax.experimental import pallas as pl
from jax.experimental.pallas import tpu as pltpu
from jax.sharding import PartitionSpec as P

H = 8
KVH = 2
HD = 128
WINDOW = 128
CONV = 3


def with_halo(cells, sides, width):
    for axis, dim in sides:
        count = lax.axis_size(axis)
        ends = count - 1
        head = lax.slice_in_dim(cells, 0, width, axis=dim)
        tail = lax.slice_in_dim(cells, cells.shape[dim] - width, cells.shape[dim], axis=dim)
        cells = jnp.concatenate(
            [
                lax.ppermute(tail, axis, [(i, (i + 1) % count) for i in range(ends)]),
                cells,
                lax.ppermute(head, axis, [((i + 1) % count, i) for i in range(ends)]),
            ],
            axis=dim,
        )
    return cells


def shards(
    queries, keys, values, sink, resid, out_proj, norm_gain, w_gate, w_up, conv_w, conv_b, w_down
):
    tokens = queries.shape[0]
    width = resid.shape[1]
    heads_here = sink.shape[0]
    group = H // KVH
    scale = HD ** (-0.5)
    first_head = lax.axis_index("tp") * heads_here
    kv_head = first_head // group
    own_keys = lax.dynamic_slice_in_dim(keys, kv_head * HD, HD, 1)
    own_values = lax.dynamic_slice_in_dim(values, kv_head * HD, HD, 1)
    extended = with_halo(jnp.stack([own_keys, own_values]), (("sp", 1),), WINDOW)
    ext_keys = extended[0]
    ext_values = extended[1]
    span = tokens + 2 * WINDOW
    q_heads = queries.reshape(tokens, heads_here, HD)
    scores = (
        jnp.einsum("qhd,kd->hqk", q_heads, ext_keys, preferred_element_type=jnp.float32) * scale
    )
    offset = lax.axis_index("sp") * tokens
    q_pos = offset + jnp.arange(tokens, dtype=jnp.int32)[:, None]
    k_pos = offset - WINDOW + jnp.arange(span, dtype=jnp.int32)[None, :]
    seq_total = tokens * lax.axis_size("sp")
    valid = (jnp.abs(q_pos - k_pos) <= WINDOW) & (k_pos >= 0) & (k_pos < seq_total)
    scores = jnp.where(valid[None], scores, jnp.float32(-1e30))
    sink_col = sink[:, None]
    top = jnp.maximum(jnp.max(scores, axis=-1), sink_col)
    expo = jnp.exp(scores - top[..., None])
    total = jnp.sum(expo, axis=-1) + jnp.exp(sink_col - top)
    weights = (expo / total[..., None]).astype(jnp.bfloat16)
    heads_out = jnp.einsum("hqk,kd->qhd", weights, ext_values, preferred_element_type=jnp.float32)
    heads_out = heads_out.astype(jnp.bfloat16).reshape(tokens, heads_here * HD)
    all_heads = lax.all_gather(heads_out, "tp", axis=1, tiled=True)
    cols = width // lax.axis_size("tp")
    col_start = lax.axis_index("tp") * cols
    full_proj = lax.all_gather(out_proj, "tp", axis=1, tiled=True)
    summed = resid.astype(jnp.float32) + jnp.dot(
        all_heads, full_proj, preferred_element_type=jnp.float32
    )
    mean = jnp.mean(summed, axis=-1, keepdims=True)
    msq = jnp.mean(summed * summed, axis=-1, keepdims=True)
    normed_full = ((summed - mean) * lax.rsqrt(msq - mean * mean + 1e-05) * norm_gain).astype(
        jnp.bfloat16
    )
    normed_own = lax.dynamic_slice_in_dim(normed_full, col_start, cols, 1)
    gate_acc = jnp.dot(
        normed_full,
        lax.all_gather(w_gate, "sp", axis=0, tiled=True),
        preferred_element_type=jnp.float32,
    )
    up_acc = jnp.dot(
        normed_full,
        lax.all_gather(w_up, "sp", axis=0, tiled=True),
        preferred_element_type=jnp.float32,
    )
    gate_pre = gate_acc.astype(jnp.bfloat16)
    up_part = up_acc.astype(jnp.bfloat16)
    padded = with_halo(gate_pre, (("sp", 0),), CONV // 2)
    conv = conv_b
    for tap in range(CONV):
        conv = conv + padded[tap : tap + tokens].astype(jnp.float32) * conv_w[tap]
    act = (jax.nn.silu(conv) * up_part.astype(jnp.float32)).astype(jnp.bfloat16)
    terms = jnp.dot(
        act, lax.all_gather(w_down, "sp", axis=1, tiled=True), preferred_element_type=jnp.float32
    )
    ffn_own = lax.psum_scatter(
        terms.astype(jnp.bfloat16), "tp", scatter_dimension=1, tiled=True
    ).astype(jnp.float32)
    return (normed_own.astype(jnp.float32) + ffn_own).astype(jnp.bfloat16)


EDGE = 16
SPLIT = 2
PIECES = 4
BF16 = jnp.bfloat16
F32 = jnp.float32


def parts_of(hidden):
    return hidden * 2 // 3, hidden // 3


def layer_kernel(
    sizes,
    q_hbm, k_hbm, v_hbm, sink_ref, resid_hbm, proj_hbm, gain_ref, wg_hbm, wu_hbm, cw_ref, cb_ref, wd_hbm,
    out_ref,
    q_ref, kv_ext, resid_ref, proj_all, mixed, summed, normed, wg_all, wu_all, wd_all, gate, up, silu, act,
    terms, near_in, pair_in, far_in, mid_in, over_in, ret_out, ret_in,
    local_sem, halo_send, halo_recv, z_send, z_recv, y_send, y_recv,
    proj_send, proj_recv, mix_send, mix_recv, norm_send, norm_recv, edge_send, edge_recv, row_send, row_recv,
    near_send, near_recv, pair_send, pair_recv, far_send, far_recv, mid_send, mid_recv, over_send, over_recv, ret_send, ret_recv,
):
    groups, n, tps = sizes
    g = lax.axis_index("grp")
    s = lax.axis_index("sp")
    t = lax.axis_index("tp")
    tokens, width = resid_hbm.shape
    heads_here = sink_ref.shape[0]
    cols = proj_hbm.shape[1]
    depth = wg_hbm.shape[0]
    hidden = wg_hbm.shape[1]
    parts = parts_of(hidden)
    starts = (0, parts[0])
    rows2 = 2 * tokens
    has_left, has_right = s > 0, s < n - 1
    inner = has_left & has_right
    outer = jnp.logical_not(inner)
    low = s < n // 2
    mate = s + 1 - 2 * lax.rem(s, 2)
    mirror = n - 1 - s
    beyond = n - 1 - mate
    role = 1 - jnp.where(inner, 1, 0)
    hidden_at = pl.multiple_of(role * parts[0], 128)
    my_part = jnp.where(inner, parts[0], parts[1])
    base = pl.multiple_of(EDGE + lax.rem(s, 2) * tokens, EDGE)
    other_base = pl.multiple_of(EDGE + (1 - lax.rem(s, 2)) * tokens, EDGE)
    core = lax.rem(t, 2)
    core_peer = t + 1 - 2 * core
    chip_peer = lax.rem(t + 2, tps)
    own = (wg_hbm, wu_hbm, wd_hbm)
    full = (wg_all, wu_all, wd_all)
    OWN = n - 1

    def remote(src, dst, send, recv, to):
        return pltpu.make_async_remote_copy(
            src_ref=src, dst_ref=dst, send_sem=send, recv_sem=recv,
            device_id=to, device_id_type=pl.DeviceIdType.MESH,
        )

    kv_head = (t * heads_here) // (H // KVH)
    kv_cols = pl.ds(pl.multiple_of(kv_head * HD, HD), HD)

    def by_role(fn):
        for r, here in enumerate((inner, outer)):
            @pl.when(here)
            def _():
                fn(r)

    def local(i, r=0):
        here, mine = pl.ds(starts[r], parts[r]), pl.ds(0, parts[r])
        src, dst = (
            (q_hbm, q_ref),
            (k_hbm.at[:, kv_cols], kv_ext.at[0, pl.ds(WINDOW, tokens)]),
            (v_hbm.at[:, kv_cols], kv_ext.at[1, pl.ds(WINDOW, tokens)]),
            (proj_hbm, proj_all.at[t]),
            (resid_hbm, resid_ref),
            (wg_hbm.at[:, here], wg_all.at[OWN, :, mine]),
            (wu_hbm.at[:, here], wu_all.at[OWN, :, mine]),
            (wd_hbm.at[here], wd_all.at[OWN, mine]),
        )[i]
        return pltpu.make_async_copy(src, dst, local_sem.at[i])

    for i in range(5):
        local(i).start()
    by_role(lambda r: [local(i, r).start() for i in (5, 6, 7)])

    barrier = pltpu.get_barrier_semaphore()

    def greet(to):
        pl.semaphore_signal(barrier, inc=1, device_id=to, device_id_type=pl.DeviceIdType.MESH)

    for j in range(1, n):
        greet({"sp": lax.rem(s + j, n)})
    for j in range(1, groups):
        greet({"grp": lax.rem(g + j, groups)})
    for j in range(1, tps):
        greet({"tp": lax.rem(t + j, tps)})
    for j in range(2):
        greet({"sp": mate, "tp": lax.rem(t - core + 2 + j, tps)})
    pl.semaphore_wait(barrier, n - 1 + groups - 1 + tps - 1 + 2)

    def halo_copy(i, to_left):
        ref = (k_hbm, v_hbm)[i]
        if to_left:
            return remote(ref.at[pl.ds(0, WINDOW), kv_cols], kv_ext.at[i, pl.ds(WINDOW + tokens, WINDOW)],
                          halo_send.at[i, 0], halo_recv.at[i, 0], {"sp": s - 1})
        return remote(ref.at[pl.ds(tokens - WINDOW, WINDOW), kv_cols], kv_ext.at[i, pl.ds(0, WINDOW)],
                      halo_send.at[i, 1], halo_recv.at[i, 1], {"sp": s + 1})

    deep = PIECES // SPLIT

    def window(m, of, c, first, count):
        if m < 2:
            step = depth // (groups * PIECES)
            return pl.ds(pl.multiple_of((of * PIECES + c) * step, EDGE), step), pl.ds(first, count)
        step = cols // (groups * SPLIT)
        at = pl.multiple_of(((c // deep) * groups + of) * step, 128)
        return pl.ds(first + (c % deep) * (count // deep), count // deep), pl.ds(at, step)

    def source(m, r, of, c):
        return own[m].at[window(m, of, c, starts[r], parts[r])]

    def place(m, slot, r, of, c):
        return full[m].at[(slot,) + window(m, of, c, 0, parts[r])]

    IN_ACROSS, IN_BEYOND, IN_MATE, IN_RELAY, OUT_MATE, OUT_MIRROR, OUT_REST = range(7)

    def ship(kind, m, c):
        slot, to, lane = {
            IN_ACROSS: (1, mirror, 0),
            IN_BEYOND: (1, beyond, 1),
            IN_MATE: (0, mate, 2),
            IN_RELAY: (2, mirror, 3),
            OUT_MATE: (0, mate, 0),
            OUT_MIRROR: (2, mirror, 1),
            OUT_REST: (0, mate, 2),
        }[kind]
        r = 0 if kind in (IN_ACROSS, IN_RELAY, OUT_MATE, OUT_REST) else 1
        of = 1 - g if kind == OUT_REST else g
        src = place(m, 0, r, of, c) if kind == IN_RELAY else source(m, r, of, c)
        arrive = y_recv.at[m, slot, c] if kind == OUT_REST else z_recv.at[m, slot, c]
        return remote(src, place(m, slot, r, of, c), z_send.at[m, lane, c], arrive, {"sp": to})

    def ship_all(kind, m):
        for c in range(PIECES):
            ship(kind, m, c).start()

    def direct(m, slot, r):
        return r == 0 and m == 2 and isinstance(slot, int) and slot == 0

    def cross(m, slot, r, c):
        return remote(place(m, slot, r, g, c), place(m, slot, r, g, c), y_send.at[m, slot, c], y_recv.at[m, slot, c],
                      {"grp": 1 - g})

    def pieces_of(m, cs):
        return range(PIECES) if m < 2 else [c * deep + d for c in cs for d in range(deep)]

    def take(m, slot, cs=range(SPLIT)):
        def run(r):
            for c in pieces_of(m, cs):
                remote(place(m, slot, r, g, c), place(m, slot, r, g, c), z_send.at[m, 0, c], z_recv.at[m, slot, c],
                       {"sp": mate}).wait_recv()
                if not direct(m, slot, r):
                    cross(m, slot, r, c).start()
                if isinstance(slot, int) and slot == 0 and r == 0:
                    ship(IN_RELAY, m, c).start()

        by_role(run)

    def have(m, slot, cs=range(SPLIT)):
        def run(r):
            for c in pieces_of(m, cs):
                ref = place(m, slot, r, 1 - g, c)
                remote(ref, ref, y_send.at[m, slot, c], y_recv.at[m, slot, c], {"grp": 1 - g}).wait_recv()

        by_role(run)

    def spread(src, ref, send, recv, step):
        origin = (t, t, chip_peer)[step]
        return remote(src if step < 2 else ref.at[origin], ref.at[origin], send.at[step], recv.at[step],
                      {"tp": (core_peer, chip_peer, core_peer)[step]})

    def spread_arrival(src, ref, send, recv, step):
        origin = (core_peer, chip_peer, lax.rem(core_peer + 2, tps))[step]
        return remote(src, ref.at[origin], send.at[step], recv.at[step],
                      {"tp": (core_peer, chip_peer, core_peer)[step]})

    proj_args = (proj_hbm, proj_all, proj_send, proj_recv)
    mix_args = (mixed.at[t], mixed, mix_send, mix_recv)

    @pl.when(has_left)
    def _():
        for i in range(2):
            halo_copy(i, True).start()

    @pl.when(has_right)
    def _():
        for i in range(2):
            halo_copy(i, False).start()

    @pl.when(outer)
    def _():
        ship_all(OUT_MATE, 0)
        ship_all(OUT_MATE, 1)
        ship_all(OUT_MIRROR, 0)

    @pl.when(inner)
    def _():
        ship_all(IN_ACROSS, 0)
        ship_all(IN_BEYOND, 0)
        ship_all(IN_MATE, 0)
        ship_all(IN_MATE, 1)

    for step in (1, 0):
        spread(*proj_args, step).start()

    @pl.when(jnp.logical_not(has_left))
    def _():
        kv_ext[:, pl.ds(0, WINDOW), :] = jnp.zeros((2, WINDOW, HD), BF16)

    @pl.when(jnp.logical_not(has_right))
    def _():
        kv_ext[:, pl.ds(WINDOW + tokens, WINDOW), :] = jnp.zeros((2, WINDOW, HD), BF16)

    for i in range(3):
        local(i).wait()

    @pl.when(has_right)
    def _():
        for i in range(2):
            halo_copy(i, True).wait_recv()

    @pl.when(has_left)
    def _():
        for i in range(2):
            halo_copy(i, False).wait_recv()

    span = 3 * WINDOW
    seq_total = tokens * n

    @pl.loop(0, tokens // WINDOW)
    def _(b):
        start = pl.multiple_of(b * WINDOW, WINDOW)
        row = lax.broadcasted_iota(jnp.int32, (WINDOW, span), 0)
        col = lax.broadcasted_iota(jnp.int32, (WINDOW, span), 1)
        k_pos = s * tokens + start - WINDOW + col
        valid = (jnp.abs(row + WINDOW - col) <= WINDOW) & (k_pos >= 0) & (k_pos < seq_total)
        kb = kv_ext[0, pl.ds(start, span), :]
        vb = kv_ext[1, pl.ds(start, span), :]
        for h in range(heads_here):
            qb = q_ref[pl.ds(start, WINDOW), h * HD:(h + 1) * HD]
            sc = lax.dot_general(qb, kb, (((1,), (1,)), ((), ())), preferred_element_type=F32) * (HD ** -0.5)
            sc = jnp.where(valid, sc, F32(-1e30))
            sink = sink_ref[h]
            top = jnp.maximum(jnp.max(sc, axis=-1, keepdims=True), sink)
            expo = jnp.exp(sc - top)
            total = jnp.sum(expo, axis=-1, keepdims=True) + jnp.exp(sink - top)
            weights = (expo / total).astype(BF16)
            o = jnp.dot(weights, vb, preferred_element_type=F32)
            mixed[t, pl.ds(start, WINDOW), h * HD:(h + 1) * HD] = o.astype(BF16)

    for step in (1, 0):
        spread(*mix_args, step).start()

    take(0, 0)

    @pl.when(inner)
    def _():
        take(0, 1)

    for args in (proj_args, mix_args):
        spread_arrival(*args, 1).wait_recv()
        spread(*args, 2).start()
    for args in (proj_args, mix_args):
        for step in (0, 2):
            spread_arrival(*args, step).wait_recv()

    @pl.when(inner)
    def _():
        take(1, 0)

    for i in (3, 4):
        local(i).wait()
    lanes = mixed.shape[2]
    block = summed.shape[0]
    strip = 64

    @pl.loop(0, tokens // block)
    def _(b):
        rows = pl.ds(pl.multiple_of(b * block, block), block)

        @pl.loop(0, tps)
        def _(i):
            at = pl.ds(pl.multiple_of(i * cols, 128), cols)
            prod = jnp.dot(mixed[0, rows, :], proj_all[i, pl.ds(0, lanes), :], preferred_element_type=F32)
            for u in range(1, tps):
                prod += jnp.dot(mixed[u, rows, :], proj_all[i, pl.ds(u * lanes, lanes), :],
                                preferred_element_type=F32)
            summed[:, at] = resid_ref[rows, at].astype(F32) + prod

        @pl.loop(0, block // strip)
        def _(i):
            at = pl.multiple_of(i * strip, strip)
            x = summed[pl.ds(at, strip), :]
            mean = jnp.mean(x, axis=-1, keepdims=True)
            msq = jnp.mean(x * x, axis=-1, keepdims=True)
            normed[pl.ds(pl.multiple_of(base + b * block + at, EDGE), strip), :] = (
                (x - mean) * lax.rsqrt(msq - mean * mean + 1e-05) * gain_ref[...]
            ).astype(BF16)

    my_cols = pl.ds(pl.multiple_of(t * cols, 128), cols)

    def norm_part(first, col, c):
        step = tokens // PIECES
        return normed.at[pl.ds(pl.multiple_of(first + c * step, EDGE), step),
                         pl.ds(pl.multiple_of(col * cols, 128), cols)]

    def norm_copy(i, c, arrival=False):
        first = base if i == 0 and not arrival else other_base
        col = (t, t, t, chip_peer)[i] if not arrival else (t, chip_peer, core_peer, lax.rem(core_peer + 2, tps))[i]
        to = ({"sp": mate}, {"tp": chip_peer}, {"tp": core_peer}, {"tp": core_peer})[i]
        ref = norm_part(first, col, c)
        return remote(ref, ref, norm_send.at[i, c], norm_recv.at[i, c], to)

    edge_from = pl.ds(pl.multiple_of(base + jnp.where(low, tokens - EDGE, 0), EDGE), EDGE)
    edge_over = pl.ds(pl.multiple_of(jnp.where(low, 0, EDGE + rows2), EDGE), EDGE)
    edge_here = pl.ds(pl.multiple_of(jnp.where(low, EDGE + rows2, 0), EDGE), EDGE)

    def edge_copy(i):
        return remote(normed.at[edge_from, my_cols], normed.at[edge_over, my_cols], edge_send.at[i],
                      edge_recv.at[0], {"sp": (mirror, beyond)[i]})

    def edge_arrival():
        ref = normed.at[edge_here, my_cols]
        return remote(ref, ref, edge_send.at[0], edge_recv.at[0], {"sp": mirror})

    def row_copy(j, arrival=False):
        col = lax.rem(t + tps - j, tps) if arrival else t
        ref = normed.at[edge_here, pl.ds(pl.multiple_of(col * cols, 128), cols)]
        return remote(ref, ref, row_send.at[j - 1], row_recv.at[j - 1], {"tp": lax.rem(t + j, tps)})

    tile = 256

    def source_of(slot):
        return (mate, jnp.where(low, n // 2, n // 2 - 1), jnp.where(low, n - 1, 0), s)[slot]

    with_edge = pl.ds(pl.multiple_of(jnp.where(low, EDGE, 0), EDGE), rows2 + EDGE)
    both = pl.ds(EDGE, rows2)

    def gate_of(slot):
        if slot != OWN:
            have(0, slot)
        k = pl.ds(pl.multiple_of(source_of(slot) * depth, 128), depth)

        @pl.loop(0, my_part // tile)
        def _(i):
            at = pl.ds(pl.multiple_of(i * tile, 128), tile)
            ga = jnp.dot(normed[with_edge, k], wg_all[slot, :, at], preferred_element_type=F32)
            gate[with_edge, at] = ga if slot == OWN else gate[with_edge, at] + ga

    def up_of(slot, last=False):
        if slot != OWN:
            have(1, slot)
        k = pl.ds(pl.multiple_of(source_of(slot) * depth, 128), depth)

        @pl.loop(0, my_part // tile)
        def _(i):
            at = pl.ds(pl.multiple_of(i * tile, 128), tile)
            ub = jnp.dot(normed[both, k], wu_all[slot, :, at], preferred_element_type=F32)
            if slot != OWN:
                ub = up[:, at] + ub
            if last:
                act[:, at] = (silu[:, at] * ub.astype(BF16).astype(F32)).astype(BF16)
            else:
                up[:, at] = ub

    @pl.when(inner)
    def _():
        for i in range(2):
            edge_copy(i).start()

    for c in range(PIECES):
        norm_copy(0, c).start()

    @pl.when(outer)
    def _():
        ship_all(OUT_MIRROR, 1)
        ship_all(OUT_MATE, 2)
        ship_all(OUT_REST, 2)
        take(0, 1)
        take(1, 0)

    @pl.when(inner)
    def _():
        ship_all(IN_ACROSS, 1)
        ship_all(IN_BEYOND, 1)
        ship_all(IN_MATE, 2)
        ship_all(IN_ACROSS, 2)
        ship_all(IN_BEYOND, 2)

    by_role(lambda r: [local(i, r).wait() for i in (5, 6, 7)])

    take(0, 2)

    @pl.when(inner)
    def _():
        take(1, 2)

    for c in range(PIECES):
        norm_copy(0, c, True).wait_recv()
        norm_copy(1, c).start()
        norm_copy(2, c).start()
    edge_arrival().wait_recv()
    for j in range(1, tps):
        row_copy(j).start()

    for c in range(PIECES):
        norm_copy(1, c, True).wait_recv()
        norm_copy(3, c).start()

    @pl.when(outer)
    def _():
        take(1, 2)

    for c in range(PIECES):
        norm_copy(2, c, True).wait_recv()
        norm_copy(3, c, True).wait_recv()
    for j in range(1, tps):
        row_copy(j, True).wait_recv()
    gate_of(OWN)
    gate_of(0)
    gate_of(2)
    gate_of(1)

    @pl.when(inner)
    def _():
        take(1, 1)

    @pl.when(low)
    def _():
        gate[0:EDGE, :] = jnp.zeros((EDGE, parts[0]), F32)

    @pl.when(jnp.logical_not(low))
    def _():
        gate[EDGE + rows2:, :] = jnp.zeros((EDGE, parts[0]), F32)

    @pl.loop(0, my_part // 128)
    def _(i):
        at = pl.ds(pl.multiple_of(i * 128, 128), 128)
        ch = pl.ds(pl.multiple_of(hidden_at + i * 128, 128), 128)
        gate[:, at] = gate[:, at].astype(BF16).astype(F32)
        conv = cb_ref[pl.ds(role * (parts[0] // 128) + i, 1), :]
        for tap in range(CONV):
            conv = conv + gate[pl.ds(EDGE - CONV // 2 + tap, rows2), at] * cw_ref[tap:tap + 1, ch]
        silu[:, at] = conv / (1.0 + jnp.exp(-conv))

    up_of(OWN)
    up_of(0)
    up_of(2)

    @pl.when(outer)
    def _():
        ship_all(OUT_MIRROR, 2)
        take(1, 1)

    take(2, 0)

    up_of(1, last=True)

    @pl.when(inner)
    def _():
        take(2, 1, (0,))

    half_rows = tokens // 2
    wide = cols // SPLIT
    far_first = (1 - t // 2) * 2

    def is_far(p):
        return (p // 2) != (t // 2)

    def rows_of(i):
        return pl.ds(pl.multiple_of((base if i else other_base) - EDGE, tokens), tokens)

    def half_of(i, c):
        first = (base if i else other_base) - EDGE + c * half_rows
        return pl.ds(pl.multiple_of(first, half_rows), half_rows)

    def half_rows_of(c):
        return pl.ds(pl.multiple_of(c * half_rows, half_rows), half_rows)

    def block_of(c):
        return pl.ds(c * wide, wide)

    def near_copy(i, c):
        return remote(terms.at[core_peer, rows_of(i), block_of(c)], near_in.at[i, :, block_of(c)],
                      near_send.at[i, c], near_recv.at[i, c], {"tp": core_peer})

    def pair_copy(p, i, c):
        q = lax.rem(p, 2)
        return remote(terms.at[p, half_of(i, 1 - core), block_of(c)], pair_in.at[q, i, :, block_of(c)],
                      pair_send.at[q, i, c], pair_recv.at[q, i, c], {"tp": core_peer})

    def mid_copy(p, c):
        q = lax.rem(p, 2)
        return remote(terms.at[p, half_of(0, core), block_of(c)], mid_in.at[q, :, block_of(c)],
                      mid_send.at[q, c], mid_recv.at[q, c], {"sp": mate})

    def far_copy(p, c):
        return remote(terms.at[p, half_of(1, core), block_of(c)], far_in.at[half_rows_of(core), block_of(c)],
                      far_send.at[lax.rem(p, 2), c], far_recv.at[core, c], {"tp": p})

    def over_copy(slot, c):
        p = source_of(slot)
        to = {"tp": p} if slot == 1 else {"sp": mate, "tp": p}
        return remote(terms.at[p, half_of(0, core), block_of(c)], over_in.at[half_rows_of(core), block_of(c)],
                      over_send.at[slot - 1, c], over_recv.at[core, c], to)

    def over_arrival(h, c):
        ref = over_in.at[half_rows_of(h), block_of(c)]
        return remote(ref, ref, over_send.at[0, c], over_recv.at[h, c], {"sp": mate, "tp": far_first + h})

    def far_arrival(h, c):
        ref = far_in.at[half_rows_of(h), block_of(c)]
        return remote(ref, ref, far_send.at[h, c], far_recv.at[h, c], {"tp": far_first + h})

    def ret_copy(c):
        return remote(ret_out.at[:, block_of(c)], ret_in.at[:, block_of(c)], ret_send.at[c], ret_recv.at[c],
                      {"sp": mate})

    def down(slot, p, c, i):
        def run(r):
            w = wd_all[slot, 0:parts[r], block_of(c)]
            x = act[rows_of(i), 0:parts[r]]
            terms[p, rows_of(i), block_of(c)] = jnp.dot(x, w, preferred_element_type=F32).astype(BF16)

        by_role(run)

        @pl.when(p == core_peer)
        def _():
            near_copy(i, c).start()

        @pl.when(is_far(p))
        def _():
            pair_copy(p, i, c).start()

    def gather(p, c, late=None):
        for i in range(2):
            @pl.when(is_far(p))
            def _():
                pair_copy(p, i, c).wait_recv()
                rows = half_of(i, core)
                total = (terms[p, rows, block_of(c)].astype(F32)
                         + pair_in[lax.rem(p, 2), i, :, block_of(c)].astype(F32))
                terms[p, rows, block_of(c)] = total.astype(BF16)
                if i == 0 and late:
                    @pl.when(inner)
                    def _():
                        over_copy(late, c).start()

                    @pl.when(outer)
                    def _():
                        mid_copy(p, c).start()
                elif i == 0:
                    mid_copy(p, c).start()

        @pl.when((p == t) & outer if late == 1 else p == t)
        def _():
            near_copy(0, c).wait_recv()
            ret_out[:, block_of(c)] = (terms[t, rows_of(0), block_of(c)].astype(F32)
                                       + near_in[0, :, block_of(c)].astype(F32)).astype(BF16)
            ret_copy(c).start()

    def ret_late(c):
        @pl.when(inner & (t == source_of(1)))
        def _():
            near_copy(0, c).wait_recv()
            for h in range(2):
                over_arrival(h, c).wait_recv()
            ret_out[:, block_of(c)] = (terms[t, rows_of(0), block_of(c)].astype(F32)
                                       + near_in[0, :, block_of(c)].astype(F32)
                                       + over_in[:, block_of(c)].astype(F32)).astype(BF16)
            ret_copy(c).start()

    def send_far(p, c, last=False):
        if last:
            @pl.when(is_far(p))
            def _():
                far_copy(p, c).start()
            return

        @pl.when(is_far(p))
        def _():
            mid_copy(p, c).wait_recv()
            rows = half_of(1, core)
            total = terms[p, rows, block_of(c)].astype(F32) + mid_in[lax.rem(p, 2), :, block_of(c)].astype(F32)
            terms[p, rows, block_of(c)] = total.astype(BF16)
            far_copy(p, c).start()

    def finish(c):
        near_copy(1, c).wait_recv()
        at = pl.ds(pl.multiple_of(t * cols + c * wide, 128), wide)
        out = normed[pl.ds(base, tokens), at].astype(F32) + terms[t, rows_of(1), block_of(c)].astype(F32)
        out = out + near_in[1, :, block_of(c)].astype(F32)
        for h in range(2):
            far_arrival(h, c).wait_recv()
        out = out + far_in[:, block_of(c)].astype(F32)
        ret_copy(c).wait_recv()
        out = out + ret_in[:, block_of(c)].astype(F32)
        out_ref[:, block_of(c)] = out.astype(BF16)

        @pl.when(outer & (t == source_of(2)))
        def _():
            for h in range(2):
                over_arrival(h, c).wait_recv()
            out_ref[:, block_of(c)] = (out + over_in[:, block_of(c)].astype(F32)).astype(BF16)

    def downs(slot, p, c):
        for i in range(2):
            down(slot, p, c, i)

    def drain(ms):
        def run(r):
            for kind in ((IN_ACROSS, IN_BEYOND, IN_MATE, IN_RELAY), (OUT_MATE, OUT_MIRROR, OUT_REST))[r]:
                for m in ms:
                    for c in range(PIECES):
                        if m == 2 or kind != OUT_REST:
                            ship(kind, m, c).wait_send()
            for m in ms:
                for slot in range(n - 1):
                    for c in range(PIECES):
                        if not direct(m, slot, r):
                            cross(m, slot, r, c).wait_send()

        by_role(run)

    def drain_first():
        drain((0, 1))
        for i in range(4):
            for c in range(PIECES):
                norm_copy(i, c).wait_send()
        for j in range(1, tps):
            row_copy(j).wait_send()

        @pl.when(inner)
        def _():
            for i in range(2):
                edge_copy(i).wait_send()

        @pl.when(has_left)
        def _():
            for i in range(2):
                halo_copy(i, True).wait_send()

        @pl.when(has_right)
        def _():
            for i in range(2):
                halo_copy(i, False).wait_send()

        for step in range(3):
            spread(*proj_args, step).wait_send()
            spread(*mix_args, step).wait_send()

    have(2, 0)
    early = [(jnp.where(inner, OWN, 0), jnp.where(inner, s, mate)), (jnp.where(inner, 0, OWN), jnp.where(inner, mate, s))]
    early = [(slot, p, c) for slot, p in early for c in range(SPLIT)]
    late = [(slot, source_of(slot), c) for slot in (1, 2) for c in range(SPLIT)]
    steps = early + late
    head = len(early)
    for at, (slot, p, c) in enumerate(steps):
        if at == head:
            gather(*steps[at - 1][1:])

            @pl.when(outer)
            def _():
                take(2, slot, (c,))

        if at >= head and at + 1 < len(steps):
            take(2, steps[at + 1][0], (steps[at + 1][2],))
        if at >= head:
            have(2, slot, (c,))
        downs(slot, p, c)
        if at >= head:
            gather(p, c, slot)
            if slot == 2:
                ret_late(c)
            send_far(*steps[at - head][1:])
            if at == head:
                drain_first()

            @pl.when(inner)
            def _():
                for late_at in {head: (), head + 1: (head, head + 1)}.get(at, (at,)):
                    send_far(*steps[late_at][1:])

            @pl.when(outer)
            def _():
                send_far(p, c, True)
        elif at:
            gather(*steps[at - 1][1:])

    drain((2,))
    for c in range(SPLIT):
        for i in range(2):
            near_copy(i, c).wait_send()
            for h in range(2):
                pair_copy(far_first + h, i, c).wait_send()

    def mids(here, owners):
        @pl.when(here)
        def _():
            for c in range(SPLIT):
                for p in owners:
                    @pl.when(is_far(p))
                    def _():
                        mid_copy(p, c).wait_send()

    mids(inner, [p for _, p, c in early if c == 0])
    mids(outer, [p for _, p, c in steps if c == 0])

    @pl.when(inner)
    def _():
        for slot in (1, 2):
            @pl.when(is_far(source_of(slot)))
            def _():
                for c in range(SPLIT):
                    over_copy(slot, c).wait_send()

    finish(0)
    ret_copy(0).wait_send()
    for h in range(2):
        far_copy(far_first + h, 0).wait_send()
    finish(1)
    ret_copy(1).wait_send()
    for h in range(2):
        far_copy(far_first + h, 1).wait_send()


def kernel_shards(
    sizes, queries, keys, values, sink, resid, out_proj, norm_gain, w_gate, w_up, conv_w, conv_b, w_down
):
    groups, n, tps = sizes
    tokens, width = resid.shape
    cols = out_proj.shape[1]
    depth, hidden = w_gate.shape
    part = parts_of(hidden)[0]
    vmem = pl.BlockSpec(memory_space=pltpu.VMEM)
    hbm = pl.BlockSpec(memory_space=pl.ANY)
    smem = pl.BlockSpec(memory_space=pltpu.SMEM)
    dma = pltpu.SemaphoreType.DMA
    block = (tokens, cols)
    return pl.pallas_call(
        functools.partial(layer_kernel, sizes),
        out_shape=jax.ShapeDtypeStruct((tokens, cols), BF16),
        in_specs=[hbm] * 3 + [smem, hbm, hbm, vmem, hbm, hbm, vmem, vmem, hbm],
        out_specs=vmem,
        scratch_shapes=[
            pltpu.VMEM(queries.shape, BF16),
            pltpu.VMEM((2, tokens + 2 * WINDOW, HD), BF16),
            pltpu.VMEM(resid.shape, BF16),
            pltpu.VMEM((tps,) + out_proj.shape, BF16),
            pltpu.VMEM((tps,) + queries.shape, BF16),
            pltpu.VMEM((tokens // 2, width), F32),
            pltpu.VMEM((2 * tokens + 2 * EDGE, width), BF16),
            pltpu.VMEM((n, depth, part), BF16),
            pltpu.VMEM((n, depth, part), BF16),
            pltpu.VMEM((n, part, cols), BF16),
            pltpu.VMEM((2 * tokens + 2 * EDGE, part), F32),
            pltpu.VMEM((2 * tokens, part), F32),
            pltpu.VMEM((2 * tokens, part), F32),
            pltpu.VMEM((2 * tokens, part), BF16),
            pltpu.VMEM((tps, 2 * tokens, cols), BF16),
            pltpu.VMEM((2,) + block, BF16),
            pltpu.VMEM((2, 2, tokens // 2, cols), BF16),
            pltpu.VMEM(block, BF16),
            pltpu.VMEM((2, tokens // 2, cols), BF16),
            pltpu.VMEM(block, BF16),
            pltpu.VMEM(block, BF16),
            pltpu.VMEM(block, BF16),
            dma((8,)), dma((2, 2)), dma((2, 2)),
            dma((3, 4, PIECES)), dma((3, 3, PIECES)), dma((3, 3, PIECES)), dma((3, 3, PIECES)),
            dma((3,)), dma((3,)), dma((3,)), dma((3,)), dma((4, PIECES)), dma((4, PIECES)), dma((2,)), dma((1,)),
            dma((3,)), dma((3,)),
            dma((2, SPLIT)), dma((2, SPLIT)), dma((2, 2, SPLIT)), dma((2, 2, SPLIT)),
            dma((2, SPLIT)), dma((2, SPLIT)), dma((2, SPLIT)), dma((2, SPLIT)),
            dma((2, SPLIT)), dma((2, SPLIT)), dma((SPLIT,)), dma((SPLIT,)),
        ],
        compiler_params=pltpu.CompilerParams(
            collective_id=0, has_side_effects=True, vmem_limit_bytes=67043328
        ),
    )(queries, keys, values, sink, resid, out_proj, norm_gain[None], w_gate, w_up, conv_w, conv_b.reshape(hidden // 128, 128), w_down)


def fits_kernel(sizes, args):
    groups, n, tps = sizes
    queries, resid, out_proj, w_gate, w_down = args[0], args[4], args[5], args[7], args[11]
    share = groups * PIECES
    weights = 3 * 2 * n * w_gate.shape[0] * w_gate.shape[1]
    return (
        n == 4
        and tps == 4
        and groups == 2
        and w_down.shape[1] == out_proj.shape[1]
        and w_gate.shape[0] % max(share * EDGE, 128) == 0
        and w_down.shape[1] % (groups * SPLIT * 128) == 0
        and w_gate.shape[1] % 768 == 0
        and resid.shape[0] % (4 * WINDOW) == 0
        and weights <= 20 * 2 ** 20
    )


def run_shards(sizes, *args):
    if fits_kernel(sizes, args):
        return kernel_shards(sizes, *args)
    return shards(*args)


def solution(mesh):
    sizes = tuple(mesh.shape[axis] for axis in ("grp", "sp", "tp"))
    return jax.shard_map(
        functools.partial(run_shards, sizes),
        mesh=mesh,
        in_specs=(
            P(("grp", "sp"), "tp"),
            P(("grp", "sp"), None),
            P(("grp", "sp"), None),
            P("tp"),
            P(("grp", "sp"), None),
            P(None, "tp"),
            P(),
            P("sp", "tp"),
            P("sp", "tp"),
            P(None, "tp"),
            P("tp"),
            P("tp", "sp"),
        ),
        out_specs=P(("grp", "sp"), "tp"),
        check_vma=False,
    )
```

```python
import functools

import jax
import jax.numpy as jnp
from jax import lax
from jax.experimental import pallas as pl
from jax.experimental.pallas import tpu as pltpu
from jax.sharding import PartitionSpec as P

H = 8
KVH = 2
HD = 128
WINDOW = 128
CONV = 3


def with_halo(cells, sides, width):
    for axis, dim in sides:
        count = lax.axis_size(axis)
        ends = count - 1
        head = lax.slice_in_dim(cells, 0, width, axis=dim)
        tail = lax.slice_in_dim(cells, cells.shape[dim] - width, cells.shape[dim], axis=dim)
        cells = jnp.concatenate(
            [
                lax.ppermute(tail, axis, [(i, (i + 1) % count) for i in range(ends)]),
                cells,
                lax.ppermute(head, axis, [((i + 1) % count, i) for i in range(ends)]),
            ],
            axis=dim,
        )
    return cells


def shards(
    queries, keys, values, sink, resid, out_proj, norm_gain, w_gate, w_up, conv_w, conv_b, w_down
):
    tokens = queries.shape[0]
    width = resid.shape[1]
    heads_here = sink.shape[0]
    group = H // KVH
    scale = HD ** (-0.5)
    first_head = lax.axis_index("tp") * heads_here
    kv_head = first_head // group
    own_keys = lax.dynamic_slice_in_dim(keys, kv_head * HD, HD, 1)
    own_values = lax.dynamic_slice_in_dim(values, kv_head * HD, HD, 1)
    extended = with_halo(jnp.stack([own_keys, own_values]), (("sp", 1),), WINDOW)
    ext_keys = extended[0]
    ext_values = extended[1]
    span = tokens + 2 * WINDOW
    q_heads = queries.reshape(tokens, heads_here, HD)
    scores = (
        jnp.einsum("qhd,kd->hqk", q_heads, ext_keys, preferred_element_type=jnp.float32) * scale
    )
    offset = lax.axis_index("sp") * tokens
    q_pos = offset + jnp.arange(tokens, dtype=jnp.int32)[:, None]
    k_pos = offset - WINDOW + jnp.arange(span, dtype=jnp.int32)[None, :]
    seq_total = tokens * lax.axis_size("sp")
    valid = (jnp.abs(q_pos - k_pos) <= WINDOW) & (k_pos >= 0) & (k_pos < seq_total)
    scores = jnp.where(valid[None], scores, jnp.float32(-1e30))
    sink_col = sink[:, None]
    top = jnp.maximum(jnp.max(scores, axis=-1), sink_col)
    expo = jnp.exp(scores - top[..., None])
    total = jnp.sum(expo, axis=-1) + jnp.exp(sink_col - top)
    weights = (expo / total[..., None]).astype(jnp.bfloat16)
    heads_out = jnp.einsum("hqk,kd->qhd", weights, ext_values, preferred_element_type=jnp.float32)
    heads_out = heads_out.astype(jnp.bfloat16).reshape(tokens, heads_here * HD)
    all_heads = lax.all_gather(heads_out, "tp", axis=1, tiled=True)
    cols = width // lax.axis_size("tp")
    col_start = lax.axis_index("tp") * cols
    full_proj = lax.all_gather(out_proj, "tp", axis=1, tiled=True)
    summed = resid.astype(jnp.float32) + jnp.dot(
        all_heads, full_proj, preferred_element_type=jnp.float32
    )
    mean = jnp.mean(summed, axis=-1, keepdims=True)
    msq = jnp.mean(summed * summed, axis=-1, keepdims=True)
    normed_full = ((summed - mean) * lax.rsqrt(msq - mean * mean + 1e-05) * norm_gain).astype(
        jnp.bfloat16
    )
    normed_own = lax.dynamic_slice_in_dim(normed_full, col_start, cols, 1)
    gate_acc = jnp.dot(
        normed_full,
        lax.all_gather(w_gate, "sp", axis=0, tiled=True),
        preferred_element_type=jnp.float32,
    )
    up_acc = jnp.dot(
        normed_full,
        lax.all_gather(w_up, "sp", axis=0, tiled=True),
        preferred_element_type=jnp.float32,
    )
    gate_pre = gate_acc.astype(jnp.bfloat16)
    up_part = up_acc.astype(jnp.bfloat16)
    padded = with_halo(gate_pre, (("sp", 0),), CONV // 2)
    conv = conv_b
    for tap in range(CONV):
        conv = conv + padded[tap : tap + tokens].astype(jnp.float32) * conv_w[tap]
    act = (jax.nn.silu(conv) * up_part.astype(jnp.float32)).astype(jnp.bfloat16)
    terms = jnp.dot(
        act, lax.all_gather(w_down, "sp", axis=1, tiled=True), preferred_element_type=jnp.float32
    )
    ffn_own = lax.psum_scatter(
        terms.astype(jnp.bfloat16), "tp", scatter_dimension=1, tiled=True
    ).astype(jnp.float32)
    return (normed_own.astype(jnp.float32) + ffn_own).astype(jnp.bfloat16)


EDGE = 16
SPLIT = 2
PIECES = 4
BF16 = jnp.bfloat16
F32 = jnp.float32


def parts_of(hidden):
    return hidden * 2 // 3, hidden // 3


def layer_kernel(
    sizes,
    q_hbm, k_hbm, v_hbm, sink_ref, resid_hbm, proj_hbm, gain_ref, wg_hbm, wu_hbm, cw_ref, cb_ref, wd_hbm,
    out_ref,
    q_ref, kv_ext, resid_ref, proj_all, mixed, summed, normed, wg_all, wu_all, wd_all, gate, up, silu, act,
    terms, near_in, pair_in, far_in, mid_in, over_in, ret_out, ret_in,
    local_sem, halo_send, halo_recv, z_send, z_recv, y_send, y_recv,
    proj_send, proj_recv, mix_send, mix_recv, norm_send, norm_recv, edge_send, edge_recv, row_send, row_recv,
    near_send, near_recv, pair_send, pair_recv, far_send, far_recv, mid_send, mid_recv, over_send, over_recv, ret_send, ret_recv,
):
    groups, n, tps = sizes
    g = lax.axis_index("grp")
    s = lax.axis_index("sp")
    t = lax.axis_index("tp")
    tokens, width = resid_hbm.shape
    heads_here = sink_ref.shape[0]
    cols = proj_hbm.shape[1]
    depth = wg_hbm.shape[0]
    hidden = wg_hbm.shape[1]
    parts = parts_of(hidden)
    starts = (0, parts[0])
    rows2 = 2 * tokens
    has_left, has_right = s > 0, s < n - 1
    inner = has_left & has_right
    outer = jnp.logical_not(inner)
    low = s < n // 2
    mate = s + 1 - 2 * lax.rem(s, 2)
    mirror = n - 1 - s
    beyond = n - 1 - mate
    role = 1 - jnp.where(inner, 1, 0)
    hidden_at = pl.multiple_of(role * parts[0], 128)
    my_part = jnp.where(inner, parts[0], parts[1])
    base = pl.multiple_of(EDGE + lax.rem(s, 2) * tokens, EDGE)
    other_base = pl.multiple_of(EDGE + (1 - lax.rem(s, 2)) * tokens, EDGE)
    core = lax.rem(t, 2)
    core_peer = t + 1 - 2 * core
    chip_peer = lax.rem(t + 2, tps)
    own = (wg_hbm, wu_hbm, wd_hbm)
    full = (wg_all, wu_all, wd_all)
    OWN = n - 1

    def remote(src, dst, send, recv, to):
        return pltpu.make_async_remote_copy(
            src_ref=src, dst_ref=dst, send_sem=send, recv_sem=recv,
            device_id=to, device_id_type=pl.DeviceIdType.MESH,
        )

    kv_head = (t * heads_here) // (H // KVH)
    kv_cols = pl.ds(pl.multiple_of(kv_head * HD, HD), HD)

    def by_role(fn):
        for r, here in enumerate((inner, outer)):
            @pl.when(here)
            def _():
                fn(r)

    def local(i, r=0):
        here, mine = pl.ds(starts[r], parts[r]), pl.ds(0, parts[r])
        src, dst = (
            (q_hbm, q_ref),
            (k_hbm.at[:, kv_cols], kv_ext.at[0, pl.ds(WINDOW, tokens)]),
            (v_hbm.at[:, kv_cols], kv_ext.at[1, pl.ds(WINDOW, tokens)]),
            (proj_hbm, proj_all.at[t]),
            (resid_hbm, resid_ref),
            (wg_hbm.at[:, here], wg_all.at[OWN, :, mine]),
            (wu_hbm.at[:, here], wu_all.at[OWN, :, mine]),
            (wd_hbm.at[here], wd_all.at[OWN, mine]),
        )[i]
        return pltpu.make_async_copy(src, dst, local_sem.at[i])

    for i in range(5):
        local(i).start()
    by_role(lambda r: [local(i, r).start() for i in (5, 6, 7)])

    barrier = pltpu.get_barrier_semaphore()

    def greet(to):
        pl.semaphore_signal(barrier, inc=1, device_id=to, device_id_type=pl.DeviceIdType.MESH)

    for j in range(1, n):
        greet({"sp": lax.rem(s + j, n)})
    for j in range(1, groups):
        greet({"grp": lax.rem(g + j, groups)})
    for j in range(1, tps):
        greet({"tp": lax.rem(t + j, tps)})
    for j in range(2):
        greet({"sp": mate, "tp": lax.rem(t - core + 2 + j, tps)})
    pl.semaphore_wait(barrier, n - 1 + groups - 1 + tps - 1 + 2)

    def halo_copy(i, to_left):
        ref = (k_hbm, v_hbm)[i]
        if to_left:
            return remote(ref.at[pl.ds(0, WINDOW), kv_cols], kv_ext.at[i, pl.ds(WINDOW + tokens, WINDOW)],
                          halo_send.at[i, 0], halo_recv.at[i, 0], {"sp": s - 1})
        return remote(ref.at[pl.ds(tokens - WINDOW, WINDOW), kv_cols], kv_ext.at[i, pl.ds(0, WINDOW)],
                      halo_send.at[i, 1], halo_recv.at[i, 1], {"sp": s + 1})

    deep = PIECES // SPLIT

    def window(m, of, c, first, count):
        if m < 2:
            step = depth // (groups * PIECES)
            return pl.ds(pl.multiple_of((of * PIECES + c) * step, EDGE), step), pl.ds(first, count)
        step = cols // (groups * SPLIT)
        at = pl.multiple_of(((c // deep) * groups + of) * step, 128)
        return pl.ds(first + (c % deep) * (count // deep), count // deep), pl.ds(at, step)

    def source(m, r, of, c):
        return own[m].at[window(m, of, c, starts[r], parts[r])]

    def place(m, slot, r, of, c):
        return full[m].at[(slot,) + window(m, of, c, 0, parts[r])]

    IN_ACROSS, IN_BEYOND, IN_MATE, IN_RELAY, OUT_MATE, OUT_MIRROR, OUT_REST = range(7)

    def ship(kind, m, c):
        slot, to, lane = {
            IN_ACROSS: (1, mirror, 0),
            IN_BEYOND: (1, beyond, 1),
            IN_MATE: (0, mate, 2),
            IN_RELAY: (2, mirror, 3),
            OUT_MATE: (0, mate, 0),
            OUT_MIRROR: (2, mirror, 1),
            OUT_REST: (0, mate, 2),
        }[kind]
        r = 0 if kind in (IN_ACROSS, IN_RELAY, OUT_MATE, OUT_REST) else 1
        of = 1 - g if kind == OUT_REST else g
        src = place(m, 0, r, of, c) if kind == IN_RELAY else source(m, r, of, c)
        arrive = y_recv.at[m, slot, c] if kind == OUT_REST else z_recv.at[m, slot, c]
        return remote(src, place(m, slot, r, of, c), z_send.at[m, lane], arrive, {"sp": to})

    def ship_all(kind, m):
        for c in range(PIECES):
            ship(kind, m, c).start()

    def direct(m, slot, r):
        return r == 0 and m == 2 and isinstance(slot, int) and slot == 0

    def cross(m, slot, r, c):
        return remote(place(m, slot, r, g, c), place(m, slot, r, g, c), y_send.at[m, slot], y_recv.at[m, slot, c],
                      {"grp": 1 - g})

    def share_of(m, r):
        if m < 2:
            return full[m].at[0, pl.ds(0, depth // groups), pl.ds(0, parts[r])]
        return full[m].at[0, pl.ds(0, parts[r]), pl.ds(0, cols // groups)]

    def shipped(kind, m):
        r = 0 if kind in (IN_ACROSS, IN_RELAY, OUT_MATE, OUT_REST) else 1
        lane = {IN_BEYOND: 1, IN_MATE: 2, IN_RELAY: 3, OUT_MIRROR: 1, OUT_REST: 2}.get(kind, 0)
        ref = share_of(m, r)
        remote(ref, ref, z_send.at[m, lane], z_recv.at[m, 0, 0], {"sp": mate}).wait_send()

    def crossed(m, slot, r):
        ref = share_of(m, r)
        remote(ref, ref, y_send.at[m, slot], y_recv.at[m, slot, 0], {"grp": 1 - g}).wait_send()

    def pieces_of(m, cs):
        return range(PIECES) if m < 2 else [c * deep + d for c in cs for d in range(deep)]

    def take(m, slot, cs=range(SPLIT)):
        def run(r):
            for c in pieces_of(m, cs):
                remote(place(m, slot, r, g, c), place(m, slot, r, g, c), z_send.at[m, 0], z_recv.at[m, slot, c],
                       {"sp": mate}).wait_recv()
                if not direct(m, slot, r):
                    cross(m, slot, r, c).start()
                if isinstance(slot, int) and slot == 0 and r == 0:
                    ship(IN_RELAY, m, c).start()

        by_role(run)

    def have(m, slot, cs=range(SPLIT)):
        def run(r):
            for c in pieces_of(m, cs):
                ref = place(m, slot, r, 1 - g, c)
                remote(ref, ref, y_send.at[m, slot], y_recv.at[m, slot, c], {"grp": 1 - g}).wait_recv()

        by_role(run)

    def spread(src, ref, send, recv, step):
        origin = (t, t, chip_peer)[step]
        return remote(src if step < 2 else ref.at[origin], ref.at[origin], send.at[step], recv.at[step],
                      {"tp": (core_peer, chip_peer, core_peer)[step]})

    def spread_arrival(src, ref, send, recv, step):
        origin = (core_peer, chip_peer, lax.rem(core_peer + 2, tps))[step]
        return remote(src, ref.at[origin], send.at[step], recv.at[step],
                      {"tp": (core_peer, chip_peer, core_peer)[step]})

    proj_args = (proj_hbm, proj_all, proj_send, proj_recv)
    mix_args = (mixed.at[t], mixed, mix_send, mix_recv)

    @pl.when(has_left)
    def _():
        for i in range(2):
            halo_copy(i, True).start()

    @pl.when(has_right)
    def _():
        for i in range(2):
            halo_copy(i, False).start()

    @pl.when(outer)
    def _():
        ship_all(OUT_MATE, 0)
        ship_all(OUT_MATE, 1)
        ship_all(OUT_MIRROR, 0)

    @pl.when(inner)
    def _():
        ship_all(IN_ACROSS, 0)
        ship_all(IN_BEYOND, 0)
        ship_all(IN_MATE, 0)
        ship_all(IN_MATE, 1)

    for step in (1, 0):
        spread(*proj_args, step).start()

    @pl.when(jnp.logical_not(has_left))
    def _():
        kv_ext[:, pl.ds(0, WINDOW), :] = jnp.zeros((2, WINDOW, HD), BF16)

    @pl.when(jnp.logical_not(has_right))
    def _():
        kv_ext[:, pl.ds(WINDOW + tokens, WINDOW), :] = jnp.zeros((2, WINDOW, HD), BF16)

    for i in range(3):
        local(i).wait()

    @pl.when(has_right)
    def _():
        for i in range(2):
            halo_copy(i, True).wait_recv()

    @pl.when(has_left)
    def _():
        for i in range(2):
            halo_copy(i, False).wait_recv()

    span = 3 * WINDOW
    seq_total = tokens * n

    @pl.loop(0, tokens // WINDOW)
    def _(b):
        start = pl.multiple_of(b * WINDOW, WINDOW)
        row = lax.broadcasted_iota(jnp.int32, (WINDOW, span), 0)
        col = lax.broadcasted_iota(jnp.int32, (WINDOW, span), 1)
        k_pos = s * tokens + start - WINDOW + col
        valid = (jnp.abs(row + WINDOW - col) <= WINDOW) & (k_pos >= 0) & (k_pos < seq_total)
        kb = kv_ext[0, pl.ds(start, span), :]
        vb = kv_ext[1, pl.ds(start, span), :]
        for h in range(heads_here):
            qb = q_ref[pl.ds(start, WINDOW), h * HD:(h + 1) * HD]
            sc = lax.dot_general(qb, kb, (((1,), (1,)), ((), ())), preferred_element_type=F32) * (HD ** -0.5)
            sc = jnp.where(valid, sc, F32(-1e30))
            sink = sink_ref[h]
            top = jnp.maximum(jnp.max(sc, axis=-1, keepdims=True), sink)
            expo = jnp.exp(sc - top)
            total = jnp.sum(expo, axis=-1, keepdims=True) + jnp.exp(sink - top)
            weights = (expo / total).astype(BF16)
            o = jnp.dot(weights, vb, preferred_element_type=F32)
            mixed[t, pl.ds(start, WINDOW), h * HD:(h + 1) * HD] = o.astype(BF16)

    for step in (1, 0):
        spread(*mix_args, step).start()

    take(0, 0)

    @pl.when(inner)
    def _():
        take(0, 1)

    for args in (proj_args, mix_args):
        spread_arrival(*args, 1).wait_recv()
        spread(*args, 2).start()
    for args in (proj_args, mix_args):
        for step in (0, 2):
            spread_arrival(*args, step).wait_recv()

    @pl.when(inner)
    def _():
        take(1, 0)

    for i in (3, 4):
        local(i).wait()
    lanes = mixed.shape[2]
    block = summed.shape[0]
    strip = 64

    @pl.loop(0, tokens // block)
    def _(b):
        rows = pl.ds(pl.multiple_of(b * block, block), block)

        @pl.loop(0, tps)
        def _(i):
            at = pl.ds(pl.multiple_of(i * cols, 128), cols)
            prod = jnp.dot(mixed[0, rows, :], proj_all[i, pl.ds(0, lanes), :], preferred_element_type=F32)
            for u in range(1, tps):
                prod += jnp.dot(mixed[u, rows, :], proj_all[i, pl.ds(u * lanes, lanes), :],
                                preferred_element_type=F32)
            summed[:, at] = resid_ref[rows, at].astype(F32) + prod

        @pl.loop(0, block // strip)
        def _(i):
            at = pl.multiple_of(i * strip, strip)
            x = summed[pl.ds(at, strip), :]
            mean = jnp.mean(x, axis=-1, keepdims=True)
            msq = jnp.mean(x * x, axis=-1, keepdims=True)
            normed[pl.ds(pl.multiple_of(base + b * block + at, EDGE), strip), :] = (
                (x - mean) * lax.rsqrt(msq - mean * mean + 1e-05) * gain_ref[...]
            ).astype(BF16)

    my_cols = pl.ds(pl.multiple_of(t * cols, 128), cols)

    def norm_part(first, col, c):
        step = tokens // PIECES
        return normed.at[pl.ds(pl.multiple_of(first + c * step, EDGE), step),
                         pl.ds(pl.multiple_of(col * cols, 128), cols)]

    def norm_copy(i, c, arrival=False):
        first = base if i == 0 and not arrival else other_base
        col = (t, t, t, chip_peer)[i] if not arrival else (t, chip_peer, core_peer, lax.rem(core_peer + 2, tps))[i]
        to = ({"sp": mate}, {"tp": chip_peer}, {"tp": core_peer}, {"tp": core_peer})[i]
        ref = norm_part(first, col, c)
        return remote(ref, ref, norm_send.at[i], norm_recv.at[i, c], to)

    edge_from = pl.ds(pl.multiple_of(base + jnp.where(low, tokens - EDGE, 0), EDGE), EDGE)
    edge_over = pl.ds(pl.multiple_of(jnp.where(low, 0, EDGE + rows2), EDGE), EDGE)
    edge_here = pl.ds(pl.multiple_of(jnp.where(low, EDGE + rows2, 0), EDGE), EDGE)

    def edge_copy(i):
        return remote(normed.at[edge_from, my_cols], normed.at[edge_over, my_cols], edge_send.at[i],
                      edge_recv.at[0], {"sp": (mirror, beyond)[i]})

    def edge_arrival():
        ref = normed.at[edge_here, my_cols]
        return remote(ref, ref, edge_send.at[0], edge_recv.at[0], {"sp": mirror})

    def row_copy(j, arrival=False):
        col = lax.rem(t + tps - j, tps) if arrival else t
        ref = normed.at[edge_here, pl.ds(pl.multiple_of(col * cols, 128), cols)]
        return remote(ref, ref, row_send.at[j - 1], row_recv.at[j - 1], {"tp": lax.rem(t + j, tps)})

    tile = 256

    def source_of(slot):
        return (mate, jnp.where(low, n // 2, n // 2 - 1), jnp.where(low, n - 1, 0), s)[slot]

    with_edge = pl.ds(pl.multiple_of(jnp.where(low, EDGE, 0), EDGE), rows2 + EDGE)
    both = pl.ds(EDGE, rows2)

    def gate_of(slot):
        if slot != OWN:
            have(0, slot)
        k = pl.ds(pl.multiple_of(source_of(slot) * depth, 128), depth)

        @pl.loop(0, my_part // tile)
        def _(i):
            at = pl.ds(pl.multiple_of(i * tile, 128), tile)
            ga = jnp.dot(normed[with_edge, k], wg_all[slot, :, at], preferred_element_type=F32)
            gate[with_edge, at] = ga if slot == OWN else gate[with_edge, at] + ga

    def up_of(slot, last=False):
        if slot != OWN:
            have(1, slot)
        k = pl.ds(pl.multiple_of(source_of(slot) * depth, 128), depth)

        @pl.loop(0, my_part // tile)
        def _(i):
            at = pl.ds(pl.multiple_of(i * tile, 128), tile)
            ub = jnp.dot(normed[both, k], wu_all[slot, :, at], preferred_element_type=F32)
            if slot != OWN:
                ub = up[:, at] + ub
            if last:
                act[:, at] = (silu[:, at] * ub.astype(BF16).astype(F32)).astype(BF16)
            else:
                up[:, at] = ub

    @pl.when(inner)
    def _():
        for i in range(2):
            edge_copy(i).start()

    for c in range(PIECES):
        norm_copy(0, c).start()

    @pl.when(outer)
    def _():
        ship_all(OUT_MIRROR, 1)
        ship_all(OUT_MATE, 2)
        ship_all(OUT_REST, 2)
        take(0, 1)
        take(1, 0)

    @pl.when(inner)
    def _():
        ship_all(IN_ACROSS, 1)
        ship_all(IN_BEYOND, 1)
        ship_all(IN_MATE, 2)
        ship_all(IN_ACROSS, 2)
        ship_all(IN_BEYOND, 2)

    by_role(lambda r: [local(i, r).wait() for i in (5, 6, 7)])

    take(0, 2)

    @pl.when(inner)
    def _():
        take(1, 2)

    for c in range(PIECES):
        norm_copy(0, c, True).wait_recv()
        norm_copy(1, c).start()
        norm_copy(2, c).start()
    edge_arrival().wait_recv()
    for j in range(1, tps):
        row_copy(j).start()

    for c in range(PIECES):
        norm_copy(1, c, True).wait_recv()
        norm_copy(3, c).start()

    @pl.when(outer)
    def _():
        take(1, 2)

    for c in range(PIECES):
        norm_copy(2, c, True).wait_recv()
        norm_copy(3, c, True).wait_recv()
    for j in range(1, tps):
        row_copy(j, True).wait_recv()
    gate_of(OWN)
    gate_of(0)
    gate_of(2)
    gate_of(1)

    @pl.when(inner)
    def _():
        take(1, 1)

    @pl.when(low)
    def _():
        gate[0:EDGE, :] = jnp.zeros((EDGE, parts[0]), F32)

    @pl.when(jnp.logical_not(low))
    def _():
        gate[EDGE + rows2:, :] = jnp.zeros((EDGE, parts[0]), F32)

    @pl.loop(0, my_part // 128)
    def _(i):
        at = pl.ds(pl.multiple_of(i * 128, 128), 128)
        ch = pl.ds(pl.multiple_of(hidden_at + i * 128, 128), 128)
        gate[:, at] = gate[:, at].astype(BF16).astype(F32)
        conv = cb_ref[pl.ds(role * (parts[0] // 128) + i, 1), :]
        for tap in range(CONV):
            conv = conv + gate[pl.ds(EDGE - CONV // 2 + tap, rows2), at] * cw_ref[tap:tap + 1, ch]
        silu[:, at] = conv / (1.0 + jnp.exp(-conv))

    up_of(OWN)
    up_of(0)
    up_of(2)

    @pl.when(outer)
    def _():
        ship_all(OUT_MIRROR, 2)
        take(1, 1)

    take(2, 0)

    up_of(1, last=True)

    @pl.when(inner)
    def _():
        take(2, 1, (0,))

    half_rows = tokens // 2
    wide = cols // SPLIT
    far_first = (1 - t // 2) * 2

    def is_far(p):
        return (p // 2) != (t // 2)

    def rows_of(i):
        return pl.ds(pl.multiple_of((base if i else other_base) - EDGE, tokens), tokens)

    def half_of(i, c):
        first = (base if i else other_base) - EDGE + c * half_rows
        return pl.ds(pl.multiple_of(first, half_rows), half_rows)

    def half_rows_of(c):
        return pl.ds(pl.multiple_of(c * half_rows, half_rows), half_rows)

    def block_of(c):
        return pl.ds(c * wide, wide)

    def near_copy(i, c):
        return remote(terms.at[core_peer, rows_of(i), block_of(c)], near_in.at[i, :, block_of(c)],
                      near_send.at[i, c], near_recv.at[i, c], {"tp": core_peer})

    def pair_copy(p, i, c):
        q = lax.rem(p, 2)
        return remote(terms.at[p, half_of(i, 1 - core), block_of(c)], pair_in.at[q, i, :, block_of(c)],
                      pair_send.at[q, i, c], pair_recv.at[q, i, c], {"tp": core_peer})

    def mid_copy(p, c):
        q = lax.rem(p, 2)
        return remote(terms.at[p, half_of(0, core), block_of(c)], mid_in.at[q, :, block_of(c)],
                      mid_send.at[q, c], mid_recv.at[q, c], {"sp": mate})

    def far_copy(p, c):
        return remote(terms.at[p, half_of(1, core), block_of(c)], far_in.at[half_rows_of(core), block_of(c)],
                      far_send.at[lax.rem(p, 2), c], far_recv.at[core, c], {"tp": p})

    def over_copy(slot, c):
        p = source_of(slot)
        to = {"tp": p} if slot == 1 else {"sp": mate, "tp": p}
        return remote(terms.at[p, half_of(0, core), block_of(c)], over_in.at[half_rows_of(core), block_of(c)],
                      over_send.at[slot - 1, c], over_recv.at[core, c], to)

    def over_arrival(h, c):
        ref = over_in.at[half_rows_of(h), block_of(c)]
        return remote(ref, ref, over_send.at[0, c], over_recv.at[h, c], {"sp": mate, "tp": far_first + h})

    def far_arrival(h, c):
        ref = far_in.at[half_rows_of(h), block_of(c)]
        return remote(ref, ref, far_send.at[h, c], far_recv.at[h, c], {"tp": far_first + h})

    def ret_copy(c):
        return remote(ret_out.at[:, block_of(c)], ret_in.at[:, block_of(c)], ret_send.at[c], ret_recv.at[c],
                      {"sp": mate})

    def down(slot, p, c, i):
        def run(r):
            w = wd_all[slot, 0:parts[r], block_of(c)]
            x = act[rows_of(i), 0:parts[r]]
            terms[p, rows_of(i), block_of(c)] = jnp.dot(x, w, preferred_element_type=F32).astype(BF16)

        by_role(run)

        @pl.when(p == core_peer)
        def _():
            near_copy(i, c).start()

        @pl.when(is_far(p))
        def _():
            pair_copy(p, i, c).start()

    def gather(p, c, late=None):
        for i in range(2):
            @pl.when(is_far(p))
            def _():
                pair_copy(p, i, c).wait_recv()
                rows = half_of(i, core)
                total = (terms[p, rows, block_of(c)].astype(F32)
                         + pair_in[lax.rem(p, 2), i, :, block_of(c)].astype(F32))
                terms[p, rows, block_of(c)] = total.astype(BF16)
                if i == 0 and late:
                    @pl.when(inner)
                    def _():
                        over_copy(late, c).start()

                    @pl.when(outer)
                    def _():
                        mid_copy(p, c).start()
                elif i == 0:
                    mid_copy(p, c).start()

        @pl.when((p == t) & outer if late == 1 else p == t)
        def _():
            near_copy(0, c).wait_recv()
            ret_out[:, block_of(c)] = (terms[t, rows_of(0), block_of(c)].astype(F32)
                                       + near_in[0, :, block_of(c)].astype(F32)).astype(BF16)
            ret_copy(c).start()

    def ret_late(c):
        @pl.when(inner & (t == source_of(1)))
        def _():
            near_copy(0, c).wait_recv()
            for h in range(2):
                over_arrival(h, c).wait_recv()
            ret_out[:, block_of(c)] = (terms[t, rows_of(0), block_of(c)].astype(F32)
                                       + near_in[0, :, block_of(c)].astype(F32)
                                       + over_in[:, block_of(c)].astype(F32)).astype(BF16)
            ret_copy(c).start()

    def send_far(p, c, last=False):
        if last:
            @pl.when(is_far(p))
            def _():
                far_copy(p, c).start()
            return

        @pl.when(is_far(p))
        def _():
            mid_copy(p, c).wait_recv()
            rows = half_of(1, core)
            total = terms[p, rows, block_of(c)].astype(F32) + mid_in[lax.rem(p, 2), :, block_of(c)].astype(F32)
            terms[p, rows, block_of(c)] = total.astype(BF16)
            far_copy(p, c).start()

    def finish(c):
        near_copy(1, c).wait_recv()
        at = pl.ds(pl.multiple_of(t * cols + c * wide, 128), wide)
        out = normed[pl.ds(base, tokens), at].astype(F32) + terms[t, rows_of(1), block_of(c)].astype(F32)
        out = out + near_in[1, :, block_of(c)].astype(F32)
        for h in range(2):
            far_arrival(h, c).wait_recv()
        out = out + far_in[:, block_of(c)].astype(F32)
        ret_copy(c).wait_recv()
        out = out + ret_in[:, block_of(c)].astype(F32)
        out_ref[:, block_of(c)] = out.astype(BF16)

        @pl.when(outer & (t == source_of(2)))
        def _():
            for h in range(2):
                over_arrival(h, c).wait_recv()
            out_ref[:, block_of(c)] = (out + over_in[:, block_of(c)].astype(F32)).astype(BF16)

    def downs(slot, p, c):
        for i in range(2):
            down(slot, p, c, i)

    def drain(ms):
        def run(r):
            for kind in ((IN_ACROSS, IN_BEYOND, IN_MATE, IN_RELAY), (OUT_MATE, OUT_MIRROR, OUT_REST))[r]:
                for m in ms:
                    if m == 2 or kind != OUT_REST:
                        shipped(kind, m)
            for m in ms:
                for slot in range(n - 1):
                    if not direct(m, slot, r):
                        crossed(m, slot, r)

        by_role(run)

    def drain_first():
        drain((0, 1))
        for i in range(4):
            ref = normed.at[pl.ds(EDGE, tokens), pl.ds(0, cols)]
            remote(ref, ref, norm_send.at[i], norm_recv.at[i, 0], {"sp": mate}).wait_send()
        for j in range(1, tps):
            row_copy(j).wait_send()

        @pl.when(inner)
        def _():
            for i in range(2):
                edge_copy(i).wait_send()

        @pl.when(has_left)
        def _():
            for i in range(2):
                halo_copy(i, True).wait_send()

        @pl.when(has_right)
        def _():
            for i in range(2):
                halo_copy(i, False).wait_send()

        for step in range(3):
            spread(*proj_args, step).wait_send()
            spread(*mix_args, step).wait_send()

    have(2, 0)
    early = [(jnp.where(inner, OWN, 0), jnp.where(inner, s, mate)), (jnp.where(inner, 0, OWN), jnp.where(inner, mate, s))]
    early = [(slot, p, c) for slot, p in early for c in range(SPLIT)]
    late = [(slot, source_of(slot), c) for slot in (1, 2) for c in range(SPLIT)]
    steps = early + late
    head = len(early)
    for at, (slot, p, c) in enumerate(steps):
        if at == head:
            gather(*steps[at - 1][1:])

            @pl.when(outer)
            def _():
                take(2, slot, (c,))

        if at >= head and at + 1 < len(steps):
            take(2, steps[at + 1][0], (steps[at + 1][2],))
        if at >= head:
            have(2, slot, (c,))
        downs(slot, p, c)
        if at >= head:
            gather(p, c, slot)
            if at in (head + 1, head + 2):
                ret_late(at - head - 1)
            send_far(*steps[at - head][1:])
            if at == head:
                drain_first()

            @pl.when(inner)
            def _():
                for late_at in {head: (), head + 1: (head,), head + 2: (head + 1, head + 2)}.get(at, (at,)):
                    send_far(*steps[late_at][1:])

            @pl.when(outer)
            def _():
                send_far(p, c, True)
        elif at:
            gather(*steps[at - 1][1:])

    drain((2,))
    for c in range(SPLIT):
        for i in range(2):
            near_copy(i, c).wait_send()
            for h in range(2):
                pair_copy(far_first + h, i, c).wait_send()

    def mids(here, owners):
        @pl.when(here)
        def _():
            for c in range(SPLIT):
                for p in owners:
                    @pl.when(is_far(p))
                    def _():
                        mid_copy(p, c).wait_send()

    mids(inner, [p for _, p, c in early if c == 0])
    mids(outer, [p for _, p, c in steps if c == 0])

    @pl.when(inner)
    def _():
        for slot in (1, 2):
            @pl.when(is_far(source_of(slot)))
            def _():
                for c in range(SPLIT):
                    over_copy(slot, c).wait_send()

    finish(0)
    ret_copy(0).wait_send()
    for h in range(2):
        far_copy(far_first + h, 0).wait_send()
    finish(1)
    ret_copy(1).wait_send()
    for h in range(2):
        far_copy(far_first + h, 1).wait_send()


def kernel_shards(
    sizes, queries, keys, values, sink, resid, out_proj, norm_gain, w_gate, w_up, conv_w, conv_b, w_down
):
    groups, n, tps = sizes
    tokens, width = resid.shape
    cols = out_proj.shape[1]
    depth, hidden = w_gate.shape
    part = parts_of(hidden)[0]
    vmem = pl.BlockSpec(memory_space=pltpu.VMEM)
    hbm = pl.BlockSpec(memory_space=pl.ANY)
    smem = pl.BlockSpec(memory_space=pltpu.SMEM)
    dma = pltpu.SemaphoreType.DMA
    block = (tokens, cols)
    return pl.pallas_call(
        functools.partial(layer_kernel, sizes),
        out_shape=jax.ShapeDtypeStruct((tokens, cols), BF16),
        in_specs=[hbm] * 3 + [smem, hbm, hbm, vmem, hbm, hbm, vmem, vmem, hbm],
        out_specs=vmem,
        scratch_shapes=[
            pltpu.VMEM(queries.shape, BF16),
            pltpu.VMEM((2, tokens + 2 * WINDOW, HD), BF16),
            pltpu.VMEM(resid.shape, BF16),
            pltpu.VMEM((tps,) + out_proj.shape, BF16),
            pltpu.VMEM((tps,) + queries.shape, BF16),
            pltpu.VMEM((tokens // 2, width), F32),
            pltpu.VMEM((2 * tokens + 2 * EDGE, width), BF16),
            pltpu.VMEM((n, depth, part), BF16),
            pltpu.VMEM((n, depth, part), BF16),
            pltpu.VMEM((n, part, cols), BF16),
            pltpu.VMEM((2 * tokens + 2 * EDGE, part), F32),
            pltpu.VMEM((2 * tokens, part), F32),
            pltpu.VMEM((2 * tokens, part), F32),
            pltpu.VMEM((2 * tokens, part), BF16),
            pltpu.VMEM((tps, 2 * tokens, cols), BF16),
            pltpu.VMEM((2,) + block, BF16),
            pltpu.VMEM((2, 2, tokens // 2, cols), BF16),
            pltpu.VMEM(block, BF16),
            pltpu.VMEM((2, tokens // 2, cols), BF16),
            pltpu.VMEM(block, BF16),
            pltpu.VMEM(block, BF16),
            pltpu.VMEM(block, BF16),
            dma((8,)), dma((2, 2)), dma((2, 2)),
            dma((3, 4)), dma((3, 3, PIECES)), dma((3, 3)), dma((3, 3, PIECES)),
            dma((3,)), dma((3,)), dma((3,)), dma((3,)), dma((4,)), dma((4, PIECES)), dma((2,)), dma((1,)),
            dma((3,)), dma((3,)),
            dma((2, SPLIT)), dma((2, SPLIT)), dma((2, 2, SPLIT)), dma((2, 2, SPLIT)),
            dma((2, SPLIT)), dma((2, SPLIT)), dma((2, SPLIT)), dma((2, SPLIT)),
            dma((2, SPLIT)), dma((2, SPLIT)), dma((SPLIT,)), dma((SPLIT,)),
        ],
        compiler_params=pltpu.CompilerParams(
            collective_id=0, has_side_effects=True, vmem_limit_bytes=67043328
        ),
    )(queries, keys, values, sink, resid, out_proj, norm_gain[None], w_gate, w_up, conv_w, conv_b.reshape(hidden // 128, 128), w_down)


def fits_kernel(sizes, args):
    groups, n, tps = sizes
    queries, resid, out_proj, w_gate, w_down = args[0], args[4], args[5], args[7], args[11]
    share = groups * PIECES
    weights = 3 * 2 * n * w_gate.shape[0] * w_gate.shape[1]
    return (
        n == 4
        and tps == 4
        and groups == 2
        and w_down.shape[1] == out_proj.shape[1]
        and w_gate.shape[0] % max(share * EDGE, 128) == 0
        and w_down.shape[1] % (groups * SPLIT * 128) == 0
        and w_gate.shape[1] % 768 == 0
        and resid.shape[0] % (4 * WINDOW) == 0
        and weights <= 20 * 2 ** 20
    )


def run_shards(sizes, *args):
    if fits_kernel(sizes, args):
        return kernel_shards(sizes, *args)
    return shards(*args)


def solution(mesh):
    sizes = tuple(mesh.shape[axis] for axis in ("grp", "sp", "tp"))
    return jax.shard_map(
        functools.partial(run_shards, sizes),
        mesh=mesh,
        in_specs=(
            P(("grp", "sp"), "tp"),
            P(("grp", "sp"), None),
            P(("grp", "sp"), None),
            P("tp"),
            P(("grp", "sp"), None),
            P(None, "tp"),
            P(),
            P("sp", "tp"),
            P("sp", "tp"),
            P(None, "tp"),
            P("tp"),
            P("tp", "sp"),
        ),
        out_specs=P(("grp", "sp"), "tp"),
        check_vma=False,
    )
```

```python
import functools

import jax
import jax.numpy as jnp
from jax import lax
from jax.experimental import pallas as pl
from jax.experimental.pallas import tpu as pltpu
from jax.sharding import PartitionSpec as P

H = 8
KVH = 2
HD = 128
WINDOW = 128
CONV = 3


def with_halo(cells, sides, width):
    for axis, dim in sides:
        count = lax.axis_size(axis)
        ends = count - 1
        head = lax.slice_in_dim(cells, 0, width, axis=dim)
        tail = lax.slice_in_dim(cells, cells.shape[dim] - width, cells.shape[dim], axis=dim)
        cells = jnp.concatenate(
            [
                lax.ppermute(tail, axis, [(i, (i + 1) % count) for i in range(ends)]),
                cells,
                lax.ppermute(head, axis, [((i + 1) % count, i) for i in range(ends)]),
            ],
            axis=dim,
        )
    return cells


def shards(
    queries, keys, values, sink, resid, out_proj, norm_gain, w_gate, w_up, conv_w, conv_b, w_down
):
    tokens = queries.shape[0]
    width = resid.shape[1]
    heads_here = sink.shape[0]
    group = H // KVH
    scale = HD ** (-0.5)
    first_head = lax.axis_index("tp") * heads_here
    kv_head = first_head // group
    own_keys = lax.dynamic_slice_in_dim(keys, kv_head * HD, HD, 1)
    own_values = lax.dynamic_slice_in_dim(values, kv_head * HD, HD, 1)
    extended = with_halo(jnp.stack([own_keys, own_values]), (("sp", 1),), WINDOW)
    ext_keys = extended[0]
    ext_values = extended[1]
    span = tokens + 2 * WINDOW
    q_heads = queries.reshape(tokens, heads_here, HD)
    scores = (
        jnp.einsum("qhd,kd->hqk", q_heads, ext_keys, preferred_element_type=jnp.float32) * scale
    )
    offset = lax.axis_index("sp") * tokens
    q_pos = offset + jnp.arange(tokens, dtype=jnp.int32)[:, None]
    k_pos = offset - WINDOW + jnp.arange(span, dtype=jnp.int32)[None, :]
    seq_total = tokens * lax.axis_size("sp")
    valid = (jnp.abs(q_pos - k_pos) <= WINDOW) & (k_pos >= 0) & (k_pos < seq_total)
    scores = jnp.where(valid[None], scores, jnp.float32(-1e30))
    sink_col = sink[:, None]
    top = jnp.maximum(jnp.max(scores, axis=-1), sink_col)
    expo = jnp.exp(scores - top[..., None])
    total = jnp.sum(expo, axis=-1) + jnp.exp(sink_col - top)
    weights = (expo / total[..., None]).astype(jnp.bfloat16)
    heads_out = jnp.einsum("hqk,kd->qhd", weights, ext_values, preferred_element_type=jnp.float32)
    heads_out = heads_out.astype(jnp.bfloat16).reshape(tokens, heads_here * HD)
    all_heads = lax.all_gather(heads_out, "tp", axis=1, tiled=True)
    cols = width // lax.axis_size("tp")
    col_start = lax.axis_index("tp") * cols
    full_proj = lax.all_gather(out_proj, "tp", axis=1, tiled=True)
    summed = resid.astype(jnp.float32) + jnp.dot(
        all_heads, full_proj, preferred_element_type=jnp.float32
    )
    mean = jnp.mean(summed, axis=-1, keepdims=True)
    msq = jnp.mean(summed * summed, axis=-1, keepdims=True)
    normed_full = ((summed - mean) * lax.rsqrt(msq - mean * mean + 1e-05) * norm_gain).astype(
        jnp.bfloat16
    )
    normed_own = lax.dynamic_slice_in_dim(normed_full, col_start, cols, 1)
    gate_acc = jnp.dot(
        normed_full,
        lax.all_gather(w_gate, "sp", axis=0, tiled=True),
        preferred_element_type=jnp.float32,
    )
    up_acc = jnp.dot(
        normed_full,
        lax.all_gather(w_up, "sp", axis=0, tiled=True),
        preferred_element_type=jnp.float32,
    )
    gate_pre = gate_acc.astype(jnp.bfloat16)
    up_part = up_acc.astype(jnp.bfloat16)
    padded = with_halo(gate_pre, (("sp", 0),), CONV // 2)
    conv = conv_b
    for tap in range(CONV):
        conv = conv + padded[tap : tap + tokens].astype(jnp.float32) * conv_w[tap]
    act = (jax.nn.silu(conv) * up_part.astype(jnp.float32)).astype(jnp.bfloat16)
    terms = jnp.dot(
        act, lax.all_gather(w_down, "sp", axis=1, tiled=True), preferred_element_type=jnp.float32
    )
    ffn_own = lax.psum_scatter(
        terms.astype(jnp.bfloat16), "tp", scatter_dimension=1, tiled=True
    ).astype(jnp.float32)
    return (normed_own.astype(jnp.float32) + ffn_own).astype(jnp.bfloat16)


EDGE = 16
SPLIT = 2
PIECES = 2
DEEP = 8
BF16 = jnp.bfloat16
F32 = jnp.float32


def parts_of(hidden):
    return hidden * 2 // 3, hidden // 3


def layer_kernel(
    sizes,
    q_hbm, k_hbm, v_hbm, sink_ref, resid_hbm, proj_hbm, gain_ref, wg_hbm, wu_hbm, cw_ref, cb_ref, wd_hbm,
    out_ref,
    q_ref, kv_ext, resid_ref, proj_all, mixed, summed, normed, wg_all, wu_all, wd_all, gate, up, silu, act,
    terms, near_in, pair_in, far_in, mid_in, over_in, ret_out, ret_in,
    local_sem, halo_send, halo_recv, z_send, z_recv, y_send, y_recv,
    proj_send, proj_recv, mix_send, mix_recv, norm_send, norm_recv, edge_send, edge_recv, row_send, row_recv,
    near_send, near_recv, pair_send, pair_recv, far_send, far_recv, mid_send, mid_recv, over_send, over_recv, ret_send, ret_recv,
):
    groups, n, tps = sizes
    g = lax.axis_index("grp")
    s = lax.axis_index("sp")
    t = lax.axis_index("tp")
    tokens, width = resid_hbm.shape
    heads_here = sink_ref.shape[0]
    cols = proj_hbm.shape[1]
    depth = wg_hbm.shape[0]
    hidden = wg_hbm.shape[1]
    parts = parts_of(hidden)
    starts = (0, parts[0])
    rows2 = 2 * tokens
    has_left, has_right = s > 0, s < n - 1
    inner = has_left & has_right
    outer = jnp.logical_not(inner)
    low = s < n // 2
    mate = s + 1 - 2 * lax.rem(s, 2)
    mirror = n - 1 - s
    beyond = n - 1 - mate
    role = 1 - jnp.where(inner, 1, 0)
    hidden_at = pl.multiple_of(role * parts[0], 128)
    my_part = jnp.where(inner, parts[0], parts[1])
    base = pl.multiple_of(EDGE + lax.rem(s, 2) * tokens, EDGE)
    other_base = pl.multiple_of(EDGE + (1 - lax.rem(s, 2)) * tokens, EDGE)
    core = lax.rem(t, 2)
    core_peer = t + 1 - 2 * core
    chip_peer = lax.rem(t + 2, tps)
    own = (wg_hbm, wu_hbm, wd_hbm)
    full = (wg_all, wu_all, wd_all)
    OWN = n - 1

    def remote(src, dst, send, recv, to):
        return pltpu.make_async_remote_copy(
            src_ref=src, dst_ref=dst, send_sem=send, recv_sem=recv,
            device_id=to, device_id_type=pl.DeviceIdType.MESH,
        )

    kv_head = (t * heads_here) // (H // KVH)
    kv_cols = pl.ds(pl.multiple_of(kv_head * HD, HD), HD)

    def by_role(fn):
        for r, here in enumerate((inner, outer)):
            @pl.when(here)
            def _():
                fn(r)

    def local(i, r=0):
        here, mine = pl.ds(starts[r], parts[r]), pl.ds(0, parts[r])
        src, dst = (
            (q_hbm, q_ref),
            (k_hbm.at[:, kv_cols], kv_ext.at[0, pl.ds(WINDOW, tokens)]),
            (v_hbm.at[:, kv_cols], kv_ext.at[1, pl.ds(WINDOW, tokens)]),
            (proj_hbm, proj_all.at[t]),
            (resid_hbm, resid_ref),
            (wg_hbm.at[:, here], wg_all.at[OWN, :, mine]),
            (wu_hbm.at[:, here], wu_all.at[OWN, :, mine]),
            (wd_hbm.at[here], wd_all.at[OWN, mine]),
        )[i]
        return pltpu.make_async_copy(src, dst, local_sem.at[i])

    for i in range(5):
        local(i).start()
    by_role(lambda r: [local(i, r).start() for i in (5, 6, 7)])

    barrier = pltpu.get_barrier_semaphore()

    def greet(to):
        pl.semaphore_signal(barrier, inc=1, device_id=to, device_id_type=pl.DeviceIdType.MESH)

    for j in range(1, n):
        greet({"sp": lax.rem(s + j, n)})
    for j in range(1, groups):
        greet({"grp": lax.rem(g + j, groups)})
    for j in range(1, tps):
        greet({"tp": lax.rem(t + j, tps)})
    for j in range(2):
        greet({"sp": mate, "tp": lax.rem(t - core + 2 + j, tps)})
    pl.semaphore_wait(barrier, n - 1 + groups - 1 + tps - 1 + 2)

    def halo_copy(i, to_left):
        ref = (k_hbm, v_hbm)[i]
        if to_left:
            return remote(ref.at[pl.ds(0, WINDOW), kv_cols], kv_ext.at[i, pl.ds(WINDOW + tokens, WINDOW)],
                          halo_send.at[i, 0], halo_recv.at[i, 0], {"sp": s - 1})
        return remote(ref.at[pl.ds(tokens - WINDOW, WINDOW), kv_cols], kv_ext.at[i, pl.ds(0, WINDOW)],
                      halo_send.at[i, 1], halo_recv.at[i, 1], {"sp": s + 1})

    deep = DEEP // SPLIT

    def count_of(m):
        return PIECES if m < 2 else DEEP

    def landing(sems, m, slot, c):
        return sems.at[(m * (n - 1) + slot) * PIECES + c if m < 2 else 2 * (n - 1) * PIECES + slot * DEEP + c]

    def window(m, of, c, first, count):
        if m < 2:
            step = depth // (groups * PIECES)
            return pl.ds(pl.multiple_of((of * PIECES + c) * step, EDGE), step), pl.ds(first, count)
        step = cols // (groups * SPLIT)
        at = pl.multiple_of(((c // deep) * groups + of) * step, 128)
        return pl.ds(first + (c % deep) * (count // deep), count // deep), pl.ds(at, step)

    def source(m, r, of, c):
        return own[m].at[window(m, of, c, starts[r], parts[r])]

    def place(m, slot, r, of, c):
        return full[m].at[(slot,) + window(m, of, c, 0, parts[r])]

    IN_ACROSS, IN_BEYOND, IN_MATE, IN_RELAY, OUT_MATE, OUT_MIRROR, OUT_REST = range(7)

    def ship(kind, m, c):
        slot, to, lane = {
            IN_ACROSS: (1, mirror, 0),
            IN_BEYOND: (1, beyond, 1),
            IN_MATE: (0, mate, 2),
            IN_RELAY: (2, mirror, 3),
            OUT_MATE: (0, mate, 0),
            OUT_MIRROR: (2, mirror, 1),
            OUT_REST: (0, mate, 2),
        }[kind]
        r = 0 if kind in (IN_ACROSS, IN_RELAY, OUT_MATE, OUT_REST) else 1
        of = 1 - g if kind == OUT_REST else g
        src = place(m, 0, r, of, c) if kind == IN_RELAY else source(m, r, of, c)
        arrive = landing(y_recv, m, slot, c) if kind == OUT_REST else landing(z_recv, m, slot, c)
        return remote(src, place(m, slot, r, of, c), z_send.at[m, lane], arrive, {"sp": to})

    def ship_all(kind, m):
        for c in range(count_of(m)):
            ship(kind, m, c).start()

    def direct(m, slot, r):
        return r == 0 and m == 2 and isinstance(slot, int) and slot == 0

    def cross(m, slot, r, c):
        return remote(place(m, slot, r, g, c), place(m, slot, r, g, c), y_send.at[m, slot], landing(y_recv, m, slot, c),
                      {"grp": 1 - g})

    def share_of(m, r):
        if m < 2:
            return full[m].at[0, pl.ds(0, depth // groups), pl.ds(0, parts[r])]
        return full[m].at[0, pl.ds(0, parts[r]), pl.ds(0, cols // groups)]

    def shipped(kind, m):
        r = 0 if kind in (IN_ACROSS, IN_RELAY, OUT_MATE, OUT_REST) else 1
        lane = {IN_BEYOND: 1, IN_MATE: 2, IN_RELAY: 3, OUT_MIRROR: 1, OUT_REST: 2}.get(kind, 0)
        ref = share_of(m, r)
        remote(ref, ref, z_send.at[m, lane], landing(z_recv, m, 0, 0), {"sp": mate}).wait_send()

    def crossed(m, slot, r):
        ref = share_of(m, r)
        remote(ref, ref, y_send.at[m, slot], landing(y_recv, m, slot, 0), {"grp": 1 - g}).wait_send()

    def pieces_of(m, cs):
        return range(PIECES) if m < 2 else [c * deep + d for c in cs for d in range(deep)]

    def take(m, slot, cs=range(SPLIT)):
        def run(r):
            for c in pieces_of(m, cs):
                remote(place(m, slot, r, g, c), place(m, slot, r, g, c), z_send.at[m, 0], landing(z_recv, m, slot, c),
                       {"sp": mate}).wait_recv()
                if not direct(m, slot, r):
                    cross(m, slot, r, c).start()
                if isinstance(slot, int) and slot == 0 and r == 0:
                    ship(IN_RELAY, m, c).start()

        by_role(run)

    def have(m, slot, cs=range(SPLIT)):
        def run(r):
            for c in pieces_of(m, cs):
                ref = place(m, slot, r, 1 - g, c)
                remote(ref, ref, y_send.at[m, slot], landing(y_recv, m, slot, c), {"grp": 1 - g}).wait_recv()

        by_role(run)

    def spread(src, ref, send, recv, step):
        origin = (t, t, chip_peer)[step]
        return remote(src if step < 2 else ref.at[origin], ref.at[origin], send.at[step], recv.at[step],
                      {"tp": (core_peer, chip_peer, core_peer)[step]})

    def spread_arrival(src, ref, send, recv, step):
        origin = (core_peer, chip_peer, lax.rem(core_peer + 2, tps))[step]
        return remote(src, ref.at[origin], send.at[step], recv.at[step],
                      {"tp": (core_peer, chip_peer, core_peer)[step]})

    proj_args = (proj_hbm, proj_all, proj_send, proj_recv)
    mix_args = (mixed.at[t], mixed, mix_send, mix_recv)

    @pl.when(has_left)
    def _():
        for i in range(2):
            halo_copy(i, True).start()

    @pl.when(has_right)
    def _():
        for i in range(2):
            halo_copy(i, False).start()

    @pl.when(outer)
    def _():
        ship_all(OUT_MATE, 0)
        ship_all(OUT_MATE, 1)
        ship_all(OUT_MIRROR, 0)

    @pl.when(inner)
    def _():
        ship_all(IN_ACROSS, 0)
        ship_all(IN_BEYOND, 0)
        ship_all(IN_MATE, 0)
        ship_all(IN_MATE, 1)

    for step in (1, 0):
        spread(*proj_args, step).start()

    @pl.when(jnp.logical_not(has_left))
    def _():
        kv_ext[:, pl.ds(0, WINDOW), :] = jnp.zeros((2, WINDOW, HD), BF16)

    @pl.when(jnp.logical_not(has_right))
    def _():
        kv_ext[:, pl.ds(WINDOW + tokens, WINDOW), :] = jnp.zeros((2, WINDOW, HD), BF16)

    for i in range(3):
        local(i).wait()

    @pl.when(has_right)
    def _():
        for i in range(2):
            halo_copy(i, True).wait_recv()

    @pl.when(has_left)
    def _():
        for i in range(2):
            halo_copy(i, False).wait_recv()

    span = 3 * WINDOW
    seq_total = tokens * n

    @pl.loop(0, tokens // WINDOW)
    def _(b):
        start = pl.multiple_of(b * WINDOW, WINDOW)
        row = lax.broadcasted_iota(jnp.int32, (WINDOW, span), 0)
        col = lax.broadcasted_iota(jnp.int32, (WINDOW, span), 1)
        k_pos = s * tokens + start - WINDOW + col
        valid = (jnp.abs(row + WINDOW - col) <= WINDOW) & (k_pos >= 0) & (k_pos < seq_total)
        kb = kv_ext[0, pl.ds(start, span), :]
        vb = kv_ext[1, pl.ds(start, span), :]
        for h in range(heads_here):
            qb = q_ref[pl.ds(start, WINDOW), h * HD:(h + 1) * HD]
            sc = lax.dot_general(qb, kb, (((1,), (1,)), ((), ())), preferred_element_type=F32) * (HD ** -0.5)
            sc = jnp.where(valid, sc, F32(-1e30))
            sink = sink_ref[h]
            top = jnp.maximum(jnp.max(sc, axis=-1, keepdims=True), sink)
            expo = jnp.exp(sc - top)
            total = jnp.sum(expo, axis=-1, keepdims=True) + jnp.exp(sink - top)
            weights = (expo / total).astype(BF16)
            o = jnp.dot(weights, vb, preferred_element_type=F32)
            mixed[t, pl.ds(start, WINDOW), h * HD:(h + 1) * HD] = o.astype(BF16)

    for step in (1, 0):
        spread(*mix_args, step).start()

    take(0, 0)

    @pl.when(inner)
    def _():
        take(0, 1)

    for args in (proj_args, mix_args):
        spread_arrival(*args, 1).wait_recv()
        spread(*args, 2).start()
    for args in (proj_args, mix_args):
        for step in (0, 2):
            spread_arrival(*args, step).wait_recv()

    @pl.when(inner)
    def _():
        take(1, 0)

    for i in (3, 4):
        local(i).wait()
    lanes = mixed.shape[2]
    block = summed.shape[0]
    strip = 64

    @pl.loop(0, tokens // block)
    def _(b):
        rows = pl.ds(pl.multiple_of(b * block, block), block)

        @pl.loop(0, tps)
        def _(i):
            at = pl.ds(pl.multiple_of(i * cols, 128), cols)
            prod = jnp.dot(mixed[0, rows, :], proj_all[i, pl.ds(0, lanes), :], preferred_element_type=F32)
            for u in range(1, tps):
                prod += jnp.dot(mixed[u, rows, :], proj_all[i, pl.ds(u * lanes, lanes), :],
                                preferred_element_type=F32)
            summed[:, at] = resid_ref[rows, at].astype(F32) + prod

        @pl.loop(0, block // strip)
        def _(i):
            at = pl.multiple_of(i * strip, strip)
            x = summed[pl.ds(at, strip), :]
            mean = jnp.mean(x, axis=-1, keepdims=True)
            msq = jnp.mean(x * x, axis=-1, keepdims=True)
            normed[pl.ds(pl.multiple_of(base + b * block + at, EDGE), strip), :] = (
                (x - mean) * lax.rsqrt(msq - mean * mean + 1e-05) * gain_ref[...]
            ).astype(BF16)

    my_cols = pl.ds(pl.multiple_of(t * cols, 128), cols)

    def norm_part(first, col, c):
        step = tokens // PIECES
        return normed.at[pl.ds(pl.multiple_of(first + c * step, EDGE), step),
                         pl.ds(pl.multiple_of(col * cols, 128), cols)]

    def norm_copy(i, c, arrival=False):
        first = base if i == 0 and not arrival else other_base
        col = (t, t, t, chip_peer)[i] if not arrival else (t, chip_peer, core_peer, lax.rem(core_peer + 2, tps))[i]
        to = ({"sp": mate}, {"tp": chip_peer}, {"tp": core_peer}, {"tp": core_peer})[i]
        ref = norm_part(first, col, c)
        return remote(ref, ref, norm_send.at[i], norm_recv.at[i, c], to)

    edge_from = pl.ds(pl.multiple_of(base + jnp.where(low, tokens - EDGE, 0), EDGE), EDGE)
    edge_over = pl.ds(pl.multiple_of(jnp.where(low, 0, EDGE + rows2), EDGE), EDGE)
    edge_here = pl.ds(pl.multiple_of(jnp.where(low, EDGE + rows2, 0), EDGE), EDGE)

    def edge_copy(i):
        return remote(normed.at[edge_from, my_cols], normed.at[edge_over, my_cols], edge_send.at[i],
                      edge_recv.at[0], {"sp": (mirror, beyond)[i]})

    def edge_arrival():
        ref = normed.at[edge_here, my_cols]
        return remote(ref, ref, edge_send.at[0], edge_recv.at[0], {"sp": mirror})

    def row_copy(j, arrival=False):
        col = lax.rem(t + tps - j, tps) if arrival else t
        ref = normed.at[edge_here, pl.ds(pl.multiple_of(col * cols, 128), cols)]
        return remote(ref, ref, row_send.at[j - 1], row_recv.at[j - 1], {"tp": lax.rem(t + j, tps)})

    tile = 256

    def source_of(slot):
        return (mate, jnp.where(low, n // 2, n // 2 - 1), jnp.where(low, n - 1, 0), s)[slot]

    with_edge = pl.ds(pl.multiple_of(jnp.where(low, EDGE, 0), EDGE), rows2 + EDGE)
    both = pl.ds(EDGE, rows2)

    def gate_of(slot):
        if slot != OWN:
            have(0, slot)
        k = pl.ds(pl.multiple_of(source_of(slot) * depth, 128), depth)

        @pl.loop(0, my_part // tile)
        def _(i):
            at = pl.ds(pl.multiple_of(i * tile, 128), tile)
            ga = jnp.dot(normed[with_edge, k], wg_all[slot, :, at], preferred_element_type=F32)
            gate[with_edge, at] = ga if slot == OWN else gate[with_edge, at] + ga

    def up_of(slot, last=False):
        if slot != OWN:
            have(1, slot)
        k = pl.ds(pl.multiple_of(source_of(slot) * depth, 128), depth)

        @pl.loop(0, my_part // tile)
        def _(i):
            at = pl.ds(pl.multiple_of(i * tile, 128), tile)
            ub = jnp.dot(normed[both, k], wu_all[slot, :, at], preferred_element_type=F32)
            if slot != OWN:
                ub = up[:, at] + ub
            if last:
                act[:, at] = (silu[:, at] * ub.astype(BF16).astype(F32)).astype(BF16)
            else:
                up[:, at] = ub

    @pl.when(inner)
    def _():
        for i in range(2):
            edge_copy(i).start()

    for c in range(PIECES):
        norm_copy(0, c).start()

    @pl.when(outer)
    def _():
        ship_all(OUT_MIRROR, 1)
        ship_all(OUT_MATE, 2)
        ship_all(OUT_REST, 2)
        take(0, 1)
        take(1, 0)

    @pl.when(inner)
    def _():
        ship_all(IN_ACROSS, 1)
        ship_all(IN_BEYOND, 1)
        ship_all(IN_MATE, 2)
        ship_all(IN_ACROSS, 2)
        ship_all(IN_BEYOND, 2)

    by_role(lambda r: [local(i, r).wait() for i in (5, 6, 7)])

    take(0, 2)

    @pl.when(inner)
    def _():
        take(1, 2)

    for c in range(PIECES):
        norm_copy(0, c, True).wait_recv()
        norm_copy(1, c).start()
        norm_copy(2, c).start()
    edge_arrival().wait_recv()
    for j in range(1, tps):
        row_copy(j).start()

    for c in range(PIECES):
        norm_copy(1, c, True).wait_recv()
        norm_copy(3, c).start()

    @pl.when(outer)
    def _():
        take(1, 2)

    for c in range(PIECES):
        norm_copy(2, c, True).wait_recv()
        norm_copy(3, c, True).wait_recv()
    for j in range(1, tps):
        row_copy(j, True).wait_recv()
    gate_of(OWN)
    gate_of(0)
    gate_of(2)
    gate_of(1)

    @pl.when(inner)
    def _():
        take(1, 1)
        take(2, 0)

    @pl.when(low)
    def _():
        gate[0:EDGE, :] = jnp.zeros((EDGE, parts[0]), F32)

    @pl.when(jnp.logical_not(low))
    def _():
        gate[EDGE + rows2:, :] = jnp.zeros((EDGE, parts[0]), F32)

    @pl.loop(0, my_part // 128)
    def _(i):
        at = pl.ds(pl.multiple_of(i * 128, 128), 128)
        ch = pl.ds(pl.multiple_of(hidden_at + i * 128, 128), 128)
        gate[:, at] = gate[:, at].astype(BF16).astype(F32)
        conv = cb_ref[pl.ds(role * (parts[0] // 128) + i, 1), :]
        for tap in range(CONV):
            conv = conv + gate[pl.ds(EDGE - CONV // 2 + tap, rows2), at] * cw_ref[tap:tap + 1, ch]
        silu[:, at] = conv / (1.0 + jnp.exp(-conv))

    @pl.when(outer)
    def _():
        take(2, 0)

    up_of(OWN)
    up_of(0)
    up_of(2)

    @pl.when(outer)
    def _():
        ship_all(OUT_MIRROR, 2)
        take(1, 1)


    up_of(1, last=True)

    @pl.when(inner)
    def _():
        take(2, 1, (0,))

    half_rows = tokens // 2
    wide = cols // SPLIT
    far_first = (1 - t // 2) * 2

    def is_far(p):
        return (p // 2) != (t // 2)

    def rows_of(i):
        return pl.ds(pl.multiple_of((base if i else other_base) - EDGE, tokens), tokens)

    def half_of(i, c):
        first = (base if i else other_base) - EDGE + c * half_rows
        return pl.ds(pl.multiple_of(first, half_rows), half_rows)

    def half_rows_of(c):
        return pl.ds(pl.multiple_of(c * half_rows, half_rows), half_rows)

    def block_of(c):
        return pl.ds(c * wide, wide)

    def near_copy(i, c):
        return remote(terms.at[core_peer, rows_of(i), block_of(c)], near_in.at[i, :, block_of(c)],
                      near_send.at[i, c], near_recv.at[i, c], {"tp": core_peer})

    def pair_copy(p, i, c):
        q = lax.rem(p, 2)
        return remote(terms.at[p, half_of(i, 1 - core), block_of(c)], pair_in.at[q, i, :, block_of(c)],
                      pair_send.at[q, i, c], pair_recv.at[q, i, c], {"tp": core_peer})

    def mid_copy(p, c):
        q = lax.rem(p, 2)
        return remote(terms.at[p, half_of(0, core), block_of(c)], mid_in.at[q, :, block_of(c)],
                      mid_send.at[q, c], mid_recv.at[q, c], {"sp": mate})

    def far_copy(p, c):
        return remote(terms.at[p, half_of(1, core), block_of(c)], far_in.at[half_rows_of(core), block_of(c)],
                      far_send.at[lax.rem(p, 2), c], far_recv.at[core, c], {"tp": p})

    def over_copy(slot, c):
        p = source_of(slot)
        to = {"tp": p} if slot == 1 else {"sp": mate, "tp": p}
        return remote(terms.at[p, half_of(0, core), block_of(c)], over_in.at[half_rows_of(core), block_of(c)],
                      over_send.at[slot - 1, c], over_recv.at[core, c], to)

    def over_arrival(h, c):
        ref = over_in.at[half_rows_of(h), block_of(c)]
        return remote(ref, ref, over_send.at[0, c], over_recv.at[h, c], {"sp": mate, "tp": far_first + h})

    def far_arrival(h, c):
        ref = far_in.at[half_rows_of(h), block_of(c)]
        return remote(ref, ref, far_send.at[h, c], far_recv.at[h, c], {"tp": far_first + h})

    def ret_copy(c):
        return remote(ret_out.at[:, block_of(c)], ret_in.at[:, block_of(c)], ret_send.at[c], ret_recv.at[c],
                      {"sp": mate})

    def down(slot, p, c, i):
        def run(r):
            w = wd_all[slot, 0:parts[r], block_of(c)]
            x = act[rows_of(i), 0:parts[r]]
            terms[p, rows_of(i), block_of(c)] = jnp.dot(x, w, preferred_element_type=F32).astype(BF16)

        by_role(run)

        @pl.when(p == core_peer)
        def _():
            near_copy(i, c).start()

        @pl.when(is_far(p))
        def _():
            pair_copy(p, i, c).start()

    def gather(p, c, late=None):
        for i in range(2):
            @pl.when(is_far(p))
            def _():
                pair_copy(p, i, c).wait_recv()
                rows = half_of(i, core)
                total = (terms[p, rows, block_of(c)].astype(F32)
                         + pair_in[lax.rem(p, 2), i, :, block_of(c)].astype(F32))
                terms[p, rows, block_of(c)] = total.astype(BF16)
                if i == 0 and late:
                    @pl.when(inner)
                    def _():
                        over_copy(late, c).start()

                    @pl.when(outer)
                    def _():
                        mid_copy(p, c).start()
                elif i == 0:
                    mid_copy(p, c).start()

        @pl.when((p == t) & outer if late == 1 else p == t)
        def _():
            near_copy(0, c).wait_recv()
            ret_out[:, block_of(c)] = (terms[t, rows_of(0), block_of(c)].astype(F32)
                                       + near_in[0, :, block_of(c)].astype(F32)).astype(BF16)
            ret_copy(c).start()

    def ret_late(c):
        @pl.when(inner & (t == source_of(1)))
        def _():
            near_copy(0, c).wait_recv()
            for h in range(2):
                over_arrival(h, c).wait_recv()
            ret_out[:, block_of(c)] = (terms[t, rows_of(0), block_of(c)].astype(F32)
                                       + near_in[0, :, block_of(c)].astype(F32)
                                       + over_in[:, block_of(c)].astype(F32)).astype(BF16)
            ret_copy(c).start()

    def send_far(p, c, last=False):
        if last:
            @pl.when(is_far(p))
            def _():
                far_copy(p, c).start()
            return

        @pl.when(is_far(p))
        def _():
            mid_copy(p, c).wait_recv()
            rows = half_of(1, core)
            total = terms[p, rows, block_of(c)].astype(F32) + mid_in[lax.rem(p, 2), :, block_of(c)].astype(F32)
            terms[p, rows, block_of(c)] = total.astype(BF16)
            far_copy(p, c).start()

    def finish(c):
        near_copy(1, c).wait_recv()
        at = pl.ds(pl.multiple_of(t * cols + c * wide, 128), wide)
        out = normed[pl.ds(base, tokens), at].astype(F32) + terms[t, rows_of(1), block_of(c)].astype(F32)
        out = out + near_in[1, :, block_of(c)].astype(F32)
        for h in range(2):
            far_arrival(h, c).wait_recv()
        out = out + far_in[:, block_of(c)].astype(F32)
        ret_copy(c).wait_recv()
        out = out + ret_in[:, block_of(c)].astype(F32)
        out_ref[:, block_of(c)] = out.astype(BF16)

        @pl.when(outer & (t == source_of(2)))
        def _():
            for h in range(2):
                over_arrival(h, c).wait_recv()
            out_ref[:, block_of(c)] = (out + over_in[:, block_of(c)].astype(F32)).astype(BF16)

    def downs(slot, p, c):
        for i in range(2):
            down(slot, p, c, i)

    def drain(ms):
        def run(r):
            for kind in ((IN_ACROSS, IN_BEYOND, IN_MATE, IN_RELAY), (OUT_MATE, OUT_MIRROR, OUT_REST))[r]:
                for m in ms:
                    if m == 2 or kind != OUT_REST:
                        shipped(kind, m)
            for m in ms:
                for slot in range(n - 1):
                    if not direct(m, slot, r):
                        crossed(m, slot, r)

        by_role(run)

    def drain_first():
        drain((0, 1))
        for i in range(4):
            ref = normed.at[pl.ds(EDGE, tokens), pl.ds(0, cols)]
            remote(ref, ref, norm_send.at[i], norm_recv.at[i, 0], {"sp": mate}).wait_send()
        for j in range(1, tps):
            row_copy(j).wait_send()

        @pl.when(inner)
        def _():
            for i in range(2):
                edge_copy(i).wait_send()

        @pl.when(has_left)
        def _():
            for i in range(2):
                halo_copy(i, True).wait_send()

        @pl.when(has_right)
        def _():
            for i in range(2):
                halo_copy(i, False).wait_send()

        for step in range(3):
            spread(*proj_args, step).wait_send()
            spread(*mix_args, step).wait_send()

    have(2, 0)
    early = [(jnp.where(inner, OWN, 0), jnp.where(inner, s, mate)), (jnp.where(inner, 0, OWN), jnp.where(inner, mate, s))]
    early = [(slot, p, c) for slot, p in early for c in range(SPLIT)]
    late = [(slot, source_of(slot), c) for slot in (1, 2) for c in range(SPLIT)]
    steps = early + late
    head = len(early)
    for at, (slot, p, c) in enumerate(steps):
        if at == head:
            gather(*steps[at - 1][1:])

            @pl.when(outer)
            def _():
                take(2, slot, (c,))

        if at >= head and at + 1 < len(steps):
            take(2, steps[at + 1][0], (steps[at + 1][2],))
        if at >= head:
            have(2, slot, (c,))
        downs(slot, p, c)
        if at >= head:
            gather(p, c, slot)
            if at in (head + 1, head + 2):
                ret_late(at - head - 1)
            send_far(*steps[at - head][1:])
            if at == head:
                drain_first()

            @pl.when(inner)
            def _():
                for late_at in {head: (), head + 1: (head,), head + 2: (head + 1, head + 2)}.get(at, (at,)):
                    send_far(*steps[late_at][1:])

            @pl.when(outer)
            def _():
                send_far(p, c, True)
        elif at:
            gather(*steps[at - 1][1:])

    drain((2,))
    for c in range(SPLIT):
        for i in range(2):
            near_copy(i, c).wait_send()
            for h in range(2):
                pair_copy(far_first + h, i, c).wait_send()

    def mids(here, owners):
        @pl.when(here)
        def _():
            for c in range(SPLIT):
                for p in owners:
                    @pl.when(is_far(p))
                    def _():
                        mid_copy(p, c).wait_send()

    mids(inner, [p for _, p, c in early if c == 0])
    mids(outer, [p for _, p, c in steps if c == 0])

    @pl.when(inner)
    def _():
        for slot in (1, 2):
            @pl.when(is_far(source_of(slot)))
            def _():
                for c in range(SPLIT):
                    over_copy(slot, c).wait_send()

    finish(0)
    ret_copy(0).wait_send()
    for h in range(2):
        far_copy(far_first + h, 0).wait_send()
    finish(1)
    ret_copy(1).wait_send()
    for h in range(2):
        far_copy(far_first + h, 1).wait_send()


def kernel_shards(
    sizes, queries, keys, values, sink, resid, out_proj, norm_gain, w_gate, w_up, conv_w, conv_b, w_down
):
    groups, n, tps = sizes
    tokens, width = resid.shape
    cols = out_proj.shape[1]
    depth, hidden = w_gate.shape
    part = parts_of(hidden)[0]
    vmem = pl.BlockSpec(memory_space=pltpu.VMEM)
    hbm = pl.BlockSpec(memory_space=pl.ANY)
    smem = pl.BlockSpec(memory_space=pltpu.SMEM)
    dma = pltpu.SemaphoreType.DMA
    block = (tokens, cols)
    return pl.pallas_call(
        functools.partial(layer_kernel, sizes),
        out_shape=jax.ShapeDtypeStruct((tokens, cols), BF16),
        in_specs=[hbm] * 3 + [smem, hbm, hbm, vmem, hbm, hbm, vmem, vmem, hbm],
        out_specs=vmem,
        scratch_shapes=[
            pltpu.VMEM(queries.shape, BF16),
            pltpu.VMEM((2, tokens + 2 * WINDOW, HD), BF16),
            pltpu.VMEM(resid.shape, BF16),
            pltpu.VMEM((tps,) + out_proj.shape, BF16),
            pltpu.VMEM((tps,) + queries.shape, BF16),
            pltpu.VMEM((tokens // 2, width), F32),
            pltpu.VMEM((2 * tokens + 2 * EDGE, width), BF16),
            pltpu.VMEM((n, depth, part), BF16),
            pltpu.VMEM((n, depth, part), BF16),
            pltpu.VMEM((n, part, cols), BF16),
            pltpu.VMEM((2 * tokens + 2 * EDGE, part), F32),
            pltpu.VMEM((2 * tokens, part), F32),
            pltpu.VMEM((2 * tokens, part), F32),
            pltpu.VMEM((2 * tokens, part), BF16),
            pltpu.VMEM((tps, 2 * tokens, cols), BF16),
            pltpu.VMEM((2,) + block, BF16),
            pltpu.VMEM((2, 2, tokens // 2, cols), BF16),
            pltpu.VMEM(block, BF16),
            pltpu.VMEM((2, tokens // 2, cols), BF16),
            pltpu.VMEM(block, BF16),
            pltpu.VMEM(block, BF16),
            pltpu.VMEM(block, BF16),
            dma((8,)), dma((2, 2)), dma((2, 2)),
            dma((3, 4)), dma((6 * PIECES + 3 * DEEP,)), dma((3, 3)), dma((6 * PIECES + 3 * DEEP,)),
            dma((3,)), dma((3,)), dma((3,)), dma((3,)), dma((4,)), dma((4, PIECES)), dma((2,)), dma((1,)),
            dma((3,)), dma((3,)),
            dma((2, SPLIT)), dma((2, SPLIT)), dma((2, 2, SPLIT)), dma((2, 2, SPLIT)),
            dma((2, SPLIT)), dma((2, SPLIT)), dma((2, SPLIT)), dma((2, SPLIT)),
            dma((2, SPLIT)), dma((2, SPLIT)), dma((SPLIT,)), dma((SPLIT,)),
        ],
        compiler_params=pltpu.CompilerParams(
            collective_id=0, has_side_effects=True, vmem_limit_bytes=67043328
        ),
    )(queries, keys, values, sink, resid, out_proj, norm_gain[None], w_gate, w_up, conv_w, conv_b.reshape(hidden // 128, 128), w_down)


def fits_kernel(sizes, args):
    groups, n, tps = sizes
    queries, resid, out_proj, w_gate, w_down = args[0], args[4], args[5], args[7], args[11]
    share = groups * PIECES
    weights = 3 * 2 * n * w_gate.shape[0] * w_gate.shape[1]
    return (
        n == 4
        and tps == 4
        and groups == 2
        and w_down.shape[1] == out_proj.shape[1]
        and w_gate.shape[0] % max(share * EDGE, 128) == 0
        and w_down.shape[1] % (groups * SPLIT * 128) == 0
        and w_gate.shape[1] % 768 == 0
        and resid.shape[0] % (4 * WINDOW) == 0
        and weights <= 20 * 2 ** 20
    )


def run_shards(sizes, *args):
    if fits_kernel(sizes, args):
        return kernel_shards(sizes, *args)
    return shards(*args)


def solution(mesh):
    sizes = tuple(mesh.shape[axis] for axis in ("grp", "sp", "tp"))
    return jax.shard_map(
        functools.partial(run_shards, sizes),
        mesh=mesh,
        in_specs=(
            P(("grp", "sp"), "tp"),
            P(("grp", "sp"), None),
            P(("grp", "sp"), None),
            P("tp"),
            P(("grp", "sp"), None),
            P(None, "tp"),
            P(),
            P("sp", "tp"),
            P("sp", "tp"),
            P(None, "tp"),
            P("tp"),
            P("tp", "sp"),
        ),
        out_specs=P(("grp", "sp"), "tp"),
        check_vma=False,
    )
```

```python
import functools

import jax
import jax.numpy as jnp
from jax import lax
from jax.experimental import pallas as pl
from jax.experimental.pallas import tpu as pltpu
from jax.sharding import PartitionSpec as P

H = 8
KVH = 2
HD = 128
WINDOW = 128
CONV = 3


def with_halo(cells, sides, width):
    for axis, dim in sides:
        count = lax.axis_size(axis)
        ends = count - 1
        head = lax.slice_in_dim(cells, 0, width, axis=dim)
        tail = lax.slice_in_dim(cells, cells.shape[dim] - width, cells.shape[dim], axis=dim)
        cells = jnp.concatenate(
            [
                lax.ppermute(tail, axis, [(i, (i + 1) % count) for i in range(ends)]),
                cells,
                lax.ppermute(head, axis, [((i + 1) % count, i) for i in range(ends)]),
            ],
            axis=dim,
        )
    return cells


def shards(
    queries, keys, values, sink, resid, out_proj, norm_gain, w_gate, w_up, conv_w, conv_b, w_down
):
    tokens = queries.shape[0]
    width = resid.shape[1]
    heads_here = sink.shape[0]
    group = H // KVH
    scale = HD ** (-0.5)
    first_head = lax.axis_index("tp") * heads_here
    kv_head = first_head // group
    own_keys = lax.dynamic_slice_in_dim(keys, kv_head * HD, HD, 1)
    own_values = lax.dynamic_slice_in_dim(values, kv_head * HD, HD, 1)
    extended = with_halo(jnp.stack([own_keys, own_values]), (("sp", 1),), WINDOW)
    ext_keys = extended[0]
    ext_values = extended[1]
    span = tokens + 2 * WINDOW
    q_heads = queries.reshape(tokens, heads_here, HD)
    scores = (
        jnp.einsum("qhd,kd->hqk", q_heads, ext_keys, preferred_element_type=jnp.float32) * scale
    )
    offset = lax.axis_index("sp") * tokens
    q_pos = offset + jnp.arange(tokens, dtype=jnp.int32)[:, None]
    k_pos = offset - WINDOW + jnp.arange(span, dtype=jnp.int32)[None, :]
    seq_total = tokens * lax.axis_size("sp")
    valid = (jnp.abs(q_pos - k_pos) <= WINDOW) & (k_pos >= 0) & (k_pos < seq_total)
    scores = jnp.where(valid[None], scores, jnp.float32(-1e30))
    sink_col = sink[:, None]
    top = jnp.maximum(jnp.max(scores, axis=-1), sink_col)
    expo = jnp.exp(scores - top[..., None])
    total = jnp.sum(expo, axis=-1) + jnp.exp(sink_col - top)
    weights = (expo / total[..., None]).astype(jnp.bfloat16)
    heads_out = jnp.einsum("hqk,kd->qhd", weights, ext_values, preferred_element_type=jnp.float32)
    heads_out = heads_out.astype(jnp.bfloat16).reshape(tokens, heads_here * HD)
    all_heads = lax.all_gather(heads_out, "tp", axis=1, tiled=True)
    cols = width // lax.axis_size("tp")
    col_start = lax.axis_index("tp") * cols
    full_proj = lax.all_gather(out_proj, "tp", axis=1, tiled=True)
    summed = resid.astype(jnp.float32) + jnp.dot(
        all_heads, full_proj, preferred_element_type=jnp.float32
    )
    mean = jnp.mean(summed, axis=-1, keepdims=True)
    msq = jnp.mean(summed * summed, axis=-1, keepdims=True)
    normed_full = ((summed - mean) * lax.rsqrt(msq - mean * mean + 1e-05) * norm_gain).astype(
        jnp.bfloat16
    )
    normed_own = lax.dynamic_slice_in_dim(normed_full, col_start, cols, 1)
    gate_acc = jnp.dot(
        normed_full,
        lax.all_gather(w_gate, "sp", axis=0, tiled=True),
        preferred_element_type=jnp.float32,
    )
    up_acc = jnp.dot(
        normed_full,
        lax.all_gather(w_up, "sp", axis=0, tiled=True),
        preferred_element_type=jnp.float32,
    )
    gate_pre = gate_acc.astype(jnp.bfloat16)
    up_part = up_acc.astype(jnp.bfloat16)
    padded = with_halo(gate_pre, (("sp", 0),), CONV // 2)
    conv = conv_b
    for tap in range(CONV):
        conv = conv + padded[tap : tap + tokens].astype(jnp.float32) * conv_w[tap]
    act = (jax.nn.silu(conv) * up_part.astype(jnp.float32)).astype(jnp.bfloat16)
    terms = jnp.dot(
        act, lax.all_gather(w_down, "sp", axis=1, tiled=True), preferred_element_type=jnp.float32
    )
    ffn_own = lax.psum_scatter(
        terms.astype(jnp.bfloat16), "tp", scatter_dimension=1, tiled=True
    ).astype(jnp.float32)
    return (normed_own.astype(jnp.float32) + ffn_own).astype(jnp.bfloat16)


EDGE = 16
SPLIT = 2
PIECES = 2
DEEP = 8
BF16 = jnp.bfloat16
F32 = jnp.float32


def parts_of(hidden):
    return hidden * 2 // 3, hidden // 3


def layer_kernel(
    sizes,
    q_hbm, k_hbm, v_hbm, sink_ref, resid_hbm, proj_hbm, gain_ref, wg_hbm, wu_hbm, cw_ref, cb_ref, wd_hbm,
    out_ref,
    q_ref, kv_ext, resid_ref, proj_all, mixed, summed, normed, wg_all, wu_all, wd_all, gate, up, silu, act,
    terms, near_in, pair_in, far_in, mid_in, over_in, ret_out, ret_in,
    local_sem, halo_send, halo_recv, z_send, z_recv, y_send, y_recv,
    proj_send, proj_recv, mix_send, mix_recv, norm_send, norm_recv, edge_send, edge_recv, row_send, row_recv,
    near_send, near_recv, pair_send, pair_recv, far_send, far_recv, mid_send, mid_recv, over_send, over_recv, ret_send, ret_recv,
):
    groups, n, tps = sizes
    g = lax.axis_index("grp")
    s = lax.axis_index("sp")
    t = lax.axis_index("tp")
    tokens, width = resid_hbm.shape
    heads_here = sink_ref.shape[0]
    cols = proj_hbm.shape[1]
    depth = wg_hbm.shape[0]
    hidden = wg_hbm.shape[1]
    parts = parts_of(hidden)
    starts = (0, parts[0])
    rows2 = 2 * tokens
    has_left, has_right = s > 0, s < n - 1
    inner = has_left & has_right
    outer = jnp.logical_not(inner)
    low = s < n // 2
    mate = s + 1 - 2 * lax.rem(s, 2)
    mirror = n - 1 - s
    beyond = n - 1 - mate
    role = 1 - jnp.where(inner, 1, 0)
    hidden_at = pl.multiple_of(role * parts[0], 128)
    my_part = jnp.where(inner, parts[0], parts[1])
    base = pl.multiple_of(EDGE + lax.rem(s, 2) * tokens, EDGE)
    other_base = pl.multiple_of(EDGE + (1 - lax.rem(s, 2)) * tokens, EDGE)
    core = lax.rem(t, 2)
    core_peer = t + 1 - 2 * core
    chip_peer = lax.rem(t + 2, tps)
    own = (wg_hbm, wu_hbm, wd_hbm)
    full = (wg_all, wu_all, wd_all)
    OWN = n - 1

    def remote(src, dst, send, recv, to):
        return pltpu.make_async_remote_copy(
            src_ref=src, dst_ref=dst, send_sem=send, recv_sem=recv,
            device_id=to, device_id_type=pl.DeviceIdType.MESH,
        )

    kv_head = (t * heads_here) // (H // KVH)
    kv_cols = pl.ds(pl.multiple_of(kv_head * HD, HD), HD)

    def by_role(fn):
        for r, here in enumerate((inner, outer)):
            @pl.when(here)
            def _():
                fn(r)

    def local(i, r=0):
        here, mine = pl.ds(starts[r], parts[r]), pl.ds(0, parts[r])
        src, dst = (
            (q_hbm, q_ref),
            (k_hbm.at[:, kv_cols], kv_ext.at[0, pl.ds(WINDOW, tokens)]),
            (v_hbm.at[:, kv_cols], kv_ext.at[1, pl.ds(WINDOW, tokens)]),
            (proj_hbm, proj_all.at[t]),
            (resid_hbm, resid_ref),
            (wg_hbm.at[:, here], wg_all.at[OWN, :, mine]),
            (wu_hbm.at[:, here], wu_all.at[OWN, :, mine]),
            (wd_hbm.at[here], wd_all.at[OWN, mine]),
        )[i]
        return pltpu.make_async_copy(src, dst, local_sem.at[i])

    for i in range(5):
        local(i).start()
    by_role(lambda r: [local(i, r).start() for i in (5, 6, 7)])

    barrier = pltpu.get_barrier_semaphore()

    def greet(to):
        pl.semaphore_signal(barrier, inc=1, device_id=to, device_id_type=pl.DeviceIdType.MESH)

    for j in range(1, n):
        greet({"sp": lax.rem(s + j, n)})
    for j in range(1, groups):
        greet({"grp": lax.rem(g + j, groups)})
    for j in range(1, tps):
        greet({"tp": lax.rem(t + j, tps)})
    for j in range(2):
        greet({"sp": mate, "tp": lax.rem(t - core + 2 + j, tps)})
    pl.semaphore_wait(barrier, n - 1 + groups - 1 + tps - 1 + 2)

    def halo_copy(i, to_left):
        ref = (k_hbm, v_hbm)[i]
        if to_left:
            return remote(ref.at[pl.ds(0, WINDOW), kv_cols], kv_ext.at[i, pl.ds(WINDOW + tokens, WINDOW)],
                          halo_send.at[i, 0], halo_recv.at[i, 0], {"sp": s - 1})
        return remote(ref.at[pl.ds(tokens - WINDOW, WINDOW), kv_cols], kv_ext.at[i, pl.ds(0, WINDOW)],
                      halo_send.at[i, 1], halo_recv.at[i, 1], {"sp": s + 1})

    deep = DEEP // SPLIT

    def count_of(m):
        return PIECES if m < 2 else DEEP

    def crossing(m, slot, c):
        return y_recv.at[m * (n - 1) + slot if m < 2 else 2 * (n - 1) + slot * SPLIT + c // deep]

    def landing(sems, m, slot, c):
        return sems.at[(m * (n - 1) + slot) * PIECES + c if m < 2 else 2 * (n - 1) * PIECES + slot * DEEP + c]

    def window(m, of, c, first, count):
        if m < 2:
            step = depth // (groups * PIECES)
            return pl.ds(pl.multiple_of((of * PIECES + c) * step, EDGE), step), pl.ds(first, count)
        step = cols // (groups * SPLIT)
        at = pl.multiple_of(((c // deep) * groups + of) * step, 128)
        return pl.ds(first + (c % deep) * (count // deep), count // deep), pl.ds(at, step)

    def source(m, r, of, c):
        return own[m].at[window(m, of, c, starts[r], parts[r])]

    def place(m, slot, r, of, c):
        return full[m].at[(slot,) + window(m, of, c, 0, parts[r])]

    IN_ACROSS, IN_BEYOND, IN_MATE, IN_RELAY, OUT_MATE, OUT_MIRROR, OUT_REST = range(7)

    def ship(kind, m, c):
        slot, to, lane = {
            IN_ACROSS: (1, mirror, 0),
            IN_BEYOND: (1, beyond, 1),
            IN_MATE: (0, mate, 2),
            IN_RELAY: (2, mirror, 3),
            OUT_MATE: (0, mate, 0),
            OUT_MIRROR: (2, mirror, 1),
            OUT_REST: (0, mate, 2),
        }[kind]
        r = 0 if kind in (IN_ACROSS, IN_RELAY, OUT_MATE, OUT_REST) else 1
        of = 1 - g if kind == OUT_REST else g
        src = place(m, 0, r, of, c) if kind == IN_RELAY else source(m, r, of, c)
        arrive = crossing(m, slot, c) if kind == OUT_REST else landing(z_recv, m, slot, c)
        return remote(src, place(m, slot, r, of, c), z_send.at[m, lane], arrive, {"sp": to})

    def ship_all(kind, m):
        for c in range(count_of(m)):
            ship(kind, m, c).start()

    def direct(m, slot, r):
        return r == 0 and m == 2 and isinstance(slot, int) and slot == 0

    def cross(m, slot, r, c):
        return remote(place(m, slot, r, g, c), place(m, slot, r, g, c), y_send.at[m, slot], crossing(m, slot, c),
                      {"grp": 1 - g})

    def share_of(m, r):
        if m < 2:
            return full[m].at[0, pl.ds(0, depth // groups), pl.ds(0, parts[r])]
        return full[m].at[0, pl.ds(0, parts[r]), pl.ds(0, cols // groups)]

    def shipped(kind, m):
        r = 0 if kind in (IN_ACROSS, IN_RELAY, OUT_MATE, OUT_REST) else 1
        lane = {IN_BEYOND: 1, IN_MATE: 2, IN_RELAY: 3, OUT_MIRROR: 1, OUT_REST: 2}.get(kind, 0)
        ref = share_of(m, r)
        remote(ref, ref, z_send.at[m, lane], landing(z_recv, m, 0, 0), {"sp": mate}).wait_send()

    def crossed(m, slot, r):
        ref = share_of(m, r)
        remote(ref, ref, y_send.at[m, slot], crossing(m, slot, 0), {"grp": 1 - g}).wait_send()

    def pieces_of(m, cs):
        return range(PIECES) if m < 2 else [c * deep + d for c in cs for d in range(deep)]

    def take(m, slot, cs=range(SPLIT)):
        def run(r):
            for c in pieces_of(m, cs):
                remote(place(m, slot, r, g, c), place(m, slot, r, g, c), z_send.at[m, 0], landing(z_recv, m, slot, c),
                       {"sp": mate}).wait_recv()
                if not direct(m, slot, r):
                    cross(m, slot, r, c).start()
                if isinstance(slot, int) and slot == 0 and r == 0:
                    ship(IN_RELAY, m, c).start()

        by_role(run)

    def have(m, slot, cs=range(SPLIT)):
        def run(r):
            for c in cs if m == 2 else (0,):
                if m < 2:
                    step = depth // groups
                    ref = full[m].at[slot, pl.ds(pl.multiple_of((1 - g) * step, EDGE), step), pl.ds(0, parts[r])]
                else:
                    step = cols // (groups * SPLIT)
                    at = pl.multiple_of((c * groups + 1 - g) * step, 128)
                    ref = full[m].at[slot, pl.ds(0, parts[r]), pl.ds(at, step)]
                remote(ref, ref, y_send.at[m, slot], crossing(m, slot, c * deep), {"grp": 1 - g}).wait_recv()

        by_role(run)

    def spread(src, ref, send, recv, step):
        origin = (t, t, chip_peer)[step]
        return remote(src if step < 2 else ref.at[origin], ref.at[origin], send.at[step], recv.at[step],
                      {"tp": (core_peer, chip_peer, core_peer)[step]})

    def spread_arrival(src, ref, send, recv, step):
        origin = (core_peer, chip_peer, lax.rem(core_peer + 2, tps))[step]
        return remote(src, ref.at[origin], send.at[step], recv.at[step],
                      {"tp": (core_peer, chip_peer, core_peer)[step]})

    proj_args = (proj_hbm, proj_all, proj_send, proj_recv)
    mix_args = (mixed.at[t], mixed, mix_send, mix_recv)

    @pl.when(has_left)
    def _():
        for i in range(2):
            halo_copy(i, True).start()

    @pl.when(has_right)
    def _():
        for i in range(2):
            halo_copy(i, False).start()

    @pl.when(outer)
    def _():
        ship_all(OUT_MATE, 0)
        ship_all(OUT_MATE, 1)
        ship_all(OUT_MIRROR, 0)

    @pl.when(inner)
    def _():
        ship_all(IN_ACROSS, 0)
        ship_all(IN_BEYOND, 0)
        ship_all(IN_MATE, 0)
        ship_all(IN_MATE, 1)

    for step in (1, 0):
        spread(*proj_args, step).start()

    @pl.when(jnp.logical_not(has_left))
    def _():
        kv_ext[:, pl.ds(0, WINDOW), :] = jnp.zeros((2, WINDOW, HD), BF16)

    @pl.when(jnp.logical_not(has_right))
    def _():
        kv_ext[:, pl.ds(WINDOW + tokens, WINDOW), :] = jnp.zeros((2, WINDOW, HD), BF16)

    for i in range(3):
        local(i).wait()

    @pl.when(has_right)
    def _():
        for i in range(2):
            halo_copy(i, True).wait_recv()

    @pl.when(has_left)
    def _():
        for i in range(2):
            halo_copy(i, False).wait_recv()

    span = 3 * WINDOW
    seq_total = tokens * n

    @pl.loop(0, tokens // WINDOW)
    def _(b):
        start = pl.multiple_of(b * WINDOW, WINDOW)
        row = lax.broadcasted_iota(jnp.int32, (WINDOW, span), 0)
        col = lax.broadcasted_iota(jnp.int32, (WINDOW, span), 1)
        k_pos = s * tokens + start - WINDOW + col
        valid = (jnp.abs(row + WINDOW - col) <= WINDOW) & (k_pos >= 0) & (k_pos < seq_total)
        kb = kv_ext[0, pl.ds(start, span), :]
        vb = kv_ext[1, pl.ds(start, span), :]
        for h in range(heads_here):
            qb = q_ref[pl.ds(start, WINDOW), h * HD:(h + 1) * HD]
            sc = lax.dot_general(qb, kb, (((1,), (1,)), ((), ())), preferred_element_type=F32) * (HD ** -0.5)
            sc = jnp.where(valid, sc, F32(-1e30))
            sink = sink_ref[h]
            top = jnp.maximum(jnp.max(sc, axis=-1, keepdims=True), sink)
            expo = jnp.exp(sc - top)
            total = jnp.sum(expo, axis=-1, keepdims=True) + jnp.exp(sink - top)
            weights = (expo / total).astype(BF16)
            o = jnp.dot(weights, vb, preferred_element_type=F32)
            mixed[t, pl.ds(start, WINDOW), h * HD:(h + 1) * HD] = o.astype(BF16)

    for step in (1, 0):
        spread(*mix_args, step).start()

    take(0, 0)

    @pl.when(inner)
    def _():
        take(0, 1)

    for args in (proj_args, mix_args):
        spread_arrival(*args, 1).wait_recv()
        spread(*args, 2).start()
    for args in (proj_args, mix_args):
        for step in (0, 2):
            spread_arrival(*args, step).wait_recv()

    @pl.when(inner)
    def _():
        take(1, 0)

    for i in (3, 4):
        local(i).wait()
    lanes = mixed.shape[2]
    block = summed.shape[0]
    strip = 64

    @pl.loop(0, tokens // block)
    def _(b):
        rows = pl.ds(pl.multiple_of(b * block, block), block)

        @pl.loop(0, tps)
        def _(i):
            at = pl.ds(pl.multiple_of(i * cols, 128), cols)
            prod = jnp.dot(mixed[0, rows, :], proj_all[i, pl.ds(0, lanes), :], preferred_element_type=F32)
            for u in range(1, tps):
                prod += jnp.dot(mixed[u, rows, :], proj_all[i, pl.ds(u * lanes, lanes), :],
                                preferred_element_type=F32)
            summed[:, at] = resid_ref[rows, at].astype(F32) + prod

        @pl.loop(0, block // strip)
        def _(i):
            at = pl.multiple_of(i * strip, strip)
            x = summed[pl.ds(at, strip), :]
            mean = jnp.mean(x, axis=-1, keepdims=True)
            msq = jnp.mean(x * x, axis=-1, keepdims=True)
            normed[pl.ds(pl.multiple_of(base + b * block + at, EDGE), strip), :] = (
                (x - mean) * lax.rsqrt(msq - mean * mean + 1e-05) * gain_ref[...]
            ).astype(BF16)

    my_cols = pl.ds(pl.multiple_of(t * cols, 128), cols)

    def norm_part(first, col, c):
        step = tokens // PIECES
        return normed.at[pl.ds(pl.multiple_of(first + c * step, EDGE), step),
                         pl.ds(pl.multiple_of(col * cols, 128), cols)]

    def norm_copy(i, c, arrival=False):
        first = base if i == 0 and not arrival else other_base
        col = (t, t, t, chip_peer)[i] if not arrival else (t, chip_peer, core_peer, lax.rem(core_peer + 2, tps))[i]
        to = ({"sp": mate}, {"tp": chip_peer}, {"tp": core_peer}, {"tp": core_peer})[i]
        ref = norm_part(first, col, c)
        return remote(ref, ref, norm_send.at[i], norm_recv.at[i, c], to)

    edge_from = pl.ds(pl.multiple_of(base + jnp.where(low, tokens - EDGE, 0), EDGE), EDGE)
    edge_over = pl.ds(pl.multiple_of(jnp.where(low, 0, EDGE + rows2), EDGE), EDGE)
    edge_here = pl.ds(pl.multiple_of(jnp.where(low, EDGE + rows2, 0), EDGE), EDGE)

    def edge_copy(i):
        return remote(normed.at[edge_from, my_cols], normed.at[edge_over, my_cols], edge_send.at[i],
                      edge_recv.at[0], {"sp": (mirror, beyond)[i]})

    def edge_arrival():
        ref = normed.at[edge_here, my_cols]
        return remote(ref, ref, edge_send.at[0], edge_recv.at[0], {"sp": mirror})

    def row_copy(j, arrival=False):
        col = lax.rem(t + tps - j, tps) if arrival else t
        ref = normed.at[edge_here, pl.ds(pl.multiple_of(col * cols, 128), cols)]
        return remote(ref, ref, row_send.at[j - 1], row_recv.at[j - 1], {"tp": lax.rem(t + j, tps)})

    tile = 256

    def source_of(slot):
        return (mate, jnp.where(low, n // 2, n // 2 - 1), jnp.where(low, n - 1, 0), s)[slot]

    with_edge = pl.ds(pl.multiple_of(jnp.where(low, EDGE, 0), EDGE), rows2 + EDGE)
    both = pl.ds(EDGE, rows2)

    def gate_of(slot):
        if slot != OWN:
            have(0, slot)
        k = pl.ds(pl.multiple_of(source_of(slot) * depth, 128), depth)

        @pl.loop(0, my_part // tile)
        def _(i):
            at = pl.ds(pl.multiple_of(i * tile, 128), tile)
            ga = jnp.dot(normed[with_edge, k], wg_all[slot, :, at], preferred_element_type=F32)
            gate[with_edge, at] = ga if slot == OWN else gate[with_edge, at] + ga

    def up_of(slot, last=False):
        if slot != OWN:
            have(1, slot)
        k = pl.ds(pl.multiple_of(source_of(slot) * depth, 128), depth)

        @pl.loop(0, my_part // tile)
        def _(i):
            at = pl.ds(pl.multiple_of(i * tile, 128), tile)
            ub = jnp.dot(normed[both, k], wu_all[slot, :, at], preferred_element_type=F32)
            if slot != OWN:
                ub = up[:, at] + ub
            if last:
                act[:, at] = (silu[:, at] * ub.astype(BF16).astype(F32)).astype(BF16)
            else:
                up[:, at] = ub

    @pl.when(inner)
    def _():
        for i in range(2):
            edge_copy(i).start()

    for c in range(PIECES):
        norm_copy(0, c).start()

    @pl.when(outer)
    def _():
        ship_all(OUT_MIRROR, 1)
        ship_all(OUT_MATE, 2)
        ship_all(OUT_REST, 2)
        take(0, 1)
        take(1, 0)

    @pl.when(inner)
    def _():
        ship_all(IN_ACROSS, 1)
        ship_all(IN_BEYOND, 1)
        ship_all(IN_MATE, 2)
        ship_all(IN_ACROSS, 2)
        ship_all(IN_BEYOND, 2)

    by_role(lambda r: [local(i, r).wait() for i in (5, 6, 7)])

    take(0, 2)

    @pl.when(inner)
    def _():
        take(1, 2)

    for c in range(PIECES):
        norm_copy(0, c, True).wait_recv()
        norm_copy(1, c).start()
        norm_copy(2, c).start()
    edge_arrival().wait_recv()
    for j in range(1, tps):
        row_copy(j).start()

    for c in range(PIECES):
        norm_copy(1, c, True).wait_recv()
        norm_copy(3, c).start()

    @pl.when(outer)
    def _():
        take(1, 2)

    for c in range(PIECES):
        norm_copy(2, c, True).wait_recv()
        norm_copy(3, c, True).wait_recv()
    for j in range(1, tps):
        row_copy(j, True).wait_recv()
    gate_of(OWN)
    gate_of(0)
    gate_of(2)
    gate_of(1)

    @pl.when(inner)
    def _():
        take(1, 1)
        take(2, 0)

    @pl.when(low)
    def _():
        gate[0:EDGE, :] = jnp.zeros((EDGE, parts[0]), F32)

    @pl.when(jnp.logical_not(low))
    def _():
        gate[EDGE + rows2:, :] = jnp.zeros((EDGE, parts[0]), F32)

    @pl.loop(0, my_part // 128)
    def _(i):
        at = pl.ds(pl.multiple_of(i * 128, 128), 128)
        ch = pl.ds(pl.multiple_of(hidden_at + i * 128, 128), 128)
        gate[:, at] = gate[:, at].astype(BF16).astype(F32)
        conv = cb_ref[pl.ds(role * (parts[0] // 128) + i, 1), :]
        for tap in range(CONV):
            conv = conv + gate[pl.ds(EDGE - CONV // 2 + tap, rows2), at] * cw_ref[tap:tap + 1, ch]
        silu[:, at] = conv / (1.0 + jnp.exp(-conv))

    @pl.when(outer)
    def _():
        take(2, 0)

    up_of(OWN)
    up_of(0)
    up_of(2)

    @pl.when(outer)
    def _():
        ship_all(OUT_MIRROR, 2)
        take(1, 1)


    up_of(1, last=True)

    @pl.when(inner)
    def _():
        take(2, 1, (0,))

    half_rows = tokens // 2
    wide = cols // SPLIT
    far_first = (1 - t // 2) * 2

    def is_far(p):
        return (p // 2) != (t // 2)

    def rows_of(i):
        return pl.ds(pl.multiple_of((base if i else other_base) - EDGE, tokens), tokens)

    def half_of(i, c):
        first = (base if i else other_base) - EDGE + c * half_rows
        return pl.ds(pl.multiple_of(first, half_rows), half_rows)

    def half_rows_of(c):
        return pl.ds(pl.multiple_of(c * half_rows, half_rows), half_rows)

    def block_of(c):
        return pl.ds(c * wide, wide)

    def near_copy(i, c):
        return remote(terms.at[core_peer, rows_of(i), block_of(c)], near_in.at[i, :, block_of(c)],
                      near_send.at[i, c], near_recv.at[i, c], {"tp": core_peer})

    def pair_copy(p, i, c):
        q = lax.rem(p, 2)
        return remote(terms.at[p, half_of(i, 1 - core), block_of(c)], pair_in.at[q, i, :, block_of(c)],
                      pair_send.at[q, i, c], pair_recv.at[q, i, c], {"tp": core_peer})

    def mid_copy(p, c):
        q = lax.rem(p, 2)
        return remote(terms.at[p, half_of(0, core), block_of(c)], mid_in.at[q, :, block_of(c)],
                      mid_send.at[q, c], mid_recv.at[q, c], {"sp": mate})

    def far_copy(p, c):
        return remote(terms.at[p, half_of(1, core), block_of(c)], far_in.at[half_rows_of(core), block_of(c)],
                      far_send.at[lax.rem(p, 2), c], far_recv.at[core, c], {"tp": p})

    def over_copy(slot, c):
        p = source_of(slot)
        to = {"tp": p} if slot == 1 else {"sp": mate, "tp": p}
        return remote(terms.at[p, half_of(0, core), block_of(c)], over_in.at[half_rows_of(core), block_of(c)],
                      over_send.at[slot - 1, c], over_recv.at[core, c], to)

    def over_arrival(h, c):
        ref = over_in.at[half_rows_of(h), block_of(c)]
        return remote(ref, ref, over_send.at[0, c], over_recv.at[h, c], {"sp": mate, "tp": far_first + h})

    def far_arrival(h, c):
        ref = far_in.at[half_rows_of(h), block_of(c)]
        return remote(ref, ref, far_send.at[h, c], far_recv.at[h, c], {"tp": far_first + h})

    def ret_copy(c):
        return remote(ret_out.at[:, block_of(c)], ret_in.at[:, block_of(c)], ret_send.at[c], ret_recv.at[c],
                      {"sp": mate})

    def down(slot, p, c, i):
        def run(r):
            w = wd_all[slot, 0:parts[r], block_of(c)]
            x = act[rows_of(i), 0:parts[r]]
            terms[p, rows_of(i), block_of(c)] = jnp.dot(x, w, preferred_element_type=F32).astype(BF16)

        by_role(run)

        @pl.when(p == core_peer)
        def _():
            near_copy(i, c).start()

        @pl.when(is_far(p))
        def _():
            pair_copy(p, i, c).start()

    def gather(p, c, late=None):
        for i in range(2):
            @pl.when(is_far(p))
            def _():
                pair_copy(p, i, c).wait_recv()
                rows = half_of(i, core)
                total = (terms[p, rows, block_of(c)].astype(F32)
                         + pair_in[lax.rem(p, 2), i, :, block_of(c)].astype(F32))
                terms[p, rows, block_of(c)] = total.astype(BF16)
                if i == 0 and late:
                    @pl.when(inner)
                    def _():
                        over_copy(late, c).start()

                    @pl.when(outer)
                    def _():
                        mid_copy(p, c).start()
                elif i == 0:
                    mid_copy(p, c).start()

        @pl.when((p == t) & outer if late == 1 else p == t)
        def _():
            near_copy(0, c).wait_recv()
            ret_out[:, block_of(c)] = (terms[t, rows_of(0), block_of(c)].astype(F32)
                                       + near_in[0, :, block_of(c)].astype(F32)).astype(BF16)
            ret_copy(c).start()

    def ret_late(c):
        @pl.when(inner & (t == source_of(1)))
        def _():
            near_copy(0, c).wait_recv()
            for h in range(2):
                over_arrival(h, c).wait_recv()
            ret_out[:, block_of(c)] = (terms[t, rows_of(0), block_of(c)].astype(F32)
                                       + near_in[0, :, block_of(c)].astype(F32)
                                       + over_in[:, block_of(c)].astype(F32)).astype(BF16)
            ret_copy(c).start()

    def send_far(p, c, last=False):
        if last:
            @pl.when(is_far(p))
            def _():
                far_copy(p, c).start()
            return

        @pl.when(is_far(p))
        def _():
            mid_copy(p, c).wait_recv()
            rows = half_of(1, core)
            total = terms[p, rows, block_of(c)].astype(F32) + mid_in[lax.rem(p, 2), :, block_of(c)].astype(F32)
            terms[p, rows, block_of(c)] = total.astype(BF16)
            far_copy(p, c).start()

    def finish(c):
        near_copy(1, c).wait_recv()
        at = pl.ds(pl.multiple_of(t * cols + c * wide, 128), wide)
        out = normed[pl.ds(base, tokens), at].astype(F32) + terms[t, rows_of(1), block_of(c)].astype(F32)
        out = out + near_in[1, :, block_of(c)].astype(F32)
        for h in range(2):
            far_arrival(h, c).wait_recv()
        out = out + far_in[:, block_of(c)].astype(F32)
        ret_copy(c).wait_recv()
        out = out + ret_in[:, block_of(c)].astype(F32)
        out_ref[:, block_of(c)] = out.astype(BF16)

        @pl.when(outer & (t == source_of(2)))
        def _():
            for h in range(2):
                over_arrival(h, c).wait_recv()
            out_ref[:, block_of(c)] = (out + over_in[:, block_of(c)].astype(F32)).astype(BF16)

    def downs(slot, p, c):
        for i in range(2):
            down(slot, p, c, i)

    def drain(ms):
        def run(r):
            for kind in ((IN_ACROSS, IN_BEYOND, IN_MATE, IN_RELAY), (OUT_MATE, OUT_MIRROR, OUT_REST))[r]:
                for m in ms:
                    if m == 2 or kind != OUT_REST:
                        shipped(kind, m)
            for m in ms:
                for slot in range(n - 1):
                    if not direct(m, slot, r):
                        crossed(m, slot, r)

        by_role(run)

    def drain_first():
        drain((0, 1))
        for i in range(4):
            ref = normed.at[pl.ds(EDGE, tokens), pl.ds(0, cols)]
            remote(ref, ref, norm_send.at[i], norm_recv.at[i, 0], {"sp": mate}).wait_send()
        for j in range(1, tps):
            row_copy(j).wait_send()

        @pl.when(inner)
        def _():
            for i in range(2):
                edge_copy(i).wait_send()

        @pl.when(has_left)
        def _():
            for i in range(2):
                halo_copy(i, True).wait_send()

        @pl.when(has_right)
        def _():
            for i in range(2):
                halo_copy(i, False).wait_send()

        for step in range(3):
            spread(*proj_args, step).wait_send()
            spread(*mix_args, step).wait_send()

    have(2, 0)
    early = [(jnp.where(inner, OWN, 0), jnp.where(inner, s, mate)), (jnp.where(inner, 0, OWN), jnp.where(inner, mate, s))]
    early = [(slot, p, c) for slot, p in early for c in range(SPLIT)]
    late = [(slot, source_of(slot), c) for slot in (1, 2) for c in range(SPLIT)]
    steps = early + late
    head = len(early)
    for at, (slot, p, c) in enumerate(steps):
        if at == head:
            gather(*steps[at - 1][1:])

            @pl.when(outer)
            def _():
                take(2, slot, (c,))

        if at >= head and at + 1 < len(steps):
            take(2, steps[at + 1][0], (steps[at + 1][2],))
        if at >= head:
            have(2, slot, (c,))
        downs(slot, p, c)
        if at >= head:
            gather(p, c, slot)
            if at in (head + 1, head + 2):
                ret_late(at - head - 1)
            send_far(*steps[at - head][1:])
            if at == head:
                drain_first()

            @pl.when(inner)
            def _():
                for late_at in {head: (), head + 1: (head,), head + 2: (head + 1, head + 2)}.get(at, (at,)):
                    send_far(*steps[late_at][1:])

            @pl.when(outer)
            def _():
                send_far(p, c, True)
        elif at:
            gather(*steps[at - 1][1:])

    drain((2,))
    for c in range(SPLIT):
        for i in range(2):
            near_copy(i, c).wait_send()
            for h in range(2):
                pair_copy(far_first + h, i, c).wait_send()

    def mids(here, owners):
        @pl.when(here)
        def _():
            for c in range(SPLIT):
                for p in owners:
                    @pl.when(is_far(p))
                    def _():
                        mid_copy(p, c).wait_send()

    mids(inner, [p for _, p, c in early if c == 0])
    mids(outer, [p for _, p, c in steps if c == 0])

    @pl.when(inner)
    def _():
        for slot in (1, 2):
            @pl.when(is_far(source_of(slot)))
            def _():
                for c in range(SPLIT):
                    over_copy(slot, c).wait_send()

    finish(0)
    ret_copy(0).wait_send()
    for h in range(2):
        far_copy(far_first + h, 0).wait_send()
    finish(1)
    ret_copy(1).wait_send()
    for h in range(2):
        far_copy(far_first + h, 1).wait_send()


def kernel_shards(
    sizes, queries, keys, values, sink, resid, out_proj, norm_gain, w_gate, w_up, conv_w, conv_b, w_down
):
    groups, n, tps = sizes
    tokens, width = resid.shape
    cols = out_proj.shape[1]
    depth, hidden = w_gate.shape
    part = parts_of(hidden)[0]
    vmem = pl.BlockSpec(memory_space=pltpu.VMEM)
    hbm = pl.BlockSpec(memory_space=pl.ANY)
    smem = pl.BlockSpec(memory_space=pltpu.SMEM)
    dma = pltpu.SemaphoreType.DMA
    block = (tokens, cols)
    return pl.pallas_call(
        functools.partial(layer_kernel, sizes),
        out_shape=jax.ShapeDtypeStruct((tokens, cols), BF16),
        in_specs=[hbm] * 3 + [smem, hbm, hbm, vmem, hbm, hbm, vmem, vmem, hbm],
        out_specs=vmem,
        scratch_shapes=[
            pltpu.VMEM(queries.shape, BF16),
            pltpu.VMEM((2, tokens + 2 * WINDOW, HD), BF16),
            pltpu.VMEM(resid.shape, BF16),
            pltpu.VMEM((tps,) + out_proj.shape, BF16),
            pltpu.VMEM((tps,) + queries.shape, BF16),
            pltpu.VMEM((tokens // 2, width), F32),
            pltpu.VMEM((2 * tokens + 2 * EDGE, width), BF16),
            pltpu.VMEM((n, depth, part), BF16),
            pltpu.VMEM((n, depth, part), BF16),
            pltpu.VMEM((n, part, cols), BF16),
            pltpu.VMEM((2 * tokens + 2 * EDGE, part), F32),
            pltpu.VMEM((2 * tokens, part), F32),
            pltpu.VMEM((2 * tokens, part), F32),
            pltpu.VMEM((2 * tokens, part), BF16),
            pltpu.VMEM((tps, 2 * tokens, cols), BF16),
            pltpu.VMEM((2,) + block, BF16),
            pltpu.VMEM((2, 2, tokens // 2, cols), BF16),
            pltpu.VMEM(block, BF16),
            pltpu.VMEM((2, tokens // 2, cols), BF16),
            pltpu.VMEM(block, BF16),
            pltpu.VMEM(block, BF16),
            pltpu.VMEM(block, BF16),
            dma((8,)), dma((2, 2)), dma((2, 2)),
            dma((3, 4)), dma((6 * PIECES + 3 * DEEP,)), dma((3, 3)), dma((6 + 3 * SPLIT,)),
            dma((3,)), dma((3,)), dma((3,)), dma((3,)), dma((4,)), dma((4, PIECES)), dma((2,)), dma((1,)),
            dma((3,)), dma((3,)),
            dma((2, SPLIT)), dma((2, SPLIT)), dma((2, 2, SPLIT)), dma((2, 2, SPLIT)),
            dma((2, SPLIT)), dma((2, SPLIT)), dma((2, SPLIT)), dma((2, SPLIT)),
            dma((2, SPLIT)), dma((2, SPLIT)), dma((SPLIT,)), dma((SPLIT,)),
        ],
        compiler_params=pltpu.CompilerParams(
            collective_id=0, has_side_effects=True, vmem_limit_bytes=67043328
        ),
    )(queries, keys, values, sink, resid, out_proj, norm_gain[None], w_gate, w_up, conv_w, conv_b.reshape(hidden // 128, 128), w_down)


def fits_kernel(sizes, args):
    groups, n, tps = sizes
    queries, resid, out_proj, w_gate, w_down = args[0], args[4], args[5], args[7], args[11]
    share = groups * PIECES
    weights = 3 * 2 * n * w_gate.shape[0] * w_gate.shape[1]
    return (
        n == 4
        and tps == 4
        and groups == 2
        and w_down.shape[1] == out_proj.shape[1]
        and w_gate.shape[0] % max(share * EDGE, 128) == 0
        and w_down.shape[1] % (groups * SPLIT * 128) == 0
        and w_gate.shape[1] % 768 == 0
        and resid.shape[0] % (4 * WINDOW) == 0
        and weights <= 20 * 2 ** 20
    )


def run_shards(sizes, *args):
    if fits_kernel(sizes, args):
        return kernel_shards(sizes, *args)
    return shards(*args)


def solution(mesh):
    sizes = tuple(mesh.shape[axis] for axis in ("grp", "sp", "tp"))
    return jax.shard_map(
        functools.partial(run_shards, sizes),
        mesh=mesh,
        in_specs=(
            P(("grp", "sp"), "tp"),
            P(("grp", "sp"), None),
            P(("grp", "sp"), None),
            P("tp"),
            P(("grp", "sp"), None),
            P(None, "tp"),
            P(),
            P("sp", "tp"),
            P("sp", "tp"),
            P(None, "tp"),
            P("tp"),
            P("tp", "sp"),
        ),
        out_specs=P(("grp", "sp"), "tp"),
        check_vma=False,
    )
```
